512 devices in a mesh: sp: 64 (over z, y), tp: 8 (over x, core).
Axes of the slice: x: 4, y: 8, z: 8, core: 2. Of those that a mesh axis runs over, the one named last changes fastest.
Arguments:
- tokens: bfloat16 [16384, 2048], P(('sp', 'tp')), may hold values from -6 to 6
- norm_gain: float32 [2048], replicated, may hold values from 0.1 to 1.9
- w_query: bfloat16 [2048, 1024], P('sp', 'tp'), may hold values from -0.125 to 0.125
- w_forget: bfloat16 [2048, 1024], P('sp', 'tp'), may hold values from -0.125 to 0.125
- w_value: bfloat16 [2048, 1024], P('sp', 'tp'), may hold values from -0.125 to 0.125
- w_outgate: bfloat16 [2048, 1024], P('sp', 'tp'), may hold values from -0.125 to 0.125
- leak: float32 [1024], P('tp'), may hold values from 1.2207031e-05 to 6.1035156e-05
- decay_shift: float32 [16384, 1024], P('sp', 'tp'), may hold values from -1 to 0
- head_gain: float32 [128], replicated, may hold values from 0.1 to 1.9
- w_glu_value: bfloat16 [2048, 2048], P('sp', 'tp'), may hold values from -0.125 to 0.125
- w_glu_gate: bfloat16 [2048, 2048], P('sp', 'tp'), may hold values from -0.125 to 0.125
- conv_kernel: float32 [31, 2048], P(None, 'tp'), may hold values from -20 to 20
- ln_gain: float32 [2048], P('tp'), may hold values from 0.1 to 1.9
- ln_bias: float32 [2048], P('tp'), may hold values from -3 to 3
- w_out_rec: bfloat16 [1024, 2048], P('tp', 'sp'), may hold values from -0.125 to 0.125
- w_out_conv: bfloat16 [2048, 2048], P('tp', 'sp'), may hold values from -0.09375 to 0.09375
Outputs:
- mixed: bfloat16 [16384, 2048], P(('sp', 'tp'))
The draws below stay inside these ranges and needn't reach their ends.
All inputs are finite; a program needn't handle non-finite values.
Results may differ from the reference program's by a relative error of at most 0.019.
Values may be sent and summed in bfloat16 or wider, within the bound.
No kernel may reach another device: no remote copies, remote signals or barrier semaphores. Data moves between devices by JAX's collectives and lax.ppermute only.
A program may use at most 64 MiB of HBM per device.

```python
import math
import jax
import jax.numpy as jnp
from jax import lax

D = 2048
HEADS = 8
HEAD_K = 128
HEAD_V = 128
CONV_CH = 2048
KERNEL = 31
BLOCK = 64
TOK_DEV = 256
SEQUENCE_SLOTS = 16384
KEYS_W = 1024
HG_W = 1024
N_TP = 8


def draw_decay_shift(key, part):
    key_width = HEADS * HEAD_K
    generator_seeds = jax.random.split(key, 7)
    fast_share = 0.5
    fast_head = jax.random.uniform(generator_seeds[0], (HEADS,), jnp.float32) < fast_share
    fast_head = jnp.repeat(fast_head, HEAD_K)
    fast_rate = jax.random.uniform(generator_seeds[1], (key_width,), jnp.float32, 0.02, 0.05)
    slow_rate = jax.random.uniform(generator_seeds[2], (key_width,), jnp.float32, 0.2, 0.7) / SEQUENCE_SLOTS
    forgetting_speeds = jnp.where(fast_head, fast_rate, slow_rate)
    block_count = SEQUENCE_SLOTS // TOK_DEV
    magnitude_multiplier = jnp.exp(jax.random.uniform(generator_seeds[3], (block_count,), jnp.float32, -0.7, 0.7))
    magnitude_multiplier = jnp.repeat(magnitude_multiplier, TOK_DEV)
    landscape_jaggedness = jax.random.uniform(generator_seeds[4], (SEQUENCE_SLOTS, key_width), jnp.float32, 0.5, 1.5)
    spike_location = jax.random.randint(generator_seeds[5], (2,), 0, SEQUENCE_SLOTS)
    within_spike_mask = jnp.any(jnp.arange(SEQUENCE_SLOTS)[:, None] == spike_location[None, :], axis=1)
    objective_readings = jax.random.uniform(generator_seeds[6], (key_width,), jnp.float32, 0.22, 0.69)
    payload_matrix_lines = -(forgetting_speeds[None, :] * magnitude_multiplier[:, None] * landscape_jaggedness) - jnp.where(within_spike_mask[:, None], objective_readings[None, :], 0.0)
    return payload_matrix_lines.astype(jnp.float32)


def draw_conv_kernel(key, part):
    generator_seeds = jax.random.split(key, 2)
    channel = jnp.arange(CONV_CH, dtype=jnp.float32) / CONV_CH
    rising = 3.0 ** channel
    spread = 0.5
    jitter = jnp.exp(jax.random.uniform(generator_seeds[0], (CONV_CH,), jnp.float32, -spread, spread))
    payload_matrix_lines = jnp.clip(jax.random.normal(generator_seeds[1], (KERNEL, CONV_CH), jnp.float32), -4.0, 4.0) * KERNEL ** (-0.5)
    return (payload_matrix_lines * rising * jitter).astype(jnp.float32)


def block_scale(stream_key, shape, shards, low, largest):
    loudness = 1.0
    for dim, parts in shards:
        draws = jax.random.uniform(jax.random.fold_in(jax.random.fold_in(stream_key, 6), dim), (parts,), jnp.float32, low / len(shards), largest / len(shards))
        loudness = loudness * jnp.repeat(jnp.exp(draws), shape[dim] // parts).reshape((-1,) + (1,) * (len(shape) - 1 - dim))
    return loudness


def scatter_about(stream_key, shape, scale, most, cuts=(), kind=jnp.bfloat16):
    array = scale * jax.random.normal(stream_key, shape, jnp.float32)
    if cuts:
        array = array * block_scale(stream_key, shape, cuts, -0.22, 0.18)
    return jnp.clip(array, -most, most).astype(kind)


def setup_inputs(seed: int = 0) -> dict:
    splits = jax.random.split(jax.random.key(seed), 17)
    return {
        "tokens": scatter_about(splits[0], (SEQUENCE_SLOTS, D), 1.0, 6.0, ((0, 512),)),
        "norm_gain": jnp.clip(1.0 + 0.18 * jax.random.normal(splits[1], (D,), jnp.float32), 0.1, 1.9),
        "w_query": scatter_about(splits[2], (D, KEYS_W), D ** -0.5, 0.125, ((0, 64), (1, 8))),
        "w_forget": scatter_about(splits[3], (D, KEYS_W), D ** -0.5, 0.125, ((0, 64), (1, 8))),
        "w_value": scatter_about(splits[4], (D, HG_W), D ** -0.5, 0.125, ((0, 64), (1, 8))),
        "w_outgate": scatter_about(splits[5], (D, HG_W), D ** -0.5, 0.125, ((0, 64), (1, 8))),
        "leak": jnp.clip(jnp.exp(math.log(6.103515625e-05) - 1.609438 * jax.random.uniform(splits[6], (KEYS_W,), jnp.float32) ** block_scale(splits[6], (KEYS_W,), ((0, 8),), -0.2, 0.2)), 1.220703143189894e-05, 6.103515625e-05),
        "decay_shift": draw_decay_shift(jax.random.fold_in(splits[16], 71), 0),
        "head_gain": jnp.clip(1.0 + 0.18 * jax.random.normal(splits[8], (HEAD_V,), jnp.float32), 0.1, 1.9),
        "w_glu_value": scatter_about(splits[9], (D, CONV_CH), D ** -0.5, 0.125, ((0, 64), (1, 8))),
        "w_glu_gate": scatter_about(splits[10], (D, CONV_CH), D ** -0.5, 0.125, ((0, 64), (1, 8))),
        "conv_kernel": draw_conv_kernel(jax.random.fold_in(splits[16], 71), 0),
        "ln_gain": jnp.clip(1.0 + 0.18 * jax.random.normal(splits[12], (CONV_CH,), jnp.float32), 0.1, 1.9),
        "ln_bias": scatter_about(splits[13], (CONV_CH,), 0.5, 3.0, ((0, 8),), jnp.float32),
        "w_out_rec": scatter_about(splits[14], (HG_W, D), (2 * HG_W) ** -0.5, 0.125, ((0, 8), (1, 64))),
        "w_out_conv": scatter_about(splits[15], (CONV_CH, D), (2 * CONV_CH) ** -0.5, 0.09375, ((0, 8), (1, 64))),
    }


exact_precision = lax.Precision.HIGHEST

def project(normed, weight):
    return jnp.dot(normed, weight, preferred_element_type=jnp.float32).astype(jnp.bfloat16)

def recurrence(queries, in_gate, payload_matrix_lines, log_decay):
    block_count = SEQUENCE_SLOTS // BLOCK

    def split_blocks(tensor):
        return tensor.reshape(block_count, BLOCK, HEADS, tensor.shape[-1])
    causal = jnp.tril(jnp.ones((BLOCK, BLOCK), jnp.float32))

    def advance(state_list, inputs):
        query_block, key_block, value_block, a_block = inputs
        cumulative_sum = jnp.cumsum(a_block, axis=0)
        gap_logs = jnp.minimum(cumulative_sum[:, None] - cumulative_sum[None, :], 0.0)
        decays = jnp.exp(gap_logs) * causal[:, :, None, None]
        scores = jnp.einsum('thk,shk,tshk->hts', query_block, key_block, decays, precision=exact_precision)
        within = jnp.einsum('hts,shv->thv', scores, value_block, precision=exact_precision)
        carried_state = jnp.einsum('aub,ubd->aud', query_block * jnp.exp(cumulative_sum), state_list, precision=exact_precision)
        block_finish = cumulative_sum[-1]
        added_terms = jnp.einsum('fjb,fji->jbi', key_block * jnp.exp(block_finish[None] - cumulative_sum), value_block, precision=exact_precision)
        state_list = jnp.exp(block_finish)[:, :, None] * state_list + added_terms
        return (state_list, within + carried_state)
    initial = jnp.zeros((HEADS, HEAD_K, HEAD_V), jnp.float32)
    _, outputs = lax.scan(advance, initial, (split_blocks(queries), split_blocks(in_gate), split_blocks(payload_matrix_lines), split_blocks(log_decay)))
    return outputs.reshape(SEQUENCE_SLOTS, HEADS, HEAD_V)

def reference(tokens, norm_gain, w_query, w_forget, w_value, w_outgate, leak, decay_shift, head_gain, w_glu_value, w_glu_gate, conv_kernel, ln_gain, ln_bias, w_out_rec, w_out_conv):
    values_in = tokens.astype(jnp.float32)
    row_scale = lax.rsqrt(lax.optimization_barrier(jnp.mean(values_in * values_in, axis=1, keepdims=True)) + 1e-06)
    normed = (values_in * row_scale * norm_gain).astype(jnp.bfloat16)
    query_pre = project(normed, w_query)
    forget_pre = project(normed, w_forget)
    value_pre = project(normed, w_value)
    gate_pre = project(normed, w_outgate)
    glu_value_pre = project(normed, w_glu_value)
    glu_gate_pre = project(normed, w_glu_gate)
    queries = jax.nn.silu(query_pre.astype(jnp.float32))
    in_gate = leak * jax.nn.sigmoid(-forget_pre.astype(jnp.float32))
    log_decay = jnp.log1p(-in_gate) + decay_shift
    recurrence_step = recurrence(queries.reshape(SEQUENCE_SLOTS, HEADS, HEAD_K), in_gate.reshape(SEQUENCE_SLOTS, HEADS, HEAD_K), value_pre.astype(jnp.float32).reshape(SEQUENCE_SLOTS, HEADS, HEAD_V), log_decay.reshape(SEQUENCE_SLOTS, HEADS, HEAD_K))
    scaling = lax.rsqrt(lax.optimization_barrier(jnp.mean(recurrence_step * recurrence_step, axis=2, keepdims=True)) + 1e-06)
    gate_act = jax.nn.silu(gate_pre.astype(jnp.float32)).reshape(SEQUENCE_SLOTS, HEADS, HEAD_V)
    head_out = (recurrence_step * scaling * head_gain * gate_act).reshape(SEQUENCE_SLOTS, HG_W).astype(jnp.bfloat16)
    glu = (glu_value_pre.astype(jnp.float32) * jax.nn.sigmoid(glu_gate_pre.astype(jnp.float32))).astype(jnp.bfloat16)
    padded = jnp.pad(glu.astype(jnp.float32), ((KERNEL - 1, 0), (0, 0)))
    conv_sum = jnp.zeros((SEQUENCE_SLOTS, CONV_CH), jnp.float32)
    for tap_index in range(KERNEL):
        conv_sum = conv_sum + conv_kernel[tap_index] * padded[tap_index:tap_index + SEQUENCE_SLOTS]
    row_mean = lax.optimization_barrier(jnp.mean(conv_sum, axis=1, keepdims=True))
    centered = conv_sum - row_mean
    row_var = lax.optimization_barrier(jnp.mean(centered * centered, axis=1, keepdims=True))
    conv_out = jax.nn.silu(centered * lax.rsqrt(row_var + 1e-05) * ln_gain + ln_bias).astype(jnp.bfloat16)
    rec_group = HG_W // N_TP
    conv_group = CONV_CH // N_TP
    summed = jnp.zeros((SEQUENCE_SLOTS, D), jnp.float32)
    for group_index in range(N_TP):
        rec_cols = slice(group_index * rec_group, (group_index + 1) * rec_group)
        conv_cols = slice(group_index * conv_group, (group_index + 1) * conv_group)
        partial_value = jnp.dot(head_out[:, rec_cols], w_out_rec[rec_cols], preferred_element_type=jnp.float32)
        partial_value = partial_value + jnp.dot(conv_out[:, conv_cols], w_out_conv[conv_cols], preferred_element_type=jnp.float32)
        rounded = lax.optimization_barrier(partial_value.astype(jnp.bfloat16))
        summed = summed + rounded.astype(jnp.float32)
    return summed.astype(jnp.bfloat16)
```

```python
import jax
import jax.numpy as jnp
from jax import lax
from jax.experimental import pallas as pl
from jax.experimental.pallas import tpu as pltpu
from jax.sharding import Mesh
from jax.sharding import PartitionSpec as P

HEAD_K = 128
KERNEL = 31
BLOCK = 64
HALO = 32
SP = ("sp_0", "sp_1")
SP_TP = ("sp_0", "sp_1", "tp")
F32 = jnp.float32
BF16 = jnp.bfloat16
EXACT = lax.Precision.HIGHEST
ANY = pl.BlockSpec(memory_space=pl.ANY)


def dot_nt(a, b):
    return lax.dot_general(a, b, (((1,), (1,)), ((), ())), preferred_element_type=F32)


def dot_tn(a, b):
    return lax.dot_general(a, b, (((0,), (0,)), ((), ())), preferred_element_type=F32)


def call(body, outs, *args, grid=None, in_specs=None, out_specs=None, scratch=()):
    specs = {}
    if in_specs is not None:
        specs["in_specs"] = in_specs
    if out_specs is not None:
        specs["out_specs"] = out_specs
    if grid is not None:
        specs["grid"] = grid
    return pl.pallas_call(body, out_shape=outs, scratch_shapes=scratch, **specs)(*args)


def whole(count):
    return [pl.BlockSpec(memory_space=pltpu.VMEM)] * count


def rec_weights_body(q, f, v, g, out):
    joined = jnp.concatenate([q[...], f[...], v[...], g[...]], axis=1)
    for k in range(out.shape[0]):
        out[k] = joined


def rest_weights_body(gv, gg, wr, wc, _, out):
    turned = [w[...].astype(F32).T.astype(BF16) for w in (wr, wc)]
    joined = jnp.concatenate([gv[...], gg[...], *turned], axis=1)
    for k in range(out.shape[0]):
        out[k] = joined


def copies_body(value, _, out):
    out[0] = value[...]


def norm_body(halo, tokens, gain, out):
    def scaled(rows):
        values_in = rows.astype(F32)
        row_scale = lax.rsqrt(jnp.mean(values_in * values_in, axis=1, keepdims=True) + 1e-06)
        return (values_in * row_scale * gain[...]).astype(BF16)

    out[:HALO] = scaled(halo[...])
    for k in range(tokens.shape[0]):
        width = tokens.shape[1]
        out[HALO + k * width : HALO + (k + 1) * width] = scaled(tokens[k])


def pack_state(out, state, total):
    high = total.astype(BF16).astype(F32)
    row = lax.broadcasted_iota(jnp.int32, (8, total.shape[1]), 0)
    tail = jnp.where(row == 0, high, jnp.where(row == 1, total - high, 0.0)).astype(BF16)
    state = state.astype(BF16)
    width = state.shape[0]
    for k in range(out.shape[0]):
        out[k, :width] = state
        out[k, width:] = tail


def rec_body(normed, weights, leak, shift, sent, local, device_query, gate_act):
    rows = normed.shape[0] - HALO
    projected = jnp.dot(normed[HALO:], weights[...], preferred_element_type=F32)
    projected = projected.astype(BF16).astype(F32)
    query_pre, forget_pre, value, gate_pre = [
        projected[:, k * HEAD_K : (k + 1) * HEAD_K] for k in range(4)
    ]
    gate_act[...] = jax.nn.silu(gate_pre)
    queries = jax.nn.silu(query_pre)
    in_gate = leak[...] * jax.nn.sigmoid(-forget_pre)
    log_decay = jnp.log1p(-in_gate) + shift[...]
    at_row = lax.broadcasted_iota(jnp.int32, (BLOCK, BLOCK), 0)
    at_col = lax.broadcasted_iota(jnp.int32, (BLOCK, BLOCK), 1)
    causal = at_row >= at_col
    triangle = jnp.where(causal, 1.0, 0.0).astype(F32)
    value = value.astype(BF16)
    state = jnp.zeros((HEAD_K, HEAD_K), F32)
    before = jnp.zeros((1, HEAD_K), F32)
    for n in range(rows // BLOCK):
        at = slice(n * BLOCK, (n + 1) * BLOCK)
        total = jnp.dot(triangle, log_decay[at], precision=EXACT, preferred_element_type=F32)
        last = total[BLOCK - 1 :]
        grown = queries[at] * jnp.exp(total)
        query = grown.astype(BF16)
        key = (in_gate[at] * jnp.exp(-total)).astype(BF16)
        scores = jnp.where(causal, dot_nt(query, key), 0.0).astype(BF16)
        within = jnp.dot(scores, value[at], preferred_element_type=F32)
        local[at] = within + dot_nt(query, state.astype(BF16))
        device_query[at] = (grown * jnp.exp(before)).astype(BF16)
        late_key = (in_gate[at] * jnp.exp(last - total)).astype(BF16)
        state = jnp.exp(last) * state + dot_tn(value[at], late_key)
        before = before + last
    pack_state(sent, state, before)


def unpack(got, k):
    tail = got[k, HEAD_K:].astype(F32)
    return got[k, :HEAD_K].astype(F32), tail[0:1] + tail[1:2]


def gathered_before(got, position):
    state = inside_state = jnp.zeros((HEAD_K, HEAD_K), F32)
    total = inside_total = jnp.zeros((1, HEAD_K), F32)
    for k in range(got.shape[0]):
        passed = k < position
        new_state, new_total = unpack(got, k)
        state = jnp.exp(new_total) * state + new_state
        total = total + new_total
        inside_state = jnp.where(passed, state, inside_state)
        inside_total = jnp.where(passed, total, inside_total)
    return inside_state, inside_total, state, total


def inner_body(position, got, sent, inner_state, inner_total):
    inside_state, inside_total, state, total = gathered_before(got, position[0])
    inner_state[...] = inside_state
    inner_total[...] = jnp.broadcast_to(inside_total, inner_total.shape)
    pack_state(sent, state, total)


def outer_body(position, got, inner_state, inner_total, device_query, local, gate_act, gain, out):
    outside_state = gathered_before(got, position[0])[0]
    incoming = jnp.exp(inner_total[0:1]) * outside_state + inner_state[...]
    recur = local[...] + dot_nt(device_query[...], incoming.astype(BF16))
    scaling = lax.rsqrt(jnp.mean(recur * recur, axis=1, keepdims=True) + 1e-06)
    out[...] = (recur * scaling * gain[...] * gate_act[...]).astype(BF16)


def conv_body(normed, weights, taps, conv, stats, shifted):
    channels = conv.shape[1]
    rows = conv.shape[0]
    filled = normed.shape[0]
    projected = jnp.dot(normed[...], weights[...], preferred_element_type=F32)
    projected = projected.astype(BF16).astype(F32)
    glu = projected[:, :channels] * jax.nn.sigmoid(projected[:, channels:])
    shifted[0, :filled] = glu.astype(BF16).astype(F32)
    for r in range(1, 8):
        shifted[r, : filled - 8] = shifted[0, r : filled - 8 + r]
    first = HALO - (KERNEL - 1)
    step = 32
    for row in range(0, rows, step):
        accum = jnp.zeros((step, channels), F32)
        for tap in range(KERNEL):
            off = row + first + tap
            base = off // 8 * 8
            accum = accum + taps[tap : tap + 1] * shifted[off - base, base : base + step]
        conv[row : row + step] = accum
    summed = conv[...]
    ones = jnp.ones((8, channels), F32)

    def over_channels(value):
        return lax.dot_general(
            ones, value, (((1,), (1,)), ((), ())), precision=EXACT, preferred_element_type=F32
        )

    row = lax.broadcasted_iota(jnp.int32, (8, rows), 0)
    both = jnp.where(row == 0, over_channels(summed), over_channels(summed * summed))[0:2]
    for k in range(stats.shape[0]):
        stats[k] = both


def out_body(stats, conv, head_out, ln_gain, ln_bias, w_rec, w_low, w_high, out):
    channels = conv.shape[1]
    both = stats[0]
    for k in range(1, stats.shape[0]):
        both = both + stats[k]
    both = both / (channels * stats.shape[0])
    mean = both[0:1]
    inverse = lax.rsqrt(both[1:2] - mean * mean + 1e-05)
    row = lax.broadcasted_iota(jnp.int32, (8, both.shape[1]), 0)
    paired = jnp.where(row == 0, mean, jnp.where(row == 1, inverse, 0.0))

    def column(k):
        chosen = jnp.where(lax.broadcasted_iota(jnp.int32, (8, channels), 0) == k, 1.0, 0.0)
        return lax.dot_general(
            paired,
            chosen.astype(F32),
            (((0,), (0,)), ((), ())),
            precision=EXACT,
            preferred_element_type=F32,
        )

    normal = (conv[...] - column(0)) * column(1) * ln_gain[...] + ln_bias[...]
    conv_out = jax.nn.silu(normal).astype(BF16)
    half = channels // 2
    mixed = dot_nt(head_out[...], w_rec[...])
    mixed = mixed + dot_nt(conv_out[:, :half], w_low[...])
    mixed = mixed + dot_nt(conv_out[:, half:], w_high[...])
    out[...] = mixed.astype(BF16)


def swap(value, axis):
    return lax.all_to_all(value, axis, split_axis=0, concat_axis=0, tiled=True)


def two_stage(copies):
    inner = swap(copies, SP[1])
    peers, rows, width = inner.shape
    return inner, lax.all_gather(inner.reshape(peers * rows, width), SP[0], axis=0, tiled=True)


def on_device(
    tokens,
    norm_gain,
    w_query,
    w_forget,
    w_value,
    w_outgate,
    leak,
    decay_shift,
    head_gain,
    w_glu_value,
    w_glu_gate,
    conv_kernel,
    ln_gain,
    ln_bias,
    w_out_rec,
    w_out_conv,
):
    shape = jax.ShapeDtypeStruct
    inner_count = lax.axis_size(SP[1])
    group = lax.axis_size("tp")
    depth, width = w_query.shape[0], 4 * HEAD_K
    copies = call(
        rec_weights_body,
        shape((inner_count, depth, width), BF16),
        w_query,
        w_forget,
        w_value,
        w_outgate,
    )
    staged, rec_weights = two_stage(copies)
    glu_width = w_glu_value.shape[1] + w_glu_gate.shape[1]
    rest = glu_width + w_out_rec.shape[0] + w_out_conv.shape[0]
    copies = call(
        rest_weights_body,
        shape((inner_count, depth, rest), BF16),
        w_glu_value,
        w_glu_gate,
        w_out_rec,
        w_out_conv,
        staged,
        in_specs=whole(4) + [ANY],
    )
    staged, rest_weights = two_stage(copies)
    share, features = tokens.shape
    copies = call(
        copies_body,
        shape((group, share, features), BF16),
        tokens,
        staged,
        grid=(group,),
        in_specs=[pl.BlockSpec((share, features), lambda k: (0, 0)), ANY],
        out_specs=pl.BlockSpec((1, share, features), lambda k: (k, 0, 0)),
    )
    block = swap(copies, "tp")
    count = lax.axis_size(SP)
    halo = lax.ppermute(block[group - 1], SP, [(k, k + 1) for k in range(count - 1)])
    rows = group * share
    normed = call(
        norm_body, shape((HALO + rows, features), BF16), halo, block, norm_gain.reshape(1, -1)
    )
    message = shape((inner_count, HEAD_K + 8, HEAD_K), BF16)
    sent, local, device_query, gate_act = call(
        rec_body,
        (message, shape((rows, HEAD_K), F32), shape((rows, HEAD_K), BF16), shape((rows, HEAD_K), F32)),
        normed,
        rec_weights,
        leak.reshape(1, -1),
        decay_shift,
    )
    smem = pl.BlockSpec(memory_space=pltpu.SMEM)
    sent, inner_state, inner_total = call(
        inner_body,
        (message, shape((HEAD_K, HEAD_K), F32), shape((8, HEAD_K), F32)),
        lax.axis_index(SP[1]).reshape(1),
        swap(sent, SP[1]),
        in_specs=[smem] + whole(1),
    )
    head_out = call(
        outer_body,
        shape((rows, HEAD_K), BF16),
        lax.axis_index(SP[0]).reshape(1),
        swap(sent, SP[0]),
        inner_state,
        inner_total,
        device_query,
        local,
        gate_act,
        head_gain.reshape(1, -1),
        in_specs=[smem] + whole(7),
    )
    channels = conv_kernel.shape[1]

    def part(size, at):
        return pl.BlockSpec((rest_weights.shape[0], size), lambda k: (0, at))

    def full(*lengths):
        return pl.BlockSpec(lengths, lambda k: (0,) * len(lengths))

    conv, stats = call(
        conv_body,
        (shape((rows, channels), F32), shape((group, 2, rows), F32)),
        normed,
        rest_weights,
        conv_kernel,
        grid=(1,),
        in_specs=[full(*normed.shape), part(glu_width, 0), full(*conv_kernel.shape)],
        out_specs=(full(rows, channels), full(group, 2, rows)),
        scratch=(pltpu.VMEM((8, HALO + rows, channels), F32),),
    )
    stats = swap(stats, "tp")
    mixed = call(
        out_body,
        shape((rows, features), BF16),
        stats,
        conv,
        head_out,
        ln_gain.reshape(1, -1),
        ln_bias.reshape(1, -1),
        rest_weights,
        rest_weights,
        rest_weights,
        grid=(1,),
        in_specs=[
            full(*stats.shape),
            full(rows, channels),
            full(rows, HEAD_K),
            full(1, channels),
            full(1, channels),
            *[part(HEAD_K, glu_width // HEAD_K + k) for k in range(3)],
        ],
        out_specs=full(rows, features),
    )
    arrived = swap(mixed.reshape(group, share, features), "tp")
    return arrived.astype(F32).sum(axis=0).astype(BF16)


def solution(mesh):
    torus = Mesh(mesh.devices.reshape(8, 8, mesh.shape["tp"]), SP_TP)
    placed = (
        P(SP_TP, None),
        P(),
        P(SP, "tp"),
        P(SP, "tp"),
        P(SP, "tp"),
        P(SP, "tp"),
        P("tp"),
        P(SP, "tp"),
        P(),
        P(SP, "tp"),
        P(SP, "tp"),
        P(None, "tp"),
        P("tp"),
        P("tp"),
        P("tp", SP),
        P("tp", SP),
    )
    return jax.shard_map(
        on_device, mesh=torus, in_specs=placed, out_specs=P(SP_TP, None), check_vma=False
    )
```

```python
import jax
import jax.numpy as jnp
from jax import lax
from jax.experimental import pallas as pl
from jax.experimental.pallas import tpu as pltpu
from jax.sharding import Mesh
from jax.sharding import PartitionSpec as P

HEAD_K = 128
KERNEL = 31
BLOCK = 64
HALO = 32
SP = ("sp_0", "sp_1")
TP = ("x", "core")
SP_TP = SP + TP
F32 = jnp.float32
BF16 = jnp.bfloat16
EXACT = lax.Precision.HIGHEST
ANY = pl.BlockSpec(memory_space=pl.ANY)


def dot_nt(a, b):
    return lax.dot_general(a, b, (((1,), (1,)), ((), ())), preferred_element_type=F32)


def dot_tn(a, b):
    return lax.dot_general(a, b, (((0,), (0,)), ((), ())), preferred_element_type=F32)


def call(body, outs, *args, grid=None, in_specs=None, out_specs=None, scratch=()):
    specs = {}
    if in_specs is not None:
        specs["in_specs"] = in_specs
    if out_specs is not None:
        specs["out_specs"] = out_specs
    if grid is not None:
        specs["grid"] = grid
    return pl.pallas_call(body, out_shape=outs, scratch_shapes=scratch, **specs)(*args)


def whole(count):
    return [pl.BlockSpec(memory_space=pltpu.VMEM)] * count


def first_body(gv, gg, q, g, wr, wc, tokens, operand, copies):
    operand[...] = jnp.concatenate([w[...] for w in (gv, gg, q, g, wr, wc)], axis=1)
    for k in range(copies.shape[0]):
        copies[k] = tokens[...]


def second_body(f, v, _, copies):
    joined = jnp.concatenate([f[...], v[...]], axis=1)
    for k in range(copies.shape[0]):
        copies[k] = joined


def norm_body(core, own, other, gain, out, tail):
    peers, share, _ = own.shape

    def scaled(rows):
        values_in = rows.astype(F32)
        row_scale = lax.rsqrt(jnp.mean(values_in * values_in, axis=1, keepdims=True) + 1e-06)
        return (values_in * row_scale * gain[...]).astype(BF16)

    def place(even, odd):
        for k in range(peers):
            out[2 * k * share : (2 * k + 1) * share] = scaled(even[k])
            done = scaled(odd[k])
            out[(2 * k + 1) * share : (2 * k + 2) * share] = done
        tail[...] = done

    @pl.when(core[0] == 0)
    def _():
        place(own, other)

    @pl.when(core[0] != 0)
    def _():
        place(other, own)


def pack_state(out, state, total):
    high = total.astype(BF16).astype(F32)
    row = lax.broadcasted_iota(jnp.int32, (8, total.shape[1]), 0)
    tail = jnp.where(row == 0, high, jnp.where(row == 1, total - high, 0.0)).astype(BF16)
    state = state.astype(BF16)
    width = state.shape[0]
    for k in range(out.shape[0]):
        out[k, :width] = state
        out[k, width:] = tail


def causal_mask():
    at_row = lax.broadcasted_iota(jnp.int32, (BLOCK, BLOCK), 0)
    at_col = lax.broadcasted_iota(jnp.int32, (BLOCK, BLOCK), 1)
    return at_row >= at_col


def state_body(normed, weights, leak, shift, sent, value_out, key, totals, starts, befores):
    rows = normed.shape[0]
    projected = jnp.dot(normed[...], weights[...], preferred_element_type=F32).astype(BF16)
    value = projected[:, HEAD_K:]
    value_out[...] = value
    in_gate = leak[...] * jax.nn.sigmoid(-projected[:, :HEAD_K].astype(F32))
    log_decay = jnp.log1p(-in_gate) + shift[...]
    triangle = jnp.where(causal_mask(), 1.0, 0.0).astype(F32)
    state = jnp.zeros((HEAD_K, HEAD_K), F32)
    before = jnp.zeros((1, HEAD_K), F32)
    kept = []
    for n in range(rows // BLOCK):
        at = slice(n * BLOCK, (n + 1) * BLOCK)
        total = jnp.dot(triangle, log_decay[at], precision=EXACT, preferred_element_type=F32)
        last = total[BLOCK - 1 :]
        totals[at] = total
        key[at] = (in_gate[at] * jnp.exp(-total)).astype(BF16)
        starts[n] = state.astype(BF16)
        kept.append(before)
        late_key = (in_gate[at] * jnp.exp(last - total)).astype(BF16)
        state = jnp.exp(last) * state + dot_tn(value[at], late_key)
        before = before + last
    befores[...] = jnp.concatenate(kept, axis=0)
    pack_state(sent, state, before)


def unpack(got, k):
    tail = got[k, HEAD_K:].astype(F32)
    return got[k, :HEAD_K].astype(F32), tail[0:1] + tail[1:2]


def gathered_before(got, position):
    state = inside_state = jnp.zeros((HEAD_K, HEAD_K), F32)
    total = inside_total = jnp.zeros((1, HEAD_K), F32)
    for k in range(got.shape[0]):
        passed = k < position
        new_state, new_total = unpack(got, k)
        state = jnp.exp(new_total) * state + new_state
        total = total + new_total
        inside_state = jnp.where(passed, state, inside_state)
        inside_total = jnp.where(passed, total, inside_total)
    return inside_state, inside_total, state, total


def inner_body(position, got, sent, inner_state, inner_total):
    inside_state, inside_total, state, total = gathered_before(got, position[0])
    inner_state[...] = inside_state
    inner_total[...] = jnp.broadcast_to(inside_total, inner_total.shape)
    pack_state(sent, state, total)


def outer_body(
    position,
    got,
    inner_state,
    inner_total,
    normed,
    weights,
    value,
    key,
    totals,
    starts,
    befores,
    gain,
    out,
):
    outside_state = gathered_before(got, position[0])[0]
    incoming = jnp.exp(inner_total[0:1]) * outside_state + inner_state[...]
    projected = jnp.dot(normed[...], weights[...], preferred_element_type=F32)
    projected = projected.astype(BF16).astype(F32)
    queries = jax.nn.silu(projected[:, :HEAD_K])
    gate_act = jax.nn.silu(projected[:, HEAD_K:])
    causal = causal_mask()
    for n in range(starts.shape[0]):
        at = slice(n * BLOCK, (n + 1) * BLOCK)
        query = (queries[at] * jnp.exp(totals[at])).astype(BF16)
        scores = jnp.where(causal, dot_nt(query, key[at]), 0.0).astype(BF16)
        state = jnp.exp(befores[n : n + 1]) * incoming + starts[n].astype(F32)
        recur = jnp.dot(scores, value[at], preferred_element_type=F32)
        recur = recur + dot_nt(query, state.astype(BF16))
        scaling = lax.rsqrt(jnp.mean(recur * recur, axis=1, keepdims=True) + 1e-06)
        out[at] = (recur * scaling * gain[...] * gate_act[at]).astype(BF16)


def conv_body(halo, normed, weights, taps, conv, stats, shifted):
    channels = conv.shape[1]
    rows = conv.shape[0]
    filled = HALO + rows
    extended = jnp.concatenate([halo[...], normed[...]], axis=0)
    projected = jnp.dot(extended, weights[...], preferred_element_type=F32)
    projected = projected.astype(BF16).astype(F32)
    glu = projected[:, :channels] * jax.nn.sigmoid(projected[:, channels:])
    shifted[0, :filled] = glu.astype(BF16).astype(F32)
    for r in range(1, 8):
        shifted[r, : filled - 8] = shifted[0, r : filled - 8 + r]
    first = HALO - (KERNEL - 1)
    step = 32
    for row in range(0, rows, step):
        accum = jnp.zeros((step, channels), F32)
        for tap in range(KERNEL):
            off = row + first + tap
            base = off // 8 * 8
            accum = accum + taps[tap : tap + 1] * shifted[off - base, base : base + step]
        conv[row : row + step] = accum
    summed = conv[...]
    ones = jnp.ones((8, channels), F32)

    def over_channels(value):
        return lax.dot_general(
            ones, value, (((1,), (1,)), ((), ())), precision=EXACT, preferred_element_type=F32
        )

    row = lax.broadcasted_iota(jnp.int32, (8, rows), 0)
    both = jnp.where(row == 0, over_channels(summed), over_channels(summed * summed))[0:2]
    for k in range(stats.shape[0]):
        stats[k] = both


def out_body(stats, conv, head_out, ln_gain, ln_bias, w_rec, w_low, w_high, out, conv_out):
    channels = conv.shape[1]

    @pl.when(pl.program_id(0) == 0)
    def _():
        both = stats[0]
        for k in range(1, stats.shape[0]):
            both = both + stats[k]
        both = both / (channels * stats.shape[0])
        mean = both[0:1]
        inverse = lax.rsqrt(both[1:2] - mean * mean + 1e-05)
        row = lax.broadcasted_iota(jnp.int32, (8, both.shape[1]), 0)
        paired = jnp.where(row == 0, mean, jnp.where(row == 1, inverse, 0.0))

        def column(k):
            chosen = jnp.where(lax.broadcasted_iota(jnp.int32, (8, channels), 0) == k, 1.0, 0.0)
            return lax.dot_general(
                paired,
                chosen.astype(F32),
                (((0,), (0,)), ((), ())),
                precision=EXACT,
                preferred_element_type=F32,
            )

        normal = (conv[...] - column(0)) * column(1) * ln_gain[...] + ln_bias[...]
        conv_out[...] = jax.nn.silu(normal).astype(BF16)

    half = channels // 2
    mixed = dot_nt(head_out[...], w_rec[...])
    mixed = mixed + dot_nt(conv_out[:, :half], w_low[...])
    mixed = mixed + dot_nt(conv_out[:, half:], w_high[...])
    out[...] = mixed.astype(BF16)


def swap(value, axis):
    return lax.all_to_all(value, axis, split_axis=0, concat_axis=0, tiled=True)


def on_device(
    tokens,
    norm_gain,
    w_query,
    w_forget,
    w_value,
    w_outgate,
    leak,
    decay_shift,
    head_gain,
    w_glu_value,
    w_glu_gate,
    conv_kernel,
    ln_gain,
    ln_bias,
    w_out_rec,
    w_out_conv,
):
    shape = jax.ShapeDtypeStruct
    smem = pl.BlockSpec(memory_space=pltpu.SMEM)
    inner_count = lax.axis_size(SP[1])
    group = lax.axis_size(TP)
    share, features = tokens.shape
    depth = w_query.shape[0]
    channels = conv_kernel.shape[1]
    columns = (w_glu_value, w_glu_gate, w_query, w_outgate, w_out_rec.T, w_out_conv.T)
    glu_width = 2 * channels
    all_width = sum(w.shape[1] for w in columns)
    operand, copies = call(
        first_body,
        (
            shape((depth, all_width), BF16),
            shape((lax.axis_size(TP[0]), share, features), BF16),
        ),
        *columns,
        tokens,
    )
    gathered = lax.all_gather(operand, SP, axis=0, tiled=True)
    own = swap(copies, TP[0])
    other = lax.ppermute(own, TP[1], [(0, 1), (1, 0)])
    rows = group * share
    normed, tail = call(
        norm_body,
        (shape((rows, features), BF16), shape((share, features), BF16)),
        lax.axis_index(TP[1]).reshape(1),
        own,
        other,
        norm_gain.reshape(1, -1),
        in_specs=[smem] + whole(3),
    )
    count = lax.axis_size(SP)
    copies = call(
        second_body,
        shape((count, depth, 2 * HEAD_K), BF16),
        w_forget,
        w_value,
        other,
        in_specs=whole(2) + [ANY],
    )
    state_weights = swap(copies, SP).reshape(count * depth, 2 * HEAD_K)
    halo = lax.ppermute(tail, SP, [(k, k + 1) for k in range(count - 1)])
    message = shape((inner_count, HEAD_K + 8, HEAD_K), BF16)
    blocks = rows // BLOCK
    sent, *kept = call(
        state_body,
        (
            message,
            shape((rows, HEAD_K), BF16),
            shape((rows, HEAD_K), BF16),
            shape((rows, HEAD_K), F32),
            shape((blocks, HEAD_K, HEAD_K), BF16),
            shape((blocks, HEAD_K), F32),
        ),
        normed,
        state_weights,
        leak.reshape(1, -1),
        decay_shift,
    )
    sent, inner_state, inner_total = call(
        inner_body,
        (message, shape((HEAD_K, HEAD_K), F32), shape((8, HEAD_K), F32)),
        lax.axis_index(SP[1]).reshape(1),
        swap(sent, SP[1]),
        in_specs=[smem] + whole(1),
    )

    def part(size, at):
        return pl.BlockSpec((gathered.shape[0], size), lambda k: (0, at))

    def full(*lengths):
        return pl.BlockSpec(lengths, lambda k: (0,) * len(lengths))

    conv, stats = call(
        conv_body,
        (shape((rows, channels), F32), shape((group, 2, rows), F32)),
        halo,
        normed,
        gathered,
        conv_kernel,
        grid=(1,),
        in_specs=[
            full(*halo.shape),
            full(*normed.shape),
            part(glu_width, 0),
            full(*conv_kernel.shape),
        ],
        out_specs=(full(rows, channels), full(group, 2, rows)),
        scratch=(pltpu.VMEM((8, HALO + rows, channels), F32),),
    )
    stats = swap(stats, TP)
    outer_sent = swap(sent, SP[0])
    head_gain = head_gain.reshape(1, -1)
    head_out = call(
        outer_body,
        shape((rows, HEAD_K), BF16),
        lax.axis_index(SP[0]).reshape(1),
        outer_sent,
        inner_state,
        inner_total,
        normed,
        gathered,
        *kept,
        head_gain,
        grid=(1,),
        in_specs=[
            smem,
            *[full(*a.shape) for a in (outer_sent, inner_state, inner_total, normed)],
            part(2 * HEAD_K, glu_width // (2 * HEAD_K)),
            *[full(*a.shape) for a in kept],
            full(*head_gain.shape),
        ],
        out_specs=full(rows, HEAD_K),
    )
    first = glu_width // HEAD_K + 2
    step = 512
    mixed = call(
        out_body,
        shape((rows, features), BF16),
        stats,
        conv,
        head_out,
        ln_gain.reshape(1, -1),
        ln_bias.reshape(1, -1),
        gathered,
        gathered,
        gathered,
        grid=(features // step,),
        in_specs=[
            full(*stats.shape),
            full(rows, channels),
            full(rows, HEAD_K),
            full(1, channels),
            full(1, channels),
            pl.BlockSpec((step, HEAD_K), lambda k: (k, first)),
            pl.BlockSpec((step, HEAD_K), lambda k: (k, first + 1)),
            pl.BlockSpec((step, HEAD_K), lambda k: (k, first + 2)),
        ],
        out_specs=pl.BlockSpec((rows, step), lambda k: (0, k)),
        scratch=(pltpu.VMEM((rows, channels), BF16),),
    )
    arrived = swap(mixed.reshape(group, share, features), TP)
    return arrived.astype(F32).sum(axis=0).astype(BF16)


def solution(mesh):
    torus = Mesh(mesh.devices.reshape(8, 8, mesh.shape["tp"] // 2, 2), SP_TP)
    placed = (
        P(SP_TP, None),
        P(),
        P(SP, TP),
        P(SP, TP),
        P(SP, TP),
        P(SP, TP),
        P(TP),
        P(SP, TP),
        P(),
        P(SP, TP),
        P(SP, TP),
        P(None, TP),
        P(TP),
        P(TP),
        P(TP, SP),
        P(TP, SP),
    )
    return jax.shard_map(
        on_device, mesh=torus, in_specs=placed, out_specs=P(SP_TP, None), check_vma=False
    )
```

```python
import jax
import jax.numpy as jnp
from jax import lax
from jax.experimental import pallas as pl
from jax.experimental.pallas import tpu as pltpu
from jax.sharding import Mesh
from jax.sharding import PartitionSpec as P

HEAD_K = 128
KERNEL = 31
BLOCK = 64
HALO = 32
SP = ("sp_0", "sp_1")
TP = ("x", "core")
SP_TP = SP + TP
F32 = jnp.float32
BF16 = jnp.bfloat16
EXACT = lax.Precision.HIGHEST
ANY = pl.BlockSpec(memory_space=pl.ANY)


def dot_nt(a, b):
    return lax.dot_general(a, b, (((1,), (1,)), ((), ())), preferred_element_type=F32)


def dot_tn(a, b):
    return lax.dot_general(a, b, (((0,), (0,)), ((), ())), preferred_element_type=F32)


def call(body, outs, *args, grid=None, in_specs=None, out_specs=None, scratch=()):
    specs = {}
    if in_specs is not None:
        specs["in_specs"] = in_specs
    if out_specs is not None:
        specs["out_specs"] = out_specs
    if grid is not None:
        specs["grid"] = grid
    return pl.pallas_call(body, out_shape=outs, scratch_shapes=scratch, **specs)(*args)


def whole(count):
    return [pl.BlockSpec(memory_space=pltpu.VMEM)] * count


def first_body(gv, gg, q, g, wr, wc, copies):
    joined = jnp.concatenate([w[...] for w in (gv, gg, q, g, wr, wc)], axis=1)
    for k in range(copies.shape[0]):
        copies[k] = joined


def second_body(f, v, _, copies):
    joined = jnp.concatenate([f[...], v[...]], axis=1)
    for k in range(copies.shape[0]):
        copies[k] = joined


def again_body(value, copies):
    for k in range(copies.shape[0]):
        copies[k] = value[...]


def norm_body(tokens, gain, out, tail):
    values_in = tokens[...].astype(F32)
    row_scale = lax.rsqrt(jnp.mean(values_in * values_in, axis=1, keepdims=True) + 1e-06)
    scaled = (values_in * row_scale * gain[...]).astype(BF16)
    out[...] = scaled
    tail[...] = scaled[scaled.shape[0] - HALO :]


def pack_state(out, state, total):
    high = total.astype(BF16).astype(F32)
    row = lax.broadcasted_iota(jnp.int32, (8, total.shape[1]), 0)
    tail = jnp.where(row == 0, high, jnp.where(row == 1, total - high, 0.0)).astype(BF16)
    state = state.astype(BF16)
    width = state.shape[0]
    for k in range(out.shape[0]):
        out[k, :width] = state
        out[k, width:] = tail


def causal_mask():
    at_row = lax.broadcasted_iota(jnp.int32, (BLOCK, BLOCK), 0)
    at_col = lax.broadcasted_iota(jnp.int32, (BLOCK, BLOCK), 1)
    return at_row >= at_col


def state_body(normed, weights, leak, shift, sent, value_out, key, totals, starts, befores):
    rows = normed.shape[0]
    peers = weights.shape[0]
    ordered = jnp.concatenate(
        [weights[inner, outer] for outer in range(weights.shape[1]) for inner in range(peers)],
        axis=0,
    )
    projected = jnp.dot(normed[...], ordered, preferred_element_type=F32).astype(BF16)
    value = projected[:, HEAD_K:]
    value_out[...] = value
    in_gate = leak[...] * jax.nn.sigmoid(-projected[:, :HEAD_K].astype(F32))
    log_decay = jnp.log1p(-in_gate) + shift[...]
    triangle = jnp.where(causal_mask(), 1.0, 0.0).astype(F32)
    state = jnp.zeros((HEAD_K, HEAD_K), F32)
    before = jnp.zeros((1, HEAD_K), F32)
    kept = []
    for n in range(rows // BLOCK):
        at = slice(n * BLOCK, (n + 1) * BLOCK)
        total = jnp.dot(triangle, log_decay[at], precision=EXACT, preferred_element_type=F32)
        last = total[BLOCK - 1 :]
        totals[at] = total
        key[at] = (in_gate[at] * jnp.exp(-total)).astype(BF16)
        starts[n] = state.astype(BF16)
        kept.append(before)
        late_key = (in_gate[at] * jnp.exp(last - total)).astype(BF16)
        state = jnp.exp(last) * state + dot_tn(value[at], late_key)
        before = before + last
    befores[...] = jnp.concatenate(kept, axis=0)
    pack_state(sent, state, before)


def unpack(got, k):
    tail = got[k, HEAD_K:].astype(F32)
    return got[k, :HEAD_K].astype(F32), tail[0:1] + tail[1:2]


def gathered_before(got, position):
    state = inside_state = jnp.zeros((HEAD_K, HEAD_K), F32)
    total = inside_total = jnp.zeros((1, HEAD_K), F32)
    for k in range(got.shape[0]):
        passed = k < position
        new_state, new_total = unpack(got, k)
        state = jnp.exp(new_total) * state + new_state
        total = total + new_total
        inside_state = jnp.where(passed, state, inside_state)
        inside_total = jnp.where(passed, total, inside_total)
    return inside_state, inside_total, state, total


def inner_body(position, got, sent, inner_state, inner_total):
    inside_state, inside_total, state, total = gathered_before(got, position[0])
    inner_state[...] = inside_state
    inner_total[...] = jnp.broadcast_to(inside_total, inner_total.shape)
    pack_state(sent, state, total)


def outer_body(
    position,
    got,
    inner_state,
    inner_total,
    normed,
    weights,
    value,
    key,
    totals,
    starts,
    befores,
    gain,
    out,
):
    outside_state = gathered_before(got, position[0])[0]
    incoming = jnp.exp(inner_total[0:1]) * outside_state + inner_state[...]
    projected = jnp.dot(normed[...], weights[...], preferred_element_type=F32)
    projected = projected.astype(BF16).astype(F32)
    queries = jax.nn.silu(projected[:, :HEAD_K])
    gate_act = jax.nn.silu(projected[:, HEAD_K:])
    causal = causal_mask()
    for n in range(starts.shape[0]):
        at = slice(n * BLOCK, (n + 1) * BLOCK)
        query = (queries[at] * jnp.exp(totals[at])).astype(BF16)
        scores = jnp.where(causal, dot_nt(query, key[at]), 0.0).astype(BF16)
        state = jnp.exp(befores[n : n + 1]) * incoming + starts[n].astype(F32)
        recur = jnp.dot(scores, value[at], preferred_element_type=F32)
        recur = recur + dot_nt(query, state.astype(BF16))
        scaling = lax.rsqrt(jnp.mean(recur * recur, axis=1, keepdims=True) + 1e-06)
        out[at] = (recur * scaling * gain[...] * gate_act[at]).astype(BF16)


def conv_body(halo, normed, weights, taps, conv, stats, shifted):
    channels = conv.shape[1]
    rows = conv.shape[0]
    filled = HALO + rows
    extended = jnp.concatenate([halo[...], normed[...]], axis=0)
    projected = jnp.dot(extended, weights[...], preferred_element_type=F32)
    projected = projected.astype(BF16).astype(F32)
    glu = projected[:, :channels] * jax.nn.sigmoid(projected[:, channels:])
    shifted[0, :filled] = glu.astype(BF16).astype(F32)
    for r in range(1, 8):
        shifted[r, : filled - 8] = shifted[0, r : filled - 8 + r]
    first = HALO - (KERNEL - 1)
    step = 32
    for row in range(0, rows, step):
        accum = jnp.zeros((step, channels), F32)
        for tap in range(KERNEL):
            off = row + first + tap
            base = off // 8 * 8
            accum = accum + taps[tap : tap + 1] * shifted[off - base, base : base + step]
        conv[row : row + step] = accum
    summed = conv[...]
    ones = jnp.ones((8, channels), F32)

    def over_channels(value):
        return lax.dot_general(
            ones, value, (((1,), (1,)), ((), ())), precision=EXACT, preferred_element_type=F32
        )

    row = lax.broadcasted_iota(jnp.int32, (8, rows), 0)
    both = jnp.where(row == 0, over_channels(summed), over_channels(summed * summed))[0:2]
    for k in range(stats.shape[0]):
        stats[k] = both


def out_body(stats, conv, head_out, ln_gain, ln_bias, w_rec, w_low, w_high, out):
    channels = conv.shape[1]

    both = stats[0]
    for k in range(1, stats.shape[0]):
        both = both + stats[k]
    both = both / (channels * stats.shape[0])
    mean = both[0:1]
    inverse = lax.rsqrt(both[1:2] - mean * mean + 1e-05)
    row = lax.broadcasted_iota(jnp.int32, (8, both.shape[1]), 0)
    paired = jnp.where(row == 0, mean, jnp.where(row == 1, inverse, 0.0))

    def column(k):
        chosen = jnp.where(lax.broadcasted_iota(jnp.int32, (8, channels), 0) == k, 1.0, 0.0)
        return lax.dot_general(
            paired,
            chosen.astype(F32),
            (((0,), (0,)), ((), ())),
            precision=EXACT,
            preferred_element_type=F32,
        )

    normal = (conv[...] - column(0)) * column(1) * ln_gain[...] + ln_bias[...]
    conv_out = jax.nn.silu(normal).astype(BF16)
    half = channels // 2
    mixed = dot_nt(head_out[...], w_rec[...])
    mixed = mixed + dot_nt(conv_out[:, :half], w_low[...])
    mixed = mixed + dot_nt(conv_out[:, half:], w_high[...])
    out[...] = mixed.astype(BF16)


def swap(value, axis):
    return lax.all_to_all(value, axis, split_axis=0, concat_axis=0, tiled=True)


def on_device(
    tokens,
    norm_gain,
    w_query,
    w_forget,
    w_value,
    w_outgate,
    leak,
    decay_shift,
    head_gain,
    w_glu_value,
    w_glu_gate,
    conv_kernel,
    ln_gain,
    ln_bias,
    w_out_rec,
    w_out_conv,
):
    shape = jax.ShapeDtypeStruct
    smem = pl.BlockSpec(memory_space=pltpu.SMEM)
    inner_count = lax.axis_size(SP[1])
    group = lax.axis_size(TP)
    share, features = tokens.shape
    depth = w_query.shape[0]
    channels = conv_kernel.shape[1]
    columns = (w_glu_value, w_glu_gate, w_query, w_outgate, w_out_rec.T, w_out_conv.T)
    glu_width = 2 * channels
    all_width = sum(w.shape[1] for w in columns)
    outer_count = lax.axis_size(SP[0])
    copies = call(first_body, shape((inner_count, depth, all_width), BF16), *columns)
    block = lax.all_gather(tokens, TP, axis=0, tiled=True)
    staged = swap(copies, SP[1]).reshape(inner_count * depth, all_width)
    gathered = lax.all_gather(staged, SP[0], axis=0, tiled=True)
    copies = call(
        second_body,
        shape((outer_count, depth, 2 * HEAD_K), BF16),
        w_forget,
        w_value,
        staged,
        in_specs=whole(2) + [ANY],
    )
    column = swap(copies, SP[0]).reshape(outer_count * depth, 2 * HEAD_K)
    copies = call(again_body, shape((inner_count, *column.shape), BF16), column)
    state_weights = swap(copies, SP[1]).reshape(inner_count, outer_count, depth, 2 * HEAD_K)
    rows = group * share
    normed, tail = call(
        norm_body,
        (shape((rows, features), BF16), shape((share, features), BF16)),
        block,
        norm_gain.reshape(1, -1),
    )
    count = lax.axis_size(SP)
    halo = lax.ppermute(tail, SP, [(k, k + 1) for k in range(count - 1)])
    message = shape((inner_count, HEAD_K + 8, HEAD_K), BF16)
    blocks = rows // BLOCK
    sent, *kept = call(
        state_body,
        (
            message,
            shape((rows, HEAD_K), BF16),
            shape((rows, HEAD_K), BF16),
            shape((rows, HEAD_K), F32),
            shape((blocks, HEAD_K, HEAD_K), BF16),
            shape((blocks, HEAD_K), F32),
        ),
        normed,
        state_weights,
        leak.reshape(1, -1),
        decay_shift,
    )
    sent, inner_state, inner_total = call(
        inner_body,
        (message, shape((HEAD_K, HEAD_K), F32), shape((8, HEAD_K), F32)),
        lax.axis_index(SP[1]).reshape(1),
        swap(sent, SP[1]),
        in_specs=[smem] + whole(1),
    )

    def part(size, at):
        return pl.BlockSpec((gathered.shape[0], size), lambda k: (0, at))

    def full(*lengths):
        return pl.BlockSpec(lengths, lambda k: (0,) * len(lengths))

    conv, stats = call(
        conv_body,
        (shape((rows, channels), F32), shape((group, 2, rows), F32)),
        halo,
        normed,
        gathered,
        conv_kernel,
        grid=(1,),
        in_specs=[
            full(*halo.shape),
            full(*normed.shape),
            part(glu_width, 0),
            full(*conv_kernel.shape),
        ],
        out_specs=(full(rows, channels), full(group, 2, rows)),
        scratch=(pltpu.VMEM((8, HALO + rows, channels), F32),),
    )
    stats = swap(stats, TP)
    outer_sent = swap(sent, SP[0])
    head_gain = head_gain.reshape(1, -1)
    head_out = call(
        outer_body,
        shape((rows, HEAD_K), BF16),
        lax.axis_index(SP[0]).reshape(1),
        outer_sent,
        inner_state,
        inner_total,
        normed,
        gathered,
        *kept,
        head_gain,
        grid=(1,),
        in_specs=[
            smem,
            *[full(*a.shape) for a in (outer_sent, inner_state, inner_total, normed)],
            part(2 * HEAD_K, glu_width // (2 * HEAD_K)),
            *[full(*a.shape) for a in kept],
            full(*head_gain.shape),
        ],
        out_specs=full(rows, HEAD_K),
    )
    first = glu_width // HEAD_K + 2
    step = features
    mixed = call(
        out_body,
        shape((rows, features), BF16),
        stats,
        conv,
        head_out,
        ln_gain.reshape(1, -1),
        ln_bias.reshape(1, -1),
        gathered,
        gathered,
        gathered,
        grid=(features // step,),
        in_specs=[
            full(*stats.shape),
            full(rows, channels),
            full(rows, HEAD_K),
            full(1, channels),
            full(1, channels),
            pl.BlockSpec((step, HEAD_K), lambda k: (k, first)),
            pl.BlockSpec((step, HEAD_K), lambda k: (k, first + 1)),
            pl.BlockSpec((step, HEAD_K), lambda k: (k, first + 2)),
        ],
        out_specs=pl.BlockSpec((rows, step), lambda k: (0, k)),
    )
    arrived = swap(mixed.reshape(group, share, features), TP)
    return arrived.astype(F32).sum(axis=0).astype(BF16)


def solution(mesh):
    torus = Mesh(mesh.devices.reshape(8, 8, mesh.shape["tp"] // 2, 2), SP_TP)
    placed = (
        P(SP_TP, None),
        P(),
        P(SP, TP),
        P(SP, TP),
        P(SP, TP),
        P(SP, TP),
        P(TP),
        P(SP, TP),
        P(),
        P(SP, TP),
        P(SP, TP),
        P(None, TP),
        P(TP),
        P(TP),
        P(TP, SP),
        P(TP, SP),
    )
    return jax.shard_map(
        on_device, mesh=torus, in_specs=placed, out_specs=P(SP_TP, None), check_vma=False
    )
```

```python
import jax
import jax.numpy as jnp
from jax import lax
from jax.experimental import pallas as pl
from jax.experimental.pallas import tpu as pltpu
from jax.sharding import Mesh
from jax.sharding import PartitionSpec as P

HEAD_K = 128
KERNEL = 31
BLOCK = 64
HALO = 32
SP = ("sp_0", "sp_1")
TP = ("x", "core")
SP_TP = SP + TP
F32 = jnp.float32
BF16 = jnp.bfloat16
EXACT = lax.Precision.HIGHEST
ANY = pl.BlockSpec(memory_space=pl.ANY)


def dot_nt(a, b):
    return lax.dot_general(a, b, (((1,), (1,)), ((), ())), preferred_element_type=F32)


def dot_tn(a, b):
    return lax.dot_general(a, b, (((0,), (0,)), ((), ())), preferred_element_type=F32)


def call(body, outs, *args, grid=None, in_specs=None, out_specs=None, scratch=()):
    specs = {}
    if in_specs is not None:
        specs["in_specs"] = in_specs
    if out_specs is not None:
        specs["out_specs"] = out_specs
    if grid is not None:
        specs["grid"] = grid
    return pl.pallas_call(body, out_shape=outs, scratch_shapes=scratch, **specs)(*args)


def whole(count):
    return [pl.BlockSpec(memory_space=pltpu.VMEM)] * count


def first_body(f, v, copies):
    joined = jnp.concatenate([f[...], v[...]], axis=1)
    for k in range(copies.shape[0]):
        copies[k] = joined


def second_body(gv, gg, q, g, wr, wc, _, copies):
    joined = jnp.concatenate([w[...] for w in (gv, gg, q, g, wr, wc)], axis=1)
    for k in range(copies.shape[0]):
        copies[k] = joined


def again_body(value, _, copies):
    for k in range(copies.shape[0]):
        copies[k] = value[...]


def norm_body(tokens, gain, out, tail):
    values_in = tokens[...].astype(F32)
    row_scale = lax.rsqrt(jnp.mean(values_in * values_in, axis=1, keepdims=True) + 1e-06)
    scaled = (values_in * row_scale * gain[...]).astype(BF16)
    out[...] = scaled
    tail[...] = scaled[scaled.shape[0] - HALO :]


def pack_state(out, state, total):
    high = total.astype(BF16).astype(F32)
    row = lax.broadcasted_iota(jnp.int32, (8, total.shape[1]), 0)
    tail = jnp.where(row == 0, high, jnp.where(row == 1, total - high, 0.0)).astype(BF16)
    state = state.astype(BF16)
    width = state.shape[0]
    for k in range(out.shape[0]):
        out[k, :width] = state
        out[k, width:] = tail


def causal_mask():
    at_row = lax.broadcasted_iota(jnp.int32, (BLOCK, BLOCK), 0)
    at_col = lax.broadcasted_iota(jnp.int32, (BLOCK, BLOCK), 1)
    return at_row >= at_col


def state_body(normed, weights, leak, shift, sent, value_out, key, totals, starts, befores):
    rows = normed.shape[0]
    peers = weights.shape[0]
    ordered = jnp.concatenate(
        [weights[inner, outer] for outer in range(weights.shape[1]) for inner in range(peers)],
        axis=0,
    )
    projected = jnp.dot(normed[...], ordered, preferred_element_type=F32).astype(BF16)
    value = projected[:, HEAD_K:]
    value_out[...] = value
    in_gate = leak[...] * jax.nn.sigmoid(-projected[:, :HEAD_K].astype(F32))
    log_decay = jnp.log1p(-in_gate) + shift[...]
    triangle = jnp.where(causal_mask(), 1.0, 0.0).astype(F32)
    state = jnp.zeros((HEAD_K, HEAD_K), F32)
    before = jnp.zeros((1, HEAD_K), F32)
    kept = []
    for n in range(rows // BLOCK):
        at = slice(n * BLOCK, (n + 1) * BLOCK)
        total = jnp.dot(triangle, log_decay[at], precision=EXACT, preferred_element_type=F32)
        last = total[BLOCK - 1 :]
        totals[at] = total
        key[at] = (in_gate[at] * jnp.exp(-total)).astype(BF16)
        starts[n] = state.astype(BF16)
        kept.append(before)
        late_key = (in_gate[at] * jnp.exp(last - total)).astype(BF16)
        state = jnp.exp(last) * state + dot_tn(value[at], late_key)
        before = before + last
    befores[...] = jnp.concatenate(kept, axis=0)
    pack_state(sent, state, before)


def unpack(got, k):
    tail = got[k, HEAD_K:].astype(F32)
    return got[k, :HEAD_K].astype(F32), tail[0:1] + tail[1:2]


def gathered_before(got, position):
    state = inside_state = jnp.zeros((HEAD_K, HEAD_K), F32)
    total = inside_total = jnp.zeros((1, HEAD_K), F32)
    for k in range(got.shape[0]):
        passed = k < position
        new_state, new_total = unpack(got, k)
        state = jnp.exp(new_total) * state + new_state
        total = total + new_total
        inside_state = jnp.where(passed, state, inside_state)
        inside_total = jnp.where(passed, total, inside_total)
    return inside_state, inside_total, state, total


def inner_body(position, got, sent, inner_state, inner_total):
    inside_state, inside_total, state, total = gathered_before(got, position[0])
    inner_state[...] = inside_state
    inner_total[...] = jnp.broadcast_to(inside_total, inner_total.shape)
    pack_state(sent, state, total)


def outer_body(
    position,
    got,
    inner_state,
    inner_total,
    normed,
    weights,
    value,
    key,
    totals,
    starts,
    befores,
    gain,
    out,
):
    outside_state = gathered_before(got, position[0])[0]
    incoming = jnp.exp(inner_total[0:1]) * outside_state + inner_state[...]
    projected = jnp.dot(normed[...], weights[...], preferred_element_type=F32)
    projected = projected.astype(BF16).astype(F32)
    queries = jax.nn.silu(projected[:, :HEAD_K])
    gate_act = jax.nn.silu(projected[:, HEAD_K:])
    causal = causal_mask()
    for n in range(starts.shape[0]):
        at = slice(n * BLOCK, (n + 1) * BLOCK)
        query = (queries[at] * jnp.exp(totals[at])).astype(BF16)
        scores = jnp.where(causal, dot_nt(query, key[at]), 0.0).astype(BF16)
        state = jnp.exp(befores[n : n + 1]) * incoming + starts[n].astype(F32)
        recur = jnp.dot(scores, value[at], preferred_element_type=F32)
        recur = recur + dot_nt(query, state.astype(BF16))
        scaling = lax.rsqrt(jnp.mean(recur * recur, axis=1, keepdims=True) + 1e-06)
        out[at] = (recur * scaling * gain[...] * gate_act[at]).astype(BF16)


def conv_body(halo, normed, weights, taps, conv, stats, shifted):
    channels = conv.shape[1]
    rows = conv.shape[0]
    filled = HALO + rows
    extended = jnp.concatenate([halo[...], normed[...]], axis=0)
    projected = jnp.dot(extended, weights[...], preferred_element_type=F32)
    projected = projected.astype(BF16).astype(F32)
    glu = projected[:, :channels] * jax.nn.sigmoid(projected[:, channels:])
    shifted[0, :filled] = glu.astype(BF16).astype(F32)
    for r in range(1, 8):
        shifted[r, : filled - 8] = shifted[0, r : filled - 8 + r]
    first = HALO - (KERNEL - 1)
    step = 32
    for row in range(0, rows, step):
        accum = jnp.zeros((step, channels), F32)
        for tap in range(KERNEL):
            off = row + first + tap
            base = off // 8 * 8
            accum = accum + taps[tap : tap + 1] * shifted[off - base, base : base + step]
        conv[row : row + step] = accum
    summed = conv[...]
    ones = jnp.ones((8, channels), F32)

    def over_channels(value):
        return lax.dot_general(
            ones, value, (((1,), (1,)), ((), ())), precision=EXACT, preferred_element_type=F32
        )

    row = lax.broadcasted_iota(jnp.int32, (8, rows), 0)
    both = jnp.where(row == 0, over_channels(summed), over_channels(summed * summed))[0:2]
    for k in range(stats.shape[0]):
        stats[k] = both


def out_body(core, stats, conv, head_out, ln_gain, ln_bias, w_rec, w_low, w_high, rows_out, out):
    channels = conv.shape[1]
    share = conv.shape[0] // stats.shape[0]
    both = stats[0]
    for k in range(1, stats.shape[0]):
        both = both + stats[k]
    both = both / (channels * stats.shape[0])
    mean = both[0:1]
    inverse = lax.rsqrt(both[1:2] - mean * mean + 1e-05)
    row = lax.broadcasted_iota(jnp.int32, (8, both.shape[1]), 0)
    paired = jnp.where(row == 0, mean, jnp.where(row == 1, inverse, 0.0))

    def column(k):
        chosen = jnp.where(lax.broadcasted_iota(jnp.int32, (8, channels), 0) == k, 1.0, 0.0)
        return lax.dot_general(
            paired,
            chosen.astype(F32),
            (((0,), (0,)), ((), ())),
            precision=EXACT,
            preferred_element_type=F32,
        )

    normal = (conv[...] - column(0)) * column(1) * ln_gain[...] + ln_bias[...]
    conv_out = jax.nn.silu(normal).astype(BF16)
    for k in range(stats.shape[0]):
        piece = slice(k * share, (k + 1) * share)
        at = slice(k // 2 * share, (k // 2 + 1) * share)
        rows_out[k % 2, at, :HEAD_K] = head_out[piece]
        rows_out[k % 2, at, HEAD_K:] = conv_out[piece]
    out[...] = product(rows_out[1 - core[0]], w_rec, w_low, w_high)


def product(rows, w_rec, w_low, w_high):
    mixed = dot_nt(rows[:, :HEAD_K], w_rec[...])
    mixed = mixed + dot_nt(rows[:, HEAD_K : 2 * HEAD_K], w_low[...])
    mixed = mixed + dot_nt(rows[:, 2 * HEAD_K :], w_high[...])
    return mixed.astype(BF16)


def own_body(core, rows, w_rec, w_low, w_high, out):
    out[...] = product(rows[core[0]], w_rec, w_low, w_high)


def swap(value, axis):
    return lax.all_to_all(value, axis, split_axis=0, concat_axis=0, tiled=True)


def on_device(
    tokens,
    norm_gain,
    w_query,
    w_forget,
    w_value,
    w_outgate,
    leak,
    decay_shift,
    head_gain,
    w_glu_value,
    w_glu_gate,
    conv_kernel,
    ln_gain,
    ln_bias,
    w_out_rec,
    w_out_conv,
):
    shape = jax.ShapeDtypeStruct
    smem = pl.BlockSpec(memory_space=pltpu.SMEM)
    inner_count = lax.axis_size(SP[1])
    group = lax.axis_size(TP)
    share, features = tokens.shape
    depth = w_query.shape[0]
    channels = conv_kernel.shape[1]
    columns = (w_glu_value, w_glu_gate, w_query, w_outgate, w_out_rec.T, w_out_conv.T)
    glu_width = 2 * channels
    all_width = sum(w.shape[1] for w in columns)
    outer_count = lax.axis_size(SP[0])
    copies = call(
        first_body, shape((outer_count, depth, 2 * HEAD_K), BF16), w_forget, w_value
    )
    block = lax.all_gather(tokens, TP, axis=0, tiled=True)
    column = swap(copies, SP[0]).reshape(outer_count * depth, 2 * HEAD_K)
    copies = call(
        second_body,
        shape((inner_count, depth, all_width), BF16),
        *columns,
        column,
        in_specs=whole(len(columns)) + [ANY],
    )
    staged = swap(copies, SP[1]).reshape(inner_count * depth, all_width)
    gathered = lax.all_gather(staged, SP[0], axis=0, tiled=True)
    copies = call(
        again_body,
        shape((inner_count, *column.shape), BF16),
        column,
        staged,
        in_specs=whole(1) + [ANY],
    )
    state_weights = swap(copies, SP[1]).reshape(inner_count, outer_count, depth, 2 * HEAD_K)
    rows = group * share
    normed, tail = call(
        norm_body,
        (shape((rows, features), BF16), shape((share, features), BF16)),
        block,
        norm_gain.reshape(1, -1),
    )
    count = lax.axis_size(SP)
    halo = lax.ppermute(tail, SP, [(k, k + 1) for k in range(count - 1)])
    message = shape((inner_count, HEAD_K + 8, HEAD_K), BF16)
    blocks = rows // BLOCK
    sent, *kept = call(
        state_body,
        (
            message,
            shape((rows, HEAD_K), BF16),
            shape((rows, HEAD_K), BF16),
            shape((rows, HEAD_K), F32),
            shape((blocks, HEAD_K, HEAD_K), BF16),
            shape((blocks, HEAD_K), F32),
        ),
        normed,
        state_weights,
        leak.reshape(1, -1),
        decay_shift,
    )
    sent, inner_state, inner_total = call(
        inner_body,
        (message, shape((HEAD_K, HEAD_K), F32), shape((8, HEAD_K), F32)),
        lax.axis_index(SP[1]).reshape(1),
        swap(sent, SP[1]),
        in_specs=[smem] + whole(1),
    )

    def part(size, at):
        return pl.BlockSpec((gathered.shape[0], size), lambda k: (0, at))

    def full(*lengths):
        return pl.BlockSpec(lengths, lambda k: (0,) * len(lengths))

    conv, stats = call(
        conv_body,
        (shape((rows, channels), F32), shape((group, 2, rows), F32)),
        halo,
        normed,
        gathered,
        conv_kernel,
        grid=(1,),
        in_specs=[
            full(*halo.shape),
            full(*normed.shape),
            part(glu_width, 0),
            full(*conv_kernel.shape),
        ],
        out_specs=(full(rows, channels), full(group, 2, rows)),
        scratch=(pltpu.VMEM((8, HALO + rows, channels), F32),),
    )
    stats = swap(stats, TP)
    outer_sent = swap(sent, SP[0])
    head_gain = head_gain.reshape(1, -1)
    head_out = call(
        outer_body,
        shape((rows, HEAD_K), BF16),
        lax.axis_index(SP[0]).reshape(1),
        outer_sent,
        inner_state,
        inner_total,
        normed,
        gathered,
        *kept,
        head_gain,
        grid=(1,),
        in_specs=[
            smem,
            *[full(*a.shape) for a in (outer_sent, inner_state, inner_total, normed)],
            part(2 * HEAD_K, glu_width // (2 * HEAD_K)),
            *[full(*a.shape) for a in kept],
            full(*head_gain.shape),
        ],
        out_specs=full(rows, HEAD_K),
    )
    first = glu_width // HEAD_K + 2
    half = rows // 2
    width = HEAD_K + channels
    core = lax.axis_index(TP[1]).reshape(1)
    weights = [gathered] * 3
    weight_specs = [part(HEAD_K, first + k) for k in range(3)]
    mixed_rows, sent = call(
        out_body,
        (shape((2, half, width), BF16), shape((half, features), BF16)),
        core,
        stats,
        conv,
        head_out,
        ln_gain.reshape(1, -1),
        ln_bias.reshape(1, -1),
        *weights,
        grid=(1,),
        in_specs=[
            smem,
            full(*stats.shape),
            full(rows, channels),
            full(rows, HEAD_K),
            full(1, channels),
            full(1, channels),
            *weight_specs,
        ],
        out_specs=(full(2, half, width), full(half, features)),
    )
    received = lax.ppermute(sent, TP[1], [(0, 1), (1, 0)])
    own = call(
        own_body,
        shape((half, features), BF16),
        core,
        mixed_rows,
        *weights,
        grid=(1,),
        in_specs=[smem, full(2, half, width), *weight_specs],
        out_specs=full(half, features),
    )
    pair = (own.astype(F32) + received.astype(F32)).astype(BF16)
    arrived = swap(pair.reshape(group // 2, share, features), TP[0])
    return arrived.astype(F32).sum(axis=0).astype(BF16)


def solution(mesh):
    torus = Mesh(mesh.devices.reshape(8, 8, mesh.shape["tp"] // 2, 2), SP_TP)
    placed = (
        P(SP_TP, None),
        P(),
        P(SP, TP),
        P(SP, TP),
        P(SP, TP),
        P(SP, TP),
        P(TP),
        P(SP, TP),
        P(),
        P(SP, TP),
        P(SP, TP),
        P(None, TP),
        P(TP),
        P(TP),
        P(TP, SP),
        P(TP, SP),
    )
    return jax.shard_map(
        on_device, mesh=torus, in_specs=placed, out_specs=P(SP_TP, None), check_vma=False
    )
```

```python
import jax
import jax.numpy as jnp
from jax import lax
from jax.experimental import pallas as pl
from jax.experimental.pallas import tpu as pltpu
from jax.sharding import Mesh
from jax.sharding import PartitionSpec as P

HEAD_K = 128
KERNEL = 31
BLOCK = 64
HALO = 32
SP = ("sp_0", "sp_1")
TP = ("x", "core")
SP_TP = SP + TP
F32 = jnp.float32
BF16 = jnp.bfloat16
EXACT = lax.Precision.HIGHEST


def dot_nt(a, b):
    return lax.dot_general(a, b, (((1,), (1,)), ((), ())), preferred_element_type=F32)


def dot_tn(a, b):
    return lax.dot_general(a, b, (((0,), (0,)), ((), ())), preferred_element_type=F32)


def call(body, outs, *args, grid=None, in_specs=None, out_specs=None, scratch=()):
    specs = {}
    if in_specs is not None:
        specs["in_specs"] = in_specs
    if out_specs is not None:
        specs["out_specs"] = out_specs
    if grid is not None:
        specs["grid"] = grid
    return pl.pallas_call(body, out_shape=outs, scratch_shapes=scratch, **specs)(*args)


def whole(count):
    return [pl.BlockSpec(memory_space=pltpu.VMEM)] * count


def first_body(gv, gg, q, g, wr, wc, f, v, copies, joined):
    together = jnp.concatenate([w[...] for w in (gv, gg, q, g, wr, wc)], axis=1)
    for k in range(copies.shape[0]):
        copies[k] = together
    joined[...] = jnp.concatenate([f[...], v[...]], axis=1)


def again_body(places, *refs):
    *pieces, copies = refs
    for n, piece in enumerate(pieces):
        value = piece[...]
        for k in range(copies.shape[0]):
            copies[k, places[n]] = value


def norm_body(places, gain, *refs):
    *pieces, out, tail = refs
    share = tail.shape[0]
    for n, piece in enumerate(pieces):
        values_in = piece[...].astype(F32)
        row_scale = lax.rsqrt(jnp.mean(values_in * values_in, axis=1, keepdims=True) + 1e-06)
        scaled = (values_in * row_scale * gain[...]).astype(BF16)
        out[pl.ds(pl.multiple_of(places[n] * share, share), share)] = scaled
    tail[...] = out[out.shape[0] - share :]


def pack_state(out, state, total):
    high = total.astype(BF16).astype(F32)
    row = lax.broadcasted_iota(jnp.int32, (8, total.shape[1]), 0)
    tail = jnp.where(row == 0, high, jnp.where(row == 1, total - high, 0.0)).astype(BF16)
    state = state.astype(BF16)
    width = state.shape[0]
    for k in range(out.shape[0]):
        out[k, :width] = state
        out[k, width:] = tail


def causal_mask():
    at_row = lax.broadcasted_iota(jnp.int32, (BLOCK, BLOCK), 0)
    at_col = lax.broadcasted_iota(jnp.int32, (BLOCK, BLOCK), 1)
    return at_row >= at_col


def state_body(normed, weights, leak, shift, sent, value_out, key, totals, starts, befores):
    rows = normed.shape[0]
    peers = weights.shape[0]
    ordered = jnp.concatenate(
        [weights[inner, outer] for outer in range(weights.shape[1]) for inner in range(peers)],
        axis=0,
    )
    projected = jnp.dot(normed[...], ordered, preferred_element_type=F32).astype(BF16)
    value = projected[:, HEAD_K:]
    value_out[...] = value
    in_gate = leak[...] * jax.nn.sigmoid(-projected[:, :HEAD_K].astype(F32))
    log_decay = jnp.log1p(-in_gate) + shift[...]
    triangle = jnp.where(causal_mask(), 1.0, 0.0).astype(F32)
    state = jnp.zeros((HEAD_K, HEAD_K), F32)
    before = jnp.zeros((1, HEAD_K), F32)
    kept = []
    for n in range(rows // BLOCK):
        at = slice(n * BLOCK, (n + 1) * BLOCK)
        total = jnp.dot(triangle, log_decay[at], precision=EXACT, preferred_element_type=F32)
        last = total[BLOCK - 1 :]
        totals[at] = total
        key[at] = (in_gate[at] * jnp.exp(-total)).astype(BF16)
        starts[n] = state.astype(BF16)
        kept.append(before)
        late_key = (in_gate[at] * jnp.exp(last - total)).astype(BF16)
        state = jnp.exp(last) * state + dot_tn(value[at], late_key)
        before = before + last
    befores[...] = jnp.concatenate(kept, axis=0)
    pack_state(sent, state, before)


def unpack(got, k):
    tail = got[k, HEAD_K:].astype(F32)
    return got[k, :HEAD_K].astype(F32), tail[0:1] + tail[1:2]


def gathered_before(got, position):
    state = inside_state = jnp.zeros((HEAD_K, HEAD_K), F32)
    total = inside_total = jnp.zeros((1, HEAD_K), F32)
    for k in range(got.shape[0]):
        passed = k < position
        new_state, new_total = unpack(got, k)
        state = jnp.exp(new_total) * state + new_state
        total = total + new_total
        inside_state = jnp.where(passed, state, inside_state)
        inside_total = jnp.where(passed, total, inside_total)
    return inside_state, inside_total, state, total


def inner_body(position, got, sent, inner_state, inner_total):
    inside_state, inside_total, state, total = gathered_before(got, position[0])
    inner_state[...] = inside_state
    inner_total[...] = jnp.broadcast_to(inside_total, inner_total.shape)
    pack_state(sent, state, total)


def outer_body(
    position,
    got,
    inner_state,
    inner_total,
    normed,
    weights,
    value,
    key,
    totals,
    starts,
    befores,
    gain,
    out,
):
    outside_state = gathered_before(got, position[0])[0]
    incoming = jnp.exp(inner_total[0:1]) * outside_state + inner_state[...]
    projected = jnp.dot(normed[...], weights[...], preferred_element_type=F32)
    projected = projected.astype(BF16).astype(F32)
    queries = jax.nn.silu(projected[:, :HEAD_K])
    gate_act = jax.nn.silu(projected[:, HEAD_K:])
    causal = causal_mask()
    for n in range(starts.shape[0]):
        at = slice(n * BLOCK, (n + 1) * BLOCK)
        query = (queries[at] * jnp.exp(totals[at])).astype(BF16)
        scores = jnp.where(causal, dot_nt(query, key[at]), 0.0).astype(BF16)
        state = jnp.exp(befores[n : n + 1]) * incoming + starts[n].astype(F32)
        recur = jnp.dot(scores, value[at], preferred_element_type=F32)
        recur = recur + dot_nt(query, state.astype(BF16))
        scaling = lax.rsqrt(jnp.mean(recur * recur, axis=1, keepdims=True) + 1e-06)
        out[at] = (recur * scaling * gain[...] * gate_act[at]).astype(BF16)


def conv_body(halo, normed, weights, taps, conv, stats, shifted):
    channels = conv.shape[1]
    rows = conv.shape[0]
    filled = HALO + rows
    extended = jnp.concatenate([halo[...], normed[...]], axis=0)
    projected = jnp.dot(extended, weights[...], preferred_element_type=F32)
    projected = projected.astype(BF16).astype(F32)
    glu = projected[:, :channels] * jax.nn.sigmoid(projected[:, channels:])
    shifted[0, :filled] = glu.astype(BF16).astype(F32)
    for r in range(1, 8):
        shifted[r, : filled - 8] = shifted[0, r : filled - 8 + r]
    first = HALO - (KERNEL - 1)
    step = 32
    for row in range(0, rows, step):
        accum = jnp.zeros((step, channels), F32)
        for tap in range(KERNEL):
            off = row + first + tap
            base = off // 8 * 8
            accum = accum + taps[tap : tap + 1] * shifted[off - base, base : base + step]
        conv[row : row + step] = accum
    summed = conv[...]
    ones = jnp.ones((8, channels), F32)

    def over_channels(value):
        return lax.dot_general(
            ones, value, (((1,), (1,)), ((), ())), precision=EXACT, preferred_element_type=F32
        )

    row = lax.broadcasted_iota(jnp.int32, (8, rows), 0)
    both = jnp.where(row == 0, over_channels(summed), over_channels(summed * summed))[0:2]
    for k in range(stats.shape[0]):
        stats[k] = both


def out_body(core, stats, conv, head_out, ln_gain, ln_bias, w_rec, w_low, w_high, rows_out, out):
    channels = conv.shape[1]
    share = conv.shape[0] // stats.shape[0]
    both = stats[0]
    for k in range(1, stats.shape[0]):
        both = both + stats[k]
    both = both / (channels * stats.shape[0])
    mean = both[0:1]
    inverse = lax.rsqrt(both[1:2] - mean * mean + 1e-05)
    row = lax.broadcasted_iota(jnp.int32, (8, both.shape[1]), 0)
    paired = jnp.where(row == 0, mean, jnp.where(row == 1, inverse, 0.0))

    def column(k):
        chosen = jnp.where(lax.broadcasted_iota(jnp.int32, (8, channels), 0) == k, 1.0, 0.0)
        return lax.dot_general(
            paired,
            chosen.astype(F32),
            (((0,), (0,)), ((), ())),
            precision=EXACT,
            preferred_element_type=F32,
        )

    normal = (conv[...] - column(0)) * column(1) * ln_gain[...] + ln_bias[...]
    conv_out = jax.nn.silu(normal).astype(BF16)
    for k in range(stats.shape[0]):
        piece = slice(k * share, (k + 1) * share)
        at = slice(k // 2 * share, (k // 2 + 1) * share)
        rows_out[k % 2, at, :HEAD_K] = head_out[piece]
        rows_out[k % 2, at, HEAD_K:] = conv_out[piece]
    out[...] = product(rows_out[1 - core[0]], w_rec, w_low, w_high)


def product(rows, w_rec, w_low, w_high):
    mixed = dot_nt(rows[:, :HEAD_K], w_rec[...])
    mixed = mixed + dot_nt(rows[:, HEAD_K : 2 * HEAD_K], w_low[...])
    mixed = mixed + dot_nt(rows[:, 2 * HEAD_K :], w_high[...])
    return mixed.astype(BF16)


def own_body(core, rows, w_rec, w_low, w_high, out):
    out[...] = product(rows[core[0]], w_rec, w_low, w_high)


def swap(value, axis):
    return lax.all_to_all(value, axis, split_axis=0, concat_axis=0, tiled=True)


def shifted_around(value, axis):
    count = lax.axis_size(axis)
    pieces = [value]
    for k in range(1, count):
        pieces.append(lax.ppermute(value, axis, [(n, (n + k) % count) for n in range(count)]))
    return pieces, (lax.axis_index(axis) + count - jnp.arange(count, dtype=jnp.int32)) % count


def on_device(
    tokens,
    norm_gain,
    w_query,
    w_forget,
    w_value,
    w_outgate,
    leak,
    decay_shift,
    head_gain,
    w_glu_value,
    w_glu_gate,
    conv_kernel,
    ln_gain,
    ln_bias,
    w_out_rec,
    w_out_conv,
):
    shape = jax.ShapeDtypeStruct
    smem = pl.BlockSpec(memory_space=pltpu.SMEM)
    inner_count = lax.axis_size(SP[1])
    group = lax.axis_size(TP)
    share, features = tokens.shape
    depth = w_query.shape[0]
    channels = conv_kernel.shape[1]
    columns = (w_glu_value, w_glu_gate, w_query, w_outgate, w_out_rec.T, w_out_conv.T)
    glu_width = 2 * channels
    all_width = sum(w.shape[1] for w in columns)
    outer_count = lax.axis_size(SP[0])
    copies, joined = call(
        first_body,
        (
            shape((inner_count, depth, all_width), BF16),
            shape((depth, 2 * HEAD_K), BF16),
        ),
        *columns,
        w_forget,
        w_value,
    )
    staged = swap(copies, SP[1]).reshape(inner_count * depth, all_width)
    gathered = lax.all_gather(staged, SP[0], axis=0, tiled=True)
    pieces, places = shifted_around(joined, SP[0])
    copies = call(
        again_body,
        shape((inner_count, outer_count, depth, 2 * HEAD_K), BF16),
        places,
        *pieces,
        in_specs=[smem] + whole(len(pieces)),
    )
    state_weights = swap(copies, SP[1])
    pieces, places = shifted_around(tokens, TP)
    rows = group * share
    normed, tail = call(
        norm_body,
        (shape((rows, features), BF16), shape((share, features), BF16)),
        places,
        norm_gain.reshape(1, -1),
        *pieces,
        in_specs=[smem] + whole(1 + len(pieces)),
    )
    count = lax.axis_size(SP)
    halo = lax.ppermute(tail, SP, [(k, k + 1) for k in range(count - 1)])
    message = shape((inner_count, HEAD_K + 8, HEAD_K), BF16)
    blocks = rows // BLOCK
    sent, *kept = call(
        state_body,
        (
            message,
            shape((rows, HEAD_K), BF16),
            shape((rows, HEAD_K), BF16),
            shape((rows, HEAD_K), F32),
            shape((blocks, HEAD_K, HEAD_K), BF16),
            shape((blocks, HEAD_K), F32),
        ),
        normed,
        state_weights,
        leak.reshape(1, -1),
        decay_shift,
    )
    sent, inner_state, inner_total = call(
        inner_body,
        (message, shape((HEAD_K, HEAD_K), F32), shape((8, HEAD_K), F32)),
        lax.axis_index(SP[1]).reshape(1),
        swap(sent, SP[1]),
        in_specs=[smem] + whole(1),
    )

    def part(size, at):
        return pl.BlockSpec((gathered.shape[0], size), lambda k: (0, at))

    def full(*lengths):
        return pl.BlockSpec(lengths, lambda k: (0,) * len(lengths))

    conv, stats = call(
        conv_body,
        (shape((rows, channels), F32), shape((group, 2, rows), F32)),
        halo,
        normed,
        gathered,
        conv_kernel,
        grid=(1,),
        in_specs=[
            full(*halo.shape),
            full(*normed.shape),
            part(glu_width, 0),
            full(*conv_kernel.shape),
        ],
        out_specs=(full(rows, channels), full(group, 2, rows)),
        scratch=(pltpu.VMEM((8, HALO + rows, channels), F32),),
    )
    stats = swap(stats, TP)
    outer_sent = swap(sent, SP[0])
    head_gain = head_gain.reshape(1, -1)
    head_out = call(
        outer_body,
        shape((rows, HEAD_K), BF16),
        lax.axis_index(SP[0]).reshape(1),
        outer_sent,
        inner_state,
        inner_total,
        normed,
        gathered,
        *kept,
        head_gain,
        grid=(1,),
        in_specs=[
            smem,
            *[full(*a.shape) for a in (outer_sent, inner_state, inner_total, normed)],
            part(2 * HEAD_K, glu_width // (2 * HEAD_K)),
            *[full(*a.shape) for a in kept],
            full(*head_gain.shape),
        ],
        out_specs=full(rows, HEAD_K),
    )
    first = glu_width // HEAD_K + 2
    half = rows // 2
    width = HEAD_K + channels
    core = lax.axis_index(TP[1]).reshape(1)
    weights = [gathered] * 3
    weight_specs = [part(HEAD_K, first + k) for k in range(3)]
    mixed_rows, sent = call(
        out_body,
        (shape((2, half, width), BF16), shape((half, features), BF16)),
        core,
        stats,
        conv,
        head_out,
        ln_gain.reshape(1, -1),
        ln_bias.reshape(1, -1),
        *weights,
        grid=(1,),
        in_specs=[
            smem,
            full(*stats.shape),
            full(rows, channels),
            full(rows, HEAD_K),
            full(1, channels),
            full(1, channels),
            *weight_specs,
        ],
        out_specs=(full(2, half, width), full(half, features)),
    )
    received = lax.ppermute(sent, TP[1], [(0, 1), (1, 0)])
    own = call(
        own_body,
        shape((half, features), BF16),
        core,
        mixed_rows,
        *weights,
        grid=(1,),
        in_specs=[smem, full(2, half, width), *weight_specs],
        out_specs=full(half, features),
    )
    pair = (own.astype(F32) + received.astype(F32)).astype(BF16)
    arrived = swap(pair.reshape(group // 2, share, features), TP[0])
    return arrived.astype(F32).sum(axis=0).astype(BF16)


def solution(mesh):
    torus = Mesh(mesh.devices.reshape(8, 8, mesh.shape["tp"] // 2, 2), SP_TP)
    placed = (
        P(SP_TP, None),
        P(),
        P(SP, TP),
        P(SP, TP),
        P(SP, TP),
        P(SP, TP),
        P(TP),
        P(SP, TP),
        P(),
        P(SP, TP),
        P(SP, TP),
        P(None, TP),
        P(TP),
        P(TP),
        P(TP, SP),
        P(TP, SP),
    )

    return jax.shard_map(
        on_device, mesh=torus, in_specs=placed, out_specs=P(SP_TP, None), check_vma=False
    )
```

```python
import jax
import jax.numpy as jnp
from jax import lax
from jax.experimental import pallas as pl
from jax.experimental.pallas import tpu as pltpu
from jax.sharding import Mesh
from jax.sharding import PartitionSpec as P

HEAD_K = 128
KERNEL = 31
BLOCK = 64
HALO = 32
SP = ("sp_0", "sp_1")
TP = ("x", "core")
SP_TP = SP + TP
F32 = jnp.float32
BF16 = jnp.bfloat16
EXACT = lax.Precision.HIGHEST


def dot_nt(a, b):
    return lax.dot_general(a, b, (((1,), (1,)), ((), ())), preferred_element_type=F32)


def dot_tn(a, b):
    return lax.dot_general(a, b, (((0,), (0,)), ((), ())), preferred_element_type=F32)


def call(body, outs, *args, grid=None, in_specs=None, out_specs=None, scratch=()):
    specs = {}
    if in_specs is not None:
        specs["in_specs"] = in_specs
    if out_specs is not None:
        specs["out_specs"] = out_specs
    if grid is not None:
        specs["grid"] = grid
    return pl.pallas_call(body, out_shape=outs, scratch_shapes=scratch, **specs)(*args)


def whole(count):
    return [pl.BlockSpec(memory_space=pltpu.VMEM)] * count


def first_body(gv, gg, q, g, wr, wc, f, v, operand, copies):
    operand[...] = jnp.concatenate([w[...] for w in (gv, gg, q, g, wr, wc)], axis=1)
    joined = jnp.concatenate([f[...], v[...]], axis=1)
    for k in range(copies.shape[0]):
        copies[k] = joined


def again_body(value, copies):
    for k in range(copies.shape[0]):
        copies[k] = value[...]


def norm_body(places, gain, *refs):
    *pieces, out, tail = refs
    share = tail.shape[0]
    for n, piece in enumerate(pieces):
        values_in = piece[...].astype(F32)
        row_scale = lax.rsqrt(jnp.mean(values_in * values_in, axis=1, keepdims=True) + 1e-06)
        scaled = (values_in * row_scale * gain[...]).astype(BF16)
        out[pl.ds(pl.multiple_of(places[n] * share, share), share)] = scaled
    tail[...] = out[out.shape[0] - share :]


def pack_state(out, state, total):
    high = total.astype(BF16).astype(F32)
    row = lax.broadcasted_iota(jnp.int32, (8, total.shape[1]), 0)
    tail = jnp.where(row == 0, high, jnp.where(row == 1, total - high, 0.0)).astype(BF16)
    state = state.astype(BF16)
    width = state.shape[0]
    for k in range(out.shape[0]):
        out[k, :width] = state
        out[k, width:] = tail


def causal_mask():
    at_row = lax.broadcasted_iota(jnp.int32, (BLOCK, BLOCK), 0)
    at_col = lax.broadcasted_iota(jnp.int32, (BLOCK, BLOCK), 1)
    return at_row >= at_col


def state_body(normed, weights, leak, shift, sent, value_out, key, totals, starts, befores):
    rows = normed.shape[0]
    peers = weights.shape[0]
    ordered = jnp.concatenate(
        [weights[inner, outer] for outer in range(weights.shape[1]) for inner in range(peers)],
        axis=0,
    )
    projected = jnp.dot(normed[...], ordered, preferred_element_type=F32).astype(BF16)
    value = projected[:, HEAD_K:]
    value_out[...] = value
    in_gate = leak[...] * jax.nn.sigmoid(-projected[:, :HEAD_K].astype(F32))
    log_decay = jnp.log1p(-in_gate) + shift[...]
    triangle = jnp.where(causal_mask(), 1.0, 0.0).astype(F32)
    state = jnp.zeros((HEAD_K, HEAD_K), F32)
    before = jnp.zeros((1, HEAD_K), F32)
    kept = []
    for n in range(rows // BLOCK):
        at = slice(n * BLOCK, (n + 1) * BLOCK)
        total = jnp.dot(triangle, log_decay[at], precision=EXACT, preferred_element_type=F32)
        last = total[BLOCK - 1 :]
        totals[at] = total
        key[at] = (in_gate[at] * jnp.exp(-total)).astype(BF16)
        starts[n] = state.astype(BF16)
        kept.append(before)
        late_key = (in_gate[at] * jnp.exp(last - total)).astype(BF16)
        state = jnp.exp(last) * state + dot_tn(value[at], late_key)
        before = before + last
    befores[...] = jnp.concatenate(kept, axis=0)
    pack_state(sent, state, before)


def unpack(got, k):
    tail = got[k, HEAD_K:].astype(F32)
    return got[k, :HEAD_K].astype(F32), tail[0:1] + tail[1:2]


def gathered_before(got, position):
    state = inside_state = jnp.zeros((HEAD_K, HEAD_K), F32)
    total = inside_total = jnp.zeros((1, HEAD_K), F32)
    for k in range(got.shape[0]):
        passed = k < position
        new_state, new_total = unpack(got, k)
        state = jnp.exp(new_total) * state + new_state
        total = total + new_total
        inside_state = jnp.where(passed, state, inside_state)
        inside_total = jnp.where(passed, total, inside_total)
    return inside_state, inside_total, state, total


def inner_body(position, got, sent, inner_state, inner_total):
    inside_state, inside_total, state, total = gathered_before(got, position[0])
    inner_state[...] = inside_state
    inner_total[...] = jnp.broadcast_to(inside_total, inner_total.shape)
    pack_state(sent, state, total)


def outer_body(
    position,
    got,
    inner_state,
    inner_total,
    normed,
    weights,
    value,
    key,
    totals,
    starts,
    befores,
    gain,
    out,
):
    outside_state = gathered_before(got, position[0])[0]
    incoming = jnp.exp(inner_total[0:1]) * outside_state + inner_state[...]
    projected = jnp.dot(normed[...], weights[...], preferred_element_type=F32)
    projected = projected.astype(BF16).astype(F32)
    queries = jax.nn.silu(projected[:, :HEAD_K])
    gate_act = jax.nn.silu(projected[:, HEAD_K:])
    causal = causal_mask()
    for n in range(starts.shape[0]):
        at = slice(n * BLOCK, (n + 1) * BLOCK)
        query = (queries[at] * jnp.exp(totals[at])).astype(BF16)
        scores = jnp.where(causal, dot_nt(query, key[at]), 0.0).astype(BF16)
        state = jnp.exp(befores[n : n + 1]) * incoming + starts[n].astype(F32)
        recur = jnp.dot(scores, value[at], preferred_element_type=F32)
        recur = recur + dot_nt(query, state.astype(BF16))
        scaling = lax.rsqrt(jnp.mean(recur * recur, axis=1, keepdims=True) + 1e-06)
        out[at] = (recur * scaling * gain[...] * gate_act[at]).astype(BF16)


def conv_body(halo, normed, weights, taps, conv, stats, shifted):
    channels = conv.shape[1]
    rows = conv.shape[0]
    filled = HALO + rows
    extended = jnp.concatenate([halo[...], normed[...]], axis=0)
    projected = jnp.dot(extended, weights[...], preferred_element_type=F32)
    projected = projected.astype(BF16).astype(F32)
    glu = projected[:, :channels] * jax.nn.sigmoid(projected[:, channels:])
    shifted[0, :filled] = glu.astype(BF16).astype(F32)
    for r in range(1, 8):
        shifted[r, : filled - 8] = shifted[0, r : filled - 8 + r]
    first = HALO - (KERNEL - 1)
    step = 32
    for row in range(0, rows, step):
        accum = jnp.zeros((step, channels), F32)
        for tap in range(KERNEL):
            off = row + first + tap
            base = off // 8 * 8
            accum = accum + taps[tap : tap + 1] * shifted[off - base, base : base + step]
        conv[row : row + step] = accum
    summed = conv[...]
    ones = jnp.ones((8, channels), F32)

    def over_channels(value):
        return lax.dot_general(
            ones, value, (((1,), (1,)), ((), ())), precision=EXACT, preferred_element_type=F32
        )

    row = lax.broadcasted_iota(jnp.int32, (8, rows), 0)
    both = jnp.where(row == 0, over_channels(summed), over_channels(summed * summed))[0:2]
    for k in range(stats.shape[0]):
        stats[k] = both


def out_body(core, stats, conv, head_out, ln_gain, ln_bias, w_rec, w_low, w_high, rows_out, out):
    channels = conv.shape[1]
    share = conv.shape[0] // stats.shape[0]
    both = stats[0]
    for k in range(1, stats.shape[0]):
        both = both + stats[k]
    both = both / (channels * stats.shape[0])
    mean = both[0:1]
    inverse = lax.rsqrt(both[1:2] - mean * mean + 1e-05)
    row = lax.broadcasted_iota(jnp.int32, (8, both.shape[1]), 0)
    paired = jnp.where(row == 0, mean, jnp.where(row == 1, inverse, 0.0))

    def column(k):
        chosen = jnp.where(lax.broadcasted_iota(jnp.int32, (8, channels), 0) == k, 1.0, 0.0)
        return lax.dot_general(
            paired,
            chosen.astype(F32),
            (((0,), (0,)), ((), ())),
            precision=EXACT,
            preferred_element_type=F32,
        )

    normal = (conv[...] - column(0)) * column(1) * ln_gain[...] + ln_bias[...]
    conv_out = jax.nn.silu(normal).astype(BF16)
    for k in range(stats.shape[0]):
        piece = slice(k * share, (k + 1) * share)
        at = slice(k // 2 * share, (k // 2 + 1) * share)
        rows_out[k % 2, at, :HEAD_K] = head_out[piece]
        rows_out[k % 2, at, HEAD_K:] = conv_out[piece]
    out[...] = product(rows_out[1 - core[0]], w_rec, w_low, w_high)


def product(rows, w_rec, w_low, w_high):
    mixed = dot_nt(rows[:, :HEAD_K], w_rec[...])
    mixed = mixed + dot_nt(rows[:, HEAD_K : 2 * HEAD_K], w_low[...])
    mixed = mixed + dot_nt(rows[:, 2 * HEAD_K :], w_high[...])
    return mixed.astype(BF16)


def own_body(core, rows, w_rec, w_low, w_high, out):
    out[...] = product(rows[core[0]], w_rec, w_low, w_high)


def swap(value, axis):
    return lax.all_to_all(value, axis, split_axis=0, concat_axis=0, tiled=True)


def shifted_around(value, axis):
    count = lax.axis_size(axis)
    pieces = [value]
    for k in range(1, count):
        pieces.append(lax.ppermute(value, axis, [(n, (n + k) % count) for n in range(count)]))
    return pieces, (lax.axis_index(axis) + count - jnp.arange(count, dtype=jnp.int32)) % count


def on_device(
    tokens,
    norm_gain,
    w_query,
    w_forget,
    w_value,
    w_outgate,
    leak,
    decay_shift,
    head_gain,
    w_glu_value,
    w_glu_gate,
    conv_kernel,
    ln_gain,
    ln_bias,
    w_out_rec,
    w_out_conv,
):
    shape = jax.ShapeDtypeStruct
    smem = pl.BlockSpec(memory_space=pltpu.SMEM)
    inner_count = lax.axis_size(SP[1])
    group = lax.axis_size(TP)
    share, features = tokens.shape
    depth = w_query.shape[0]
    channels = conv_kernel.shape[1]
    columns = (w_glu_value, w_glu_gate, w_query, w_outgate, w_out_rec.T, w_out_conv.T)
    glu_width = 2 * channels
    all_width = sum(w.shape[1] for w in columns)
    outer_count = lax.axis_size(SP[0])
    operand, copies = call(
        first_body,
        (
            shape((depth, all_width), BF16),
            shape((outer_count, depth, 2 * HEAD_K), BF16),
        ),
        *columns,
        w_forget,
        w_value,
    )
    gathered = lax.all_gather(operand, SP, axis=0, tiled=True)
    column = swap(copies, SP[0])
    copies = call(again_body, shape((inner_count, *column.shape), BF16), column)
    state_weights = swap(copies, SP[1])
    pieces, places = shifted_around(tokens, TP)
    rows = group * share
    normed, tail = call(
        norm_body,
        (shape((rows, features), BF16), shape((share, features), BF16)),
        places,
        norm_gain.reshape(1, -1),
        *pieces,
        in_specs=[smem] + whole(1 + len(pieces)),
    )
    count = lax.axis_size(SP)
    halo = lax.ppermute(tail, SP, [(k, k + 1) for k in range(count - 1)])
    message = shape((inner_count, HEAD_K + 8, HEAD_K), BF16)
    blocks = rows // BLOCK
    sent, *kept = call(
        state_body,
        (
            message,
            shape((rows, HEAD_K), BF16),
            shape((rows, HEAD_K), BF16),
            shape((rows, HEAD_K), F32),
            shape((blocks, HEAD_K, HEAD_K), BF16),
            shape((blocks, HEAD_K), F32),
        ),
        normed,
        state_weights,
        leak.reshape(1, -1),
        decay_shift,
    )
    sent, inner_state, inner_total = call(
        inner_body,
        (message, shape((HEAD_K, HEAD_K), F32), shape((8, HEAD_K), F32)),
        lax.axis_index(SP[1]).reshape(1),
        swap(sent, SP[1]),
        in_specs=[smem] + whole(1),
    )

    def part(size, at):
        return pl.BlockSpec((gathered.shape[0], size), lambda k: (0, at))

    def full(*lengths):
        return pl.BlockSpec(lengths, lambda k: (0,) * len(lengths))

    conv, stats = call(
        conv_body,
        (shape((rows, channels), F32), shape((group, 2, rows), F32)),
        halo,
        normed,
        gathered,
        conv_kernel,
        grid=(1,),
        in_specs=[
            full(*halo.shape),
            full(*normed.shape),
            part(glu_width, 0),
            full(*conv_kernel.shape),
        ],
        out_specs=(full(rows, channels), full(group, 2, rows)),
        scratch=(pltpu.VMEM((8, HALO + rows, channels), F32),),
    )
    stats = swap(stats, TP)
    outer_sent = swap(sent, SP[0])
    head_gain = head_gain.reshape(1, -1)
    head_out = call(
        outer_body,
        shape((rows, HEAD_K), BF16),
        lax.axis_index(SP[0]).reshape(1),
        outer_sent,
        inner_state,
        inner_total,
        normed,
        gathered,
        *kept,
        head_gain,
        grid=(1,),
        in_specs=[
            smem,
            *[full(*a.shape) for a in (outer_sent, inner_state, inner_total, normed)],
            part(2 * HEAD_K, glu_width // (2 * HEAD_K)),
            *[full(*a.shape) for a in kept],
            full(*head_gain.shape),
        ],
        out_specs=full(rows, HEAD_K),
    )
    first = glu_width // HEAD_K + 2
    half = rows // 2
    width = HEAD_K + channels
    core = lax.axis_index(TP[1]).reshape(1)
    weights = [gathered] * 3
    weight_specs = [part(HEAD_K, first + k) for k in range(3)]
    mixed_rows, sent = call(
        out_body,
        (shape((2, half, width), BF16), shape((half, features), BF16)),
        core,
        stats,
        conv,
        head_out,
        ln_gain.reshape(1, -1),
        ln_bias.reshape(1, -1),
        *weights,
        grid=(1,),
        in_specs=[
            smem,
            full(*stats.shape),
            full(rows, channels),
            full(rows, HEAD_K),
            full(1, channels),
            full(1, channels),
            *weight_specs,
        ],
        out_specs=(full(2, half, width), full(half, features)),
    )
    received = lax.ppermute(sent, TP[1], [(0, 1), (1, 0)])
    own = call(
        own_body,
        shape((half, features), BF16),
        core,
        mixed_rows,
        *weights,
        grid=(1,),
        in_specs=[smem, full(2, half, width), *weight_specs],
        out_specs=full(half, features),
    )
    pair = (own.astype(F32) + received.astype(F32)).astype(BF16)
    arrived = swap(pair.reshape(group // 2, share, features), TP[0])
    return arrived.astype(F32).sum(axis=0).astype(BF16)


def solution(mesh):
    torus = Mesh(mesh.devices.reshape(8, 8, mesh.shape["tp"] // 2, 2), SP_TP)
    placed = (
        P(SP_TP, None),
        P(),
        P(SP, TP),
        P(SP, TP),
        P(SP, TP),
        P(SP, TP),
        P(TP),
        P(SP, TP),
        P(),
        P(SP, TP),
        P(SP, TP),
        P(None, TP),
        P(TP),
        P(TP),
        P(TP, SP),
        P(TP, SP),
    )

    return jax.shard_map(
        on_device, mesh=torus, in_specs=placed, out_specs=P(SP_TP, None), check_vma=False
    )
```

```python
import jax
import jax.numpy as jnp
from jax import lax
from jax.experimental import pallas as pl
from jax.experimental.pallas import tpu as pltpu
from jax.sharding import Mesh
from jax.sharding import PartitionSpec as P

HEAD_K = 128
KERNEL = 31
BLOCK = 64
HALO = 32
SP = ("sp_0", "sp_1")
TP = ("x", "core")
SP_TP = SP + TP
F32 = jnp.float32
BF16 = jnp.bfloat16
EXACT = lax.Precision.HIGHEST


def dot_nt(a, b):
    return lax.dot_general(a, b, (((1,), (1,)), ((), ())), preferred_element_type=F32)


def dot_tn(a, b):
    return lax.dot_general(a, b, (((0,), (0,)), ((), ())), preferred_element_type=F32)


def call(body, outs, *args, grid=None, in_specs=None, out_specs=None, scratch=()):
    specs = {}
    if in_specs is not None:
        specs["in_specs"] = in_specs
    if out_specs is not None:
        specs["out_specs"] = out_specs
    if grid is not None:
        specs["grid"] = grid
    return pl.pallas_call(body, out_shape=outs, scratch_shapes=scratch, **specs)(*args)


def whole(count):
    return [pl.BlockSpec(memory_space=pltpu.VMEM)] * count


def first_body(gv, gg, q, g, wr, wc, f, v, operand, copies):
    together = jnp.concatenate([w[...] for w in (gv, gg, q, g, wr, wc)], axis=1)
    operand[:, : together.shape[1]] = together
    operand[:, together.shape[1] :] = jnp.zeros_like(operand[:, together.shape[1] :])
    joined = jnp.concatenate([f[...], v[...]], axis=1)
    for k in range(copies.shape[0]):
        copies[k] = joined


def trim_body(value, out):
    out[...] = value[...]


def again_body(value, copies):
    for k in range(copies.shape[0]):
        copies[k] = value[...]


def norm_body(places, gain, *refs):
    *pieces, out, tail = refs
    share = tail.shape[0]
    for n, piece in enumerate(pieces):
        values_in = piece[...].astype(F32)
        row_scale = lax.rsqrt(jnp.mean(values_in * values_in, axis=1, keepdims=True) + 1e-06)
        scaled = (values_in * row_scale * gain[...]).astype(BF16)
        out[pl.ds(pl.multiple_of(places[n] * share, share), share)] = scaled
    tail[...] = out[out.shape[0] - share :]


def pack_state(out, state, total):
    high = total.astype(BF16).astype(F32)
    row = lax.broadcasted_iota(jnp.int32, (8, total.shape[1]), 0)
    tail = jnp.where(row == 0, high, jnp.where(row == 1, total - high, 0.0)).astype(BF16)
    state = state.astype(BF16)
    width = state.shape[0]
    for k in range(out.shape[0]):
        out[k, :width] = state
        out[k, width:] = tail


def causal_mask():
    at_row = lax.broadcasted_iota(jnp.int32, (BLOCK, BLOCK), 0)
    at_col = lax.broadcasted_iota(jnp.int32, (BLOCK, BLOCK), 1)
    return at_row >= at_col


def state_body(normed, weights, leak, shift, sent, value_out, key, totals, starts, befores):
    rows = normed.shape[0]
    peers = weights.shape[0]
    ordered = jnp.concatenate(
        [weights[inner, outer] for outer in range(weights.shape[1]) for inner in range(peers)],
        axis=0,
    )
    projected = jnp.dot(normed[...], ordered, preferred_element_type=F32).astype(BF16)
    value = projected[:, HEAD_K:]
    value_out[...] = value
    in_gate = leak[...] * jax.nn.sigmoid(-projected[:, :HEAD_K].astype(F32))
    log_decay = jnp.log1p(-in_gate) + shift[...]
    triangle = jnp.where(causal_mask(), 1.0, 0.0).astype(F32)
    state = jnp.zeros((HEAD_K, HEAD_K), F32)
    before = jnp.zeros((1, HEAD_K), F32)
    kept = []
    for n in range(rows // BLOCK):
        at = slice(n * BLOCK, (n + 1) * BLOCK)
        total = jnp.dot(triangle, log_decay[at], precision=EXACT, preferred_element_type=F32)
        last = total[BLOCK - 1 :]
        totals[at] = total
        key[at] = (in_gate[at] * jnp.exp(-total)).astype(BF16)
        starts[n] = state.astype(BF16)
        kept.append(before)
        late_key = (in_gate[at] * jnp.exp(last - total)).astype(BF16)
        state = jnp.exp(last) * state + dot_tn(value[at], late_key)
        before = before + last
    befores[...] = jnp.concatenate(kept, axis=0)
    pack_state(sent, state, before)


def unpack(got, k):
    tail = got[k, HEAD_K:].astype(F32)
    return got[k, :HEAD_K].astype(F32), tail[0:1] + tail[1:2]


def gathered_before(got, position):
    state = inside_state = jnp.zeros((HEAD_K, HEAD_K), F32)
    total = inside_total = jnp.zeros((1, HEAD_K), F32)
    for k in range(got.shape[0]):
        passed = k < position
        new_state, new_total = unpack(got, k)
        state = jnp.exp(new_total) * state + new_state
        total = total + new_total
        inside_state = jnp.where(passed, state, inside_state)
        inside_total = jnp.where(passed, total, inside_total)
    return inside_state, inside_total, state, total


def inner_body(position, got, sent, inner_state, inner_total):
    inside_state, inside_total, state, total = gathered_before(got, position[0])
    inner_state[...] = inside_state
    inner_total[...] = jnp.broadcast_to(inside_total, inner_total.shape)
    pack_state(sent, state, total)


def outer_body(
    position,
    got,
    inner_state,
    inner_total,
    normed,
    weights,
    value,
    key,
    totals,
    starts,
    befores,
    gain,
    out,
):
    outside_state = gathered_before(got, position[0])[0]
    incoming = jnp.exp(inner_total[0:1]) * outside_state + inner_state[...]
    projected = jnp.dot(normed[...], weights[...], preferred_element_type=F32)
    projected = projected.astype(BF16).astype(F32)
    queries = jax.nn.silu(projected[:, :HEAD_K])
    gate_act = jax.nn.silu(projected[:, HEAD_K:])
    causal = causal_mask()
    for n in range(starts.shape[0]):
        at = slice(n * BLOCK, (n + 1) * BLOCK)
        query = (queries[at] * jnp.exp(totals[at])).astype(BF16)
        scores = jnp.where(causal, dot_nt(query, key[at]), 0.0).astype(BF16)
        state = jnp.exp(befores[n : n + 1]) * incoming + starts[n].astype(F32)
        recur = jnp.dot(scores, value[at], preferred_element_type=F32)
        recur = recur + dot_nt(query, state.astype(BF16))
        scaling = lax.rsqrt(jnp.mean(recur * recur, axis=1, keepdims=True) + 1e-06)
        out[at] = (recur * scaling * gain[...] * gate_act[at]).astype(BF16)


def conv_body(halo, normed, weights, taps, conv, stats, shifted):
    channels = conv.shape[1]
    rows = conv.shape[0]
    filled = HALO + rows
    extended = jnp.concatenate([halo[...], normed[...]], axis=0)
    projected = jnp.dot(extended, weights[...], preferred_element_type=F32)
    projected = projected.astype(BF16).astype(F32)
    glu = projected[:, :channels] * jax.nn.sigmoid(projected[:, channels:])
    shifted[0, :filled] = glu.astype(BF16).astype(F32)
    for r in range(1, 8):
        shifted[r, : filled - 8] = shifted[0, r : filled - 8 + r]
    first = HALO - (KERNEL - 1)
    step = 32
    for row in range(0, rows, step):
        accum = jnp.zeros((step, channels), F32)
        for tap in range(KERNEL):
            off = row + first + tap
            base = off // 8 * 8
            accum = accum + taps[tap : tap + 1] * shifted[off - base, base : base + step]
        conv[row : row + step] = accum
    summed = conv[...]
    ones = jnp.ones((8, channels), F32)

    def over_channels(value):
        return lax.dot_general(
            ones, value, (((1,), (1,)), ((), ())), precision=EXACT, preferred_element_type=F32
        )

    row = lax.broadcasted_iota(jnp.int32, (8, rows), 0)
    both = jnp.where(row == 0, over_channels(summed), over_channels(summed * summed))[0:2]
    for k in range(stats.shape[0]):
        stats[k] = both


def out_body(core, stats, conv, head_out, ln_gain, ln_bias, w_rec, w_low, w_high, rows_out, out):
    channels = conv.shape[1]
    share = conv.shape[0] // stats.shape[0]
    both = stats[0]
    for k in range(1, stats.shape[0]):
        both = both + stats[k]
    both = both / (channels * stats.shape[0])
    mean = both[0:1]
    inverse = lax.rsqrt(both[1:2] - mean * mean + 1e-05)
    row = lax.broadcasted_iota(jnp.int32, (8, both.shape[1]), 0)
    paired = jnp.where(row == 0, mean, jnp.where(row == 1, inverse, 0.0))

    def column(k):
        chosen = jnp.where(lax.broadcasted_iota(jnp.int32, (8, channels), 0) == k, 1.0, 0.0)
        return lax.dot_general(
            paired,
            chosen.astype(F32),
            (((0,), (0,)), ((), ())),
            precision=EXACT,
            preferred_element_type=F32,
        )

    normal = (conv[...] - column(0)) * column(1) * ln_gain[...] + ln_bias[...]
    conv_out = jax.nn.silu(normal).astype(BF16)
    for k in range(stats.shape[0]):
        piece = slice(k * share, (k + 1) * share)
        at = slice(k // 2 * share, (k // 2 + 1) * share)
        rows_out[k % 2, at, :HEAD_K] = head_out[piece]
        rows_out[k % 2, at, HEAD_K:] = conv_out[piece]
    out[...] = product(rows_out[1 - core[0]], w_rec, w_low, w_high)


def product(rows, w_rec, w_low, w_high):
    mixed = dot_nt(rows[:, :HEAD_K], w_rec[...])
    mixed = mixed + dot_nt(rows[:, HEAD_K : 2 * HEAD_K], w_low[...])
    mixed = mixed + dot_nt(rows[:, 2 * HEAD_K :], w_high[...])
    return mixed.astype(BF16)


def own_body(core, rows, w_rec, w_low, w_high, out):
    out[...] = product(rows[core[0]], w_rec, w_low, w_high)


def swap(value, axis):
    return lax.all_to_all(value, axis, split_axis=0, concat_axis=0, tiled=True)


def shifted_around(value, axis):
    count = lax.axis_size(axis)
    pieces = [value]
    for k in range(1, count):
        pieces.append(lax.ppermute(value, axis, [(n, (n + k) % count) for n in range(count)]))
    return pieces, (lax.axis_index(axis) + count - jnp.arange(count, dtype=jnp.int32)) % count


def on_device(
    tokens,
    norm_gain,
    w_query,
    w_forget,
    w_value,
    w_outgate,
    leak,
    decay_shift,
    head_gain,
    w_glu_value,
    w_glu_gate,
    conv_kernel,
    ln_gain,
    ln_bias,
    w_out_rec,
    w_out_conv,
):
    shape = jax.ShapeDtypeStruct
    smem = pl.BlockSpec(memory_space=pltpu.SMEM)
    inner_count = lax.axis_size(SP[1])
    group = lax.axis_size(TP)
    share, features = tokens.shape
    depth = w_query.shape[0]
    channels = conv_kernel.shape[1]
    columns = (w_glu_value, w_glu_gate, w_query, w_outgate, w_out_rec.T, w_out_conv.T)
    glu_width = 2 * channels
    all_width = sum(w.shape[1] for w in columns)
    outer_count = lax.axis_size(SP[0])
    operand, copies = call(
        first_body,
        (
            shape((depth, features), BF16),
            shape((outer_count, depth, 2 * HEAD_K), BF16),
        ),
        *columns,
        w_forget,
        w_value,
    )
    inner = lax.all_gather(operand, SP[1], axis=0, tiled=True)
    piece = pl.BlockSpec((inner_count * depth, all_width), lambda k: (0, 0))
    inner = call(
        trim_body,
        shape((inner_count * depth, all_width), BF16),
        inner,
        grid=(1,),
        in_specs=[piece],
        out_specs=piece,
    )
    gathered = lax.all_gather(inner, SP[0], axis=0, tiled=True)
    column = swap(copies, SP[0])
    copies = call(again_body, shape((inner_count, *column.shape), BF16), column)
    state_weights = swap(copies, SP[1])
    pieces, places = shifted_around(tokens, TP)
    rows = group * share
    normed, tail = call(
        norm_body,
        (shape((rows, features), BF16), shape((share, features), BF16)),
        places,
        norm_gain.reshape(1, -1),
        *pieces,
        in_specs=[smem] + whole(1 + len(pieces)),
    )
    count = lax.axis_size(SP)
    halo = lax.ppermute(tail, SP, [(k, k + 1) for k in range(count - 1)])
    message = shape((inner_count, HEAD_K + 8, HEAD_K), BF16)
    blocks = rows // BLOCK
    sent, *kept = call(
        state_body,
        (
            message,
            shape((rows, HEAD_K), BF16),
            shape((rows, HEAD_K), BF16),
            shape((rows, HEAD_K), F32),
            shape((blocks, HEAD_K, HEAD_K), BF16),
            shape((blocks, HEAD_K), F32),
        ),
        normed,
        state_weights,
        leak.reshape(1, -1),
        decay_shift,
    )
    sent, inner_state, inner_total = call(
        inner_body,
        (message, shape((HEAD_K, HEAD_K), F32), shape((8, HEAD_K), F32)),
        lax.axis_index(SP[1]).reshape(1),
        swap(sent, SP[1]),
        in_specs=[smem] + whole(1),
    )

    def part(size, at):
        return pl.BlockSpec((gathered.shape[0], size), lambda k: (0, at))

    def full(*lengths):
        return pl.BlockSpec(lengths, lambda k: (0,) * len(lengths))

    conv, stats = call(
        conv_body,
        (shape((rows, channels), F32), shape((group, 2, rows), F32)),
        halo,
        normed,
        gathered,
        conv_kernel,
        grid=(1,),
        in_specs=[
            full(*halo.shape),
            full(*normed.shape),
            part(glu_width, 0),
            full(*conv_kernel.shape),
        ],
        out_specs=(full(rows, channels), full(group, 2, rows)),
        scratch=(pltpu.VMEM((8, HALO + rows, channels), F32),),
    )
    stats = swap(stats, TP)
    outer_sent = swap(sent, SP[0])
    head_gain = head_gain.reshape(1, -1)
    head_out = call(
        outer_body,
        shape((rows, HEAD_K), BF16),
        lax.axis_index(SP[0]).reshape(1),
        outer_sent,
        inner_state,
        inner_total,
        normed,
        gathered,
        *kept,
        head_gain,
        grid=(1,),
        in_specs=[
            smem,
            *[full(*a.shape) for a in (outer_sent, inner_state, inner_total, normed)],
            part(2 * HEAD_K, glu_width // (2 * HEAD_K)),
            *[full(*a.shape) for a in kept],
            full(*head_gain.shape),
        ],
        out_specs=full(rows, HEAD_K),
    )
    first = glu_width // HEAD_K + 2
    half = rows // 2
    width = HEAD_K + channels
    core = lax.axis_index(TP[1]).reshape(1)
    weights = [gathered] * 3
    weight_specs = [part(HEAD_K, first + k) for k in range(3)]
    mixed_rows, sent = call(
        out_body,
        (shape((2, half, width), BF16), shape((half, features), BF16)),
        core,
        stats,
        conv,
        head_out,
        ln_gain.reshape(1, -1),
        ln_bias.reshape(1, -1),
        *weights,
        grid=(1,),
        in_specs=[
            smem,
            full(*stats.shape),
            full(rows, channels),
            full(rows, HEAD_K),
            full(1, channels),
            full(1, channels),
            *weight_specs,
        ],
        out_specs=(full(2, half, width), full(half, features)),
    )
    received = lax.ppermute(sent, TP[1], [(0, 1), (1, 0)])
    own = call(
        own_body,
        shape((half, features), BF16),
        core,
        mixed_rows,
        *weights,
        grid=(1,),
        in_specs=[smem, full(2, half, width), *weight_specs],
        out_specs=full(half, features),
    )
    pair = (own.astype(F32) + received.astype(F32)).astype(BF16)
    arrived = swap(pair.reshape(group // 2, share, features), TP[0])
    return arrived.astype(F32).sum(axis=0).astype(BF16)


def solution(mesh):
    torus = Mesh(mesh.devices.reshape(8, 8, mesh.shape["tp"] // 2, 2), SP_TP)
    placed = (
        P(SP_TP, None),
        P(),
        P(SP, TP),
        P(SP, TP),
        P(SP, TP),
        P(SP, TP),
        P(TP),
        P(SP, TP),
        P(),
        P(SP, TP),
        P(SP, TP),
        P(None, TP),
        P(TP),
        P(TP),
        P(TP, SP),
        P(TP, SP),
    )

    return jax.shard_map(
        on_device, mesh=torus, in_specs=placed, out_specs=P(SP_TP, None), check_vma=False
    )
```

```python
import jax
import jax.numpy as jnp
from jax import lax
from jax.experimental import pallas as pl
from jax.experimental.pallas import tpu as pltpu
from jax.sharding import Mesh
from jax.sharding import PartitionSpec as P

HEAD_K = 128
KERNEL = 31
BLOCK = 64
HALO = 32
SP = ("sp_0", "sp_1")
TP = ("x", "core")
SP_TP = SP + TP
F32 = jnp.float32
BF16 = jnp.bfloat16
EXACT = lax.Precision.HIGHEST


def dot_nt(a, b):
    return lax.dot_general(a, b, (((1,), (1,)), ((), ())), preferred_element_type=F32)


def dot_tn(a, b):
    return lax.dot_general(a, b, (((0,), (0,)), ((), ())), preferred_element_type=F32)


def call(body, outs, *args, grid=None, in_specs=None, out_specs=None, scratch=()):
    specs = {}
    if in_specs is not None:
        specs["in_specs"] = in_specs
    if out_specs is not None:
        specs["out_specs"] = out_specs
    if grid is not None:
        specs["grid"] = grid
    return pl.pallas_call(body, out_shape=outs, scratch_shapes=scratch, **specs)(*args)


def whole(count):
    return [pl.BlockSpec(memory_space=pltpu.VMEM)] * count


def first_body(gv, gg, q, g, wr, wc, copies):
    together = jnp.concatenate([w[...] for w in (gv, gg, q, g, wr, wc)], axis=1)
    for k in range(copies.shape[0]):
        copies[k] = together


def second_body(f, v, copies):
    joined = jnp.concatenate([f[...], v[...]], axis=1)
    for k in range(copies.shape[0]):
        copies[k] = joined


def norm_body(places, gain, *refs):
    *pieces, out, tail = refs
    share = tail.shape[0]
    for n, piece in enumerate(pieces):
        values_in = piece[...].astype(F32)
        row_scale = lax.rsqrt(jnp.mean(values_in * values_in, axis=1, keepdims=True) + 1e-06)
        scaled = (values_in * row_scale * gain[...]).astype(BF16)
        out[pl.ds(pl.multiple_of(places[n] * share, share), share)] = scaled
    tail[...] = out[out.shape[0] - share :]


def pack_state(out, state, total):
    high = total.astype(BF16).astype(F32)
    row = lax.broadcasted_iota(jnp.int32, (8, total.shape[1]), 0)
    tail = jnp.where(row == 0, high, jnp.where(row == 1, total - high, 0.0)).astype(BF16)
    state = state.astype(BF16)
    width = state.shape[0]
    for k in range(out.shape[0]):
        out[k, :width] = state
        out[k, width:] = tail


def causal_mask():
    at_row = lax.broadcasted_iota(jnp.int32, (BLOCK, BLOCK), 0)
    at_col = lax.broadcasted_iota(jnp.int32, (BLOCK, BLOCK), 1)
    return at_row >= at_col


def state_body(normed, weights, leak, shift, sent, value_out, key, totals, starts, befores):
    rows = normed.shape[0]
    projected = jnp.dot(normed[...], weights[...], preferred_element_type=F32).astype(BF16)
    value = projected[:, HEAD_K:]
    value_out[...] = value
    in_gate = leak[...] * jax.nn.sigmoid(-projected[:, :HEAD_K].astype(F32))
    log_decay = jnp.log1p(-in_gate) + shift[...]
    triangle = jnp.where(causal_mask(), 1.0, 0.0).astype(F32)
    state = jnp.zeros((HEAD_K, HEAD_K), F32)
    before = jnp.zeros((1, HEAD_K), F32)
    kept = []
    for n in range(rows // BLOCK):
        at = slice(n * BLOCK, (n + 1) * BLOCK)
        total = jnp.dot(triangle, log_decay[at], precision=EXACT, preferred_element_type=F32)
        last = total[BLOCK - 1 :]
        totals[at] = total
        key[at] = (in_gate[at] * jnp.exp(-total)).astype(BF16)
        starts[n] = state.astype(BF16)
        kept.append(before)
        late_key = (in_gate[at] * jnp.exp(last - total)).astype(BF16)
        state = jnp.exp(last) * state + dot_tn(value[at], late_key)
        before = before + last
    befores[...] = jnp.concatenate(kept, axis=0)
    pack_state(sent, state, before)


def unpack(got, k):
    tail = got[k, HEAD_K:].astype(F32)
    return got[k, :HEAD_K].astype(F32), tail[0:1] + tail[1:2]


def gathered_before(got, position):
    state = inside_state = jnp.zeros((HEAD_K, HEAD_K), F32)
    total = inside_total = jnp.zeros((1, HEAD_K), F32)
    for k in range(got.shape[0]):
        passed = k < position
        new_state, new_total = unpack(got, k)
        state = jnp.exp(new_total) * state + new_state
        total = total + new_total
        inside_state = jnp.where(passed, state, inside_state)
        inside_total = jnp.where(passed, total, inside_total)
    return inside_state, inside_total, state, total


def inner_body(position, got, sent, inner_state, inner_total):
    inside_state, inside_total, state, total = gathered_before(got, position[0])
    inner_state[...] = inside_state
    inner_total[...] = jnp.broadcast_to(inside_total, inner_total.shape)
    pack_state(sent, state, total)


def outer_body(
    position,
    got,
    inner_state,
    inner_total,
    normed,
    weights,
    value,
    key,
    totals,
    starts,
    befores,
    gain,
    out,
):
    outside_state = gathered_before(got, position[0])[0]
    incoming = jnp.exp(inner_total[0:1]) * outside_state + inner_state[...]
    projected = jnp.dot(normed[...], weights[...], preferred_element_type=F32)
    projected = projected.astype(BF16).astype(F32)
    queries = jax.nn.silu(projected[:, :HEAD_K])
    gate_act = jax.nn.silu(projected[:, HEAD_K:])
    causal = causal_mask()
    for n in range(starts.shape[0]):
        at = slice(n * BLOCK, (n + 1) * BLOCK)
        query = (queries[at] * jnp.exp(totals[at])).astype(BF16)
        scores = jnp.where(causal, dot_nt(query, key[at]), 0.0).astype(BF16)
        state = jnp.exp(befores[n : n + 1]) * incoming + starts[n].astype(F32)
        recur = jnp.dot(scores, value[at], preferred_element_type=F32)
        recur = recur + dot_nt(query, state.astype(BF16))
        scaling = lax.rsqrt(jnp.mean(recur * recur, axis=1, keepdims=True) + 1e-06)
        out[at] = (recur * scaling * gain[...] * gate_act[at]).astype(BF16)


def conv_body(halo, normed, weights, taps, conv, stats, shifted):
    channels = conv.shape[1]
    rows = conv.shape[0]
    filled = HALO + rows
    extended = jnp.concatenate([halo[...], normed[...]], axis=0)
    projected = jnp.dot(extended, weights[...], preferred_element_type=F32)
    projected = projected.astype(BF16).astype(F32)
    glu = projected[:, :channels] * jax.nn.sigmoid(projected[:, channels:])
    shifted[0, :filled] = glu.astype(BF16).astype(F32)
    for r in range(1, 8):
        shifted[r, : filled - 8] = shifted[0, r : filled - 8 + r]
    first = HALO - (KERNEL - 1)
    step = 32
    for row in range(0, rows, step):
        accum = jnp.zeros((step, channels), F32)
        for tap in range(KERNEL):
            off = row + first + tap
            base = off // 8 * 8
            accum = accum + taps[tap : tap + 1] * shifted[off - base, base : base + step]
        conv[row : row + step] = accum
    summed = conv[...]
    ones = jnp.ones((8, channels), F32)

    def over_channels(value):
        return lax.dot_general(
            ones, value, (((1,), (1,)), ((), ())), precision=EXACT, preferred_element_type=F32
        )

    row = lax.broadcasted_iota(jnp.int32, (8, rows), 0)
    both = jnp.where(row == 0, over_channels(summed), over_channels(summed * summed))[0:2]
    for k in range(stats.shape[0]):
        stats[k] = both


def out_body(core, stats, conv, head_out, ln_gain, ln_bias, w_rec, w_low, w_high, rows_out, out):
    channels = conv.shape[1]
    share = conv.shape[0] // stats.shape[0]
    both = stats[0]
    for k in range(1, stats.shape[0]):
        both = both + stats[k]
    both = both / (channels * stats.shape[0])
    mean = both[0:1]
    inverse = lax.rsqrt(both[1:2] - mean * mean + 1e-05)
    row = lax.broadcasted_iota(jnp.int32, (8, both.shape[1]), 0)
    paired = jnp.where(row == 0, mean, jnp.where(row == 1, inverse, 0.0))

    def column(k):
        chosen = jnp.where(lax.broadcasted_iota(jnp.int32, (8, channels), 0) == k, 1.0, 0.0)
        return lax.dot_general(
            paired,
            chosen.astype(F32),
            (((0,), (0,)), ((), ())),
            precision=EXACT,
            preferred_element_type=F32,
        )

    normal = (conv[...] - column(0)) * column(1) * ln_gain[...] + ln_bias[...]
    conv_out = jax.nn.silu(normal).astype(BF16)
    for k in range(stats.shape[0]):
        piece = slice(k * share, (k + 1) * share)
        at = slice(k // 2 * share, (k // 2 + 1) * share)
        rows_out[k % 2, at, :HEAD_K] = head_out[piece]
        rows_out[k % 2, at, HEAD_K:] = conv_out[piece]
    out[...] = product(rows_out[1 - core[0]], w_rec, w_low, w_high)


def product(rows, w_rec, w_low, w_high):
    mixed = dot_nt(rows[:, :HEAD_K], w_rec[...])
    mixed = mixed + dot_nt(rows[:, HEAD_K : 2 * HEAD_K], w_low[...])
    mixed = mixed + dot_nt(rows[:, 2 * HEAD_K :], w_high[...])
    return mixed.astype(BF16)


def own_body(core, rows, w_rec, w_low, w_high, out):
    out[...] = product(rows[core[0]], w_rec, w_low, w_high)


def swap(value, axis):
    return lax.all_to_all(value, axis, split_axis=0, concat_axis=0, tiled=True)


def shifted_around(value, axis):
    count = lax.axis_size(axis)
    pieces = [value]
    for k in range(1, count):
        pieces.append(lax.ppermute(value, axis, [(n, (n + k) % count) for n in range(count)]))
    return pieces, (lax.axis_index(axis) + count - jnp.arange(count, dtype=jnp.int32)) % count


def on_device(
    tokens,
    norm_gain,
    w_query,
    w_forget,
    w_value,
    w_outgate,
    leak,
    decay_shift,
    head_gain,
    w_glu_value,
    w_glu_gate,
    conv_kernel,
    ln_gain,
    ln_bias,
    w_out_rec,
    w_out_conv,
):
    shape = jax.ShapeDtypeStruct
    smem = pl.BlockSpec(memory_space=pltpu.SMEM)
    inner_count = lax.axis_size(SP[1])
    group = lax.axis_size(TP)
    share, features = tokens.shape
    depth = w_query.shape[0]
    channels = conv_kernel.shape[1]
    columns = (w_glu_value, w_glu_gate, w_query, w_outgate, w_out_rec.T, w_out_conv.T)
    glu_width = 2 * channels
    all_width = sum(w.shape[1] for w in columns)
    copies = call(first_body, shape((inner_count, depth, all_width), BF16), *columns)
    staged = swap(copies, SP[1]).reshape(inner_count * depth, all_width)
    gathered = lax.all_gather(staged, SP[0], axis=0, tiled=True)
    count = lax.axis_size(SP)
    copies = call(
        second_body, shape((count, depth, 2 * HEAD_K), BF16), w_forget, w_value
    )
    state_weights = swap(copies, SP).reshape(count * depth, 2 * HEAD_K)
    pieces, places = shifted_around(tokens, TP)
    rows = group * share
    normed, tail = call(
        norm_body,
        (shape((rows, features), BF16), shape((share, features), BF16)),
        places,
        norm_gain.reshape(1, -1),
        *pieces,
        in_specs=[smem] + whole(1 + len(pieces)),
    )
    count = lax.axis_size(SP)
    halo = lax.ppermute(tail, SP, [(k, k + 1) for k in range(count - 1)])
    message = shape((inner_count, HEAD_K + 8, HEAD_K), BF16)
    blocks = rows // BLOCK
    sent, *kept = call(
        state_body,
        (
            message,
            shape((rows, HEAD_K), BF16),
            shape((rows, HEAD_K), BF16),
            shape((rows, HEAD_K), F32),
            shape((blocks, HEAD_K, HEAD_K), BF16),
            shape((blocks, HEAD_K), F32),
        ),
        normed,
        state_weights,
        leak.reshape(1, -1),
        decay_shift,
    )
    sent, inner_state, inner_total = call(
        inner_body,
        (message, shape((HEAD_K, HEAD_K), F32), shape((8, HEAD_K), F32)),
        lax.axis_index(SP[1]).reshape(1),
        swap(sent, SP[1]),
        in_specs=[smem] + whole(1),
    )

    def part(size, at):
        return pl.BlockSpec((gathered.shape[0], size), lambda k: (0, at))

    def full(*lengths):
        return pl.BlockSpec(lengths, lambda k: (0,) * len(lengths))

    conv, stats = call(
        conv_body,
        (shape((rows, channels), F32), shape((group, 2, rows), F32)),
        halo,
        normed,
        gathered,
        conv_kernel,
        grid=(1,),
        in_specs=[
            full(*halo.shape),
            full(*normed.shape),
            part(glu_width, 0),
            full(*conv_kernel.shape),
        ],
        out_specs=(full(rows, channels), full(group, 2, rows)),
        scratch=(pltpu.VMEM((8, HALO + rows, channels), F32),),
    )
    stats = swap(stats, TP)
    outer_sent = swap(sent, SP[0])
    head_gain = head_gain.reshape(1, -1)
    head_out = call(
        outer_body,
        shape((rows, HEAD_K), BF16),
        lax.axis_index(SP[0]).reshape(1),
        outer_sent,
        inner_state,
        inner_total,
        normed,
        gathered,
        *kept,
        head_gain,
        grid=(1,),
        in_specs=[
            smem,
            *[full(*a.shape) for a in (outer_sent, inner_state, inner_total, normed)],
            part(2 * HEAD_K, glu_width // (2 * HEAD_K)),
            *[full(*a.shape) for a in kept],
            full(*head_gain.shape),
        ],
        out_specs=full(rows, HEAD_K),
    )
    first = glu_width // HEAD_K + 2
    half = rows // 2
    width = HEAD_K + channels
    core = lax.axis_index(TP[1]).reshape(1)
    weights = [gathered] * 3
    weight_specs = [part(HEAD_K, first + k) for k in range(3)]
    mixed_rows, sent = call(
        out_body,
        (shape((2, half, width), BF16), shape((half, features), BF16)),
        core,
        stats,
        conv,
        head_out,
        ln_gain.reshape(1, -1),
        ln_bias.reshape(1, -1),
        *weights,
        grid=(1,),
        in_specs=[
            smem,
            full(*stats.shape),
            full(rows, channels),
            full(rows, HEAD_K),
            full(1, channels),
            full(1, channels),
            *weight_specs,
        ],
        out_specs=(full(2, half, width), full(half, features)),
    )
    received = lax.ppermute(sent, TP[1], [(0, 1), (1, 0)])
    own = call(
        own_body,
        shape((half, features), BF16),
        core,
        mixed_rows,
        *weights,
        grid=(1,),
        in_specs=[smem, full(2, half, width), *weight_specs],
        out_specs=full(half, features),
    )
    pair = (own.astype(F32) + received.astype(F32)).astype(BF16)
    arrived = swap(pair.reshape(group // 2, share, features), TP[0])
    return arrived.astype(F32).sum(axis=0).astype(BF16)


def solution(mesh):
    torus = Mesh(mesh.devices.reshape(8, 8, mesh.shape["tp"] // 2, 2), SP_TP)
    placed = (
        P(SP_TP, None),
        P(),
        P(SP, TP),
        P(SP, TP),
        P(SP, TP),
        P(SP, TP),
        P(TP),
        P(SP, TP),
        P(),
        P(SP, TP),
        P(SP, TP),
        P(None, TP),
        P(TP),
        P(TP),
        P(TP, SP),
        P(TP, SP),
    )

    return jax.shard_map(
        on_device, mesh=torus, in_specs=placed, out_specs=P(SP_TP, None), check_vma=False
    )
```

```python
import jax
import jax.numpy as jnp
from jax import lax
from jax.experimental import pallas as pl
from jax.experimental.pallas import tpu as pltpu
from jax.sharding import Mesh
from jax.sharding import PartitionSpec as P

HEAD_K = 128
KERNEL = 31
BLOCK = 64
HALO = 32
SP = ("sp_0", "sp_1")
TP = ("x", "core")
SP_TP = SP + TP
F32 = jnp.float32
BF16 = jnp.bfloat16
EXACT = lax.Precision.HIGHEST


def dot_nt(a, b):
    return lax.dot_general(a, b, (((1,), (1,)), ((), ())), preferred_element_type=F32)


def dot_tn(a, b):
    return lax.dot_general(a, b, (((0,), (0,)), ((), ())), preferred_element_type=F32)


def call(body, outs, *args, grid=None, in_specs=None, out_specs=None, scratch=()):
    specs = {}
    if in_specs is not None:
        specs["in_specs"] = in_specs
    if out_specs is not None:
        specs["out_specs"] = out_specs
    if grid is not None:
        specs["grid"] = grid
    return pl.pallas_call(body, out_shape=outs, scratch_shapes=scratch, **specs)(*args)


def whole(count):
    return [pl.BlockSpec(memory_space=pltpu.VMEM)] * count


def first_body(gv, gg, q, g, wr, wc, f, v, operand, copies):
    operand[...] = jnp.concatenate([w[...] for w in (gv, gg, q, g, wr, wc)], axis=1)
    joined = jnp.concatenate([f[...], v[...]], axis=1)
    for k in range(copies.shape[0]):
        copies[k] = joined


def again_body(value, copies):
    for k in range(copies.shape[0]):
        copies[k] = value[...]


def norm_body(places, gain, *refs):
    *pieces, out, tail = refs
    share = tail.shape[0]
    for n, piece in enumerate(pieces):
        values_in = piece[...].astype(F32)
        row_scale = lax.rsqrt(jnp.mean(values_in * values_in, axis=1, keepdims=True) + 1e-06)
        scaled = (values_in * row_scale * gain[...]).astype(BF16)
        out[pl.ds(pl.multiple_of(places[n] * share, share), share)] = scaled
    tail[...] = out[out.shape[0] - share :]


def pack_state(out, state, total):
    high = total.astype(BF16).astype(F32)
    row = lax.broadcasted_iota(jnp.int32, (8, total.shape[1]), 0)
    tail = jnp.where(row == 0, high, jnp.where(row == 1, total - high, 0.0)).astype(BF16)
    state = state.astype(BF16)
    width = state.shape[0]
    for k in range(out.shape[0]):
        out[k, :width] = state
        out[k, width:] = tail


def causal_mask():
    at_row = lax.broadcasted_iota(jnp.int32, (BLOCK, BLOCK), 0)
    at_col = lax.broadcasted_iota(jnp.int32, (BLOCK, BLOCK), 1)
    return at_row >= at_col


def state_body(normed, weights, leak, shift, sent, value_out, key, totals, starts, befores):
    rows = normed.shape[0]
    peers = weights.shape[0]
    ordered = jnp.concatenate(
        [weights[inner, outer] for outer in range(weights.shape[1]) for inner in range(peers)],
        axis=0,
    )
    projected = jnp.dot(normed[...], ordered, preferred_element_type=F32).astype(BF16)
    value = projected[:, HEAD_K:]
    value_out[...] = value
    in_gate = leak[...] * jax.nn.sigmoid(-projected[:, :HEAD_K].astype(F32))
    log_decay = jnp.log1p(-in_gate) + shift[...]
    triangle = jnp.where(causal_mask(), 1.0, 0.0).astype(F32)
    state = jnp.zeros((HEAD_K, HEAD_K), F32)
    before = jnp.zeros((1, HEAD_K), F32)
    kept = []
    for n in range(rows // BLOCK):
        at = slice(n * BLOCK, (n + 1) * BLOCK)
        total = jnp.dot(triangle, log_decay[at], precision=EXACT, preferred_element_type=F32)
        last = total[BLOCK - 1 :]
        totals[at] = total
        key[at] = (in_gate[at] * jnp.exp(-total)).astype(BF16)
        starts[n] = state.astype(BF16)
        kept.append(before)
        late_key = (in_gate[at] * jnp.exp(last - total)).astype(BF16)
        state = jnp.exp(last) * state + dot_tn(value[at], late_key)
        before = before + last
    befores[...] = jnp.concatenate(kept, axis=0)
    pack_state(sent, state, before)


def unpack(got, k):
    tail = got[k, HEAD_K:].astype(F32)
    return got[k, :HEAD_K].astype(F32), tail[0:1] + tail[1:2]


def gathered_before(got, position):
    state = inside_state = jnp.zeros((HEAD_K, HEAD_K), F32)
    total = inside_total = jnp.zeros((1, HEAD_K), F32)
    for k in range(got.shape[0]):
        passed = k < position
        new_state, new_total = unpack(got, k)
        state = jnp.exp(new_total) * state + new_state
        total = total + new_total
        inside_state = jnp.where(passed, state, inside_state)
        inside_total = jnp.where(passed, total, inside_total)
    return inside_state, inside_total, state, total


def inner_body(position, got, sent, inner_state, inner_total):
    inside_state, inside_total, state, total = gathered_before(got, position[0])
    inner_state[...] = inside_state
    inner_total[...] = jnp.broadcast_to(inside_total, inner_total.shape)
    pack_state(sent, state, total)


def outer_body(
    position,
    got,
    inner_state,
    inner_total,
    normed,
    weights,
    value,
    key,
    totals,
    starts,
    befores,
    gain,
    out,
):
    outside_state = gathered_before(got, position[0])[0]
    incoming = jnp.exp(inner_total[0:1]) * outside_state + inner_state[...]
    projected = jnp.dot(normed[...], weights[...], preferred_element_type=F32)
    projected = projected.astype(BF16).astype(F32)
    queries = jax.nn.silu(projected[:, :HEAD_K])
    gate_act = jax.nn.silu(projected[:, HEAD_K:])
    causal = causal_mask()
    for n in range(starts.shape[0]):
        at = slice(n * BLOCK, (n + 1) * BLOCK)
        query = (queries[at] * jnp.exp(totals[at])).astype(BF16)
        scores = jnp.where(causal, dot_nt(query, key[at]), 0.0).astype(BF16)
        state = jnp.exp(befores[n : n + 1]) * incoming + starts[n].astype(F32)
        recur = jnp.dot(scores, value[at], preferred_element_type=F32)
        recur = recur + dot_nt(query, state.astype(BF16))
        scaling = lax.rsqrt(jnp.mean(recur * recur, axis=1, keepdims=True) + 1e-06)
        out[at] = (recur * scaling * gain[...] * gate_act[at]).astype(BF16)


def conv_body(halo, normed, weights, taps, conv, stats, shifted):
    channels = conv.shape[1]
    rows = conv.shape[0]
    filled = HALO + rows
    extended = jnp.concatenate([halo[...], normed[...]], axis=0)
    projected = jnp.dot(extended, weights[...], preferred_element_type=F32)
    projected = projected.astype(BF16).astype(F32)
    glu = projected[:, :channels] * jax.nn.sigmoid(projected[:, channels:])
    shifted[0, :filled] = glu.astype(BF16).astype(F32)
    for r in range(1, 8):
        shifted[r, : filled - 8] = shifted[0, r : filled - 8 + r]
    first = HALO - (KERNEL - 1)
    step = 32
    for row in range(0, rows, step):
        accum = jnp.zeros((step, channels), F32)
        for tap in range(KERNEL):
            off = row + first + tap
            base = off // 8 * 8
            accum = accum + taps[tap : tap + 1] * shifted[off - base, base : base + step]
        conv[row : row + step] = accum
    summed = conv[...]
    ones = jnp.ones((8, channels), F32)

    def over_channels(value):
        return lax.dot_general(
            ones, value, (((1,), (1,)), ((), ())), precision=EXACT, preferred_element_type=F32
        )

    row = lax.broadcasted_iota(jnp.int32, (8, rows), 0)
    both = jnp.where(row == 0, over_channels(summed), over_channels(summed * summed))[0:2]
    for k in range(stats.shape[0]):
        stats[k] = both


def out_body(core, stats, conv, head_out, ln_gain, ln_bias, w_rec, w_low, w_high, out, own, rows_out):
    channels = conv.shape[1]
    share = conv.shape[0] // stats.shape[0]
    both = stats[0]
    for k in range(1, stats.shape[0]):
        both = both + stats[k]
    both = both / (channels * stats.shape[0])
    mean = both[0:1]
    inverse = lax.rsqrt(both[1:2] - mean * mean + 1e-05)
    row = lax.broadcasted_iota(jnp.int32, (8, both.shape[1]), 0)
    paired = jnp.where(row == 0, mean, jnp.where(row == 1, inverse, 0.0))

    def column(k):
        chosen = jnp.where(lax.broadcasted_iota(jnp.int32, (8, channels), 0) == k, 1.0, 0.0)
        return lax.dot_general(
            paired,
            chosen.astype(F32),
            (((0,), (0,)), ((), ())),
            precision=EXACT,
            preferred_element_type=F32,
        )

    normal = (conv[...] - column(0)) * column(1) * ln_gain[...] + ln_bias[...]
    conv_out = jax.nn.silu(normal).astype(BF16)
    for k in range(stats.shape[0]):
        piece = slice(k * share, (k + 1) * share)
        at = slice(k // 2 * share, (k // 2 + 1) * share)
        rows_out[k % 2, at, :HEAD_K] = head_out[piece]
        rows_out[k % 2, at, HEAD_K:] = conv_out[piece]
    out[...] = product(rows_out[1 - core[0]], w_rec, w_low, w_high)
    own[...] = product(rows_out[core[0]], w_rec, w_low, w_high)


def product(rows, w_rec, w_low, w_high):
    mixed = dot_nt(rows[:, :HEAD_K], w_rec[...])
    mixed = mixed + dot_nt(rows[:, HEAD_K : 2 * HEAD_K], w_low[...])
    mixed = mixed + dot_nt(rows[:, 2 * HEAD_K :], w_high[...])
    return mixed.astype(BF16)


def swap(value, axis):
    return lax.all_to_all(value, axis, split_axis=0, concat_axis=0, tiled=True)


def shifted_around(value, axis):
    count = lax.axis_size(axis)
    pieces = [value]
    for k in range(1, count):
        pieces.append(lax.ppermute(value, axis, [(n, (n + k) % count) for n in range(count)]))
    return pieces, (lax.axis_index(axis) + count - jnp.arange(count, dtype=jnp.int32)) % count


def on_device(
    tokens,
    norm_gain,
    w_query,
    w_forget,
    w_value,
    w_outgate,
    leak,
    decay_shift,
    head_gain,
    w_glu_value,
    w_glu_gate,
    conv_kernel,
    ln_gain,
    ln_bias,
    w_out_rec,
    w_out_conv,
):
    shape = jax.ShapeDtypeStruct
    smem = pl.BlockSpec(memory_space=pltpu.SMEM)
    inner_count = lax.axis_size(SP[1])
    group = lax.axis_size(TP)
    share, features = tokens.shape
    depth = w_query.shape[0]
    channels = conv_kernel.shape[1]
    columns = (w_glu_value, w_glu_gate, w_query, w_outgate, w_out_rec.T, w_out_conv.T)
    glu_width = 2 * channels
    all_width = sum(w.shape[1] for w in columns)
    outer_count = lax.axis_size(SP[0])
    operand, copies = call(
        first_body,
        (
            shape((depth, all_width), BF16),
            shape((outer_count, depth, 2 * HEAD_K), BF16),
        ),
        *columns,
        w_forget,
        w_value,
    )
    gathered = lax.all_gather(operand, SP, axis=0, tiled=True)
    column = swap(copies, SP[0])
    copies = call(again_body, shape((inner_count, *column.shape), BF16), column)
    state_weights = swap(copies, SP[1])
    pieces, places = shifted_around(tokens, TP)
    rows = group * share
    normed, tail = call(
        norm_body,
        (shape((rows, features), BF16), shape((share, features), BF16)),
        places,
        norm_gain.reshape(1, -1),
        *pieces,
        in_specs=[smem] + whole(1 + len(pieces)),
    )
    count = lax.axis_size(SP)
    halo = lax.ppermute(tail, SP, [(k, k + 1) for k in range(count - 1)])
    message = shape((inner_count, HEAD_K + 8, HEAD_K), BF16)
    blocks = rows // BLOCK
    sent, *kept = call(
        state_body,
        (
            message,
            shape((rows, HEAD_K), BF16),
            shape((rows, HEAD_K), BF16),
            shape((rows, HEAD_K), F32),
            shape((blocks, HEAD_K, HEAD_K), BF16),
            shape((blocks, HEAD_K), F32),
        ),
        normed,
        state_weights,
        leak.reshape(1, -1),
        decay_shift,
    )
    sent, inner_state, inner_total = call(
        inner_body,
        (message, shape((HEAD_K, HEAD_K), F32), shape((8, HEAD_K), F32)),
        lax.axis_index(SP[1]).reshape(1),
        swap(sent, SP[1]),
        in_specs=[smem] + whole(1),
    )

    def part(size, at):
        return pl.BlockSpec((gathered.shape[0], size), lambda k: (0, at))

    def full(*lengths):
        return pl.BlockSpec(lengths, lambda k: (0,) * len(lengths))

    conv, stats = call(
        conv_body,
        (shape((rows, channels), F32), shape((group, 2, rows), F32)),
        halo,
        normed,
        gathered,
        conv_kernel,
        grid=(1,),
        in_specs=[
            full(*halo.shape),
            full(*normed.shape),
            part(glu_width, 0),
            full(*conv_kernel.shape),
        ],
        out_specs=(full(rows, channels), full(group, 2, rows)),
        scratch=(pltpu.VMEM((8, HALO + rows, channels), F32),),
    )
    stats = swap(stats, TP)
    outer_sent = swap(sent, SP[0])
    head_gain = head_gain.reshape(1, -1)
    head_out = call(
        outer_body,
        shape((rows, HEAD_K), BF16),
        lax.axis_index(SP[0]).reshape(1),
        outer_sent,
        inner_state,
        inner_total,
        normed,
        gathered,
        *kept,
        head_gain,
        grid=(1,),
        in_specs=[
            smem,
            *[full(*a.shape) for a in (outer_sent, inner_state, inner_total, normed)],
            part(2 * HEAD_K, glu_width // (2 * HEAD_K)),
            *[full(*a.shape) for a in kept],
            full(*head_gain.shape),
        ],
        out_specs=full(rows, HEAD_K),
    )
    first = glu_width // HEAD_K + 2
    half = rows // 2
    width = HEAD_K + channels
    core = lax.axis_index(TP[1]).reshape(1)
    weights = [gathered] * 3
    weight_specs = [part(HEAD_K, first + k) for k in range(3)]
    sent, own = call(
        out_body,
        (shape((half, features), BF16),) * 2,
        core,
        stats,
        conv,
        head_out,
        ln_gain.reshape(1, -1),
        ln_bias.reshape(1, -1),
        *weights,
        grid=(1,),
        in_specs=[
            smem,
            full(*stats.shape),
            full(rows, channels),
            full(rows, HEAD_K),
            full(1, channels),
            full(1, channels),
            *weight_specs,
        ],
        out_specs=(full(half, features),) * 2,
        scratch=(pltpu.VMEM((2, half, width), BF16),),
    )
    received = lax.ppermute(sent, TP[1], [(0, 1), (1, 0)])
    pair = (own.astype(F32) + received.astype(F32)).astype(BF16)
    arrived = swap(pair.reshape(group // 2, share, features), TP[0])
    return arrived.astype(F32).sum(axis=0).astype(BF16)


def solution(mesh):
    torus = Mesh(mesh.devices.reshape(8, 8, mesh.shape["tp"] // 2, 2), SP_TP)
    placed = (
        P(SP_TP, None),
        P(),
        P(SP, TP),
        P(SP, TP),
        P(SP, TP),
        P(SP, TP),
        P(TP),
        P(SP, TP),
        P(),
        P(SP, TP),
        P(SP, TP),
        P(None, TP),
        P(TP),
        P(TP),
        P(TP, SP),
        P(TP, SP),
    )

    return jax.shard_map(
        on_device, mesh=torus, in_specs=placed, out_specs=P(SP_TP, None), check_vma=False
    )
```

```python
import jax
import jax.numpy as jnp
from jax import lax
from jax.experimental import pallas as pl
from jax.experimental.pallas import tpu as pltpu
from jax.sharding import Mesh
from jax.sharding import PartitionSpec as P

HEAD_K = 128
KERNEL = 31
BLOCK = 64
HALO = 32
SP = ("sp_0", "sp_1")
TP = ("x", "core")
SP_TP = SP + TP
F32 = jnp.float32
BF16 = jnp.bfloat16
EXACT = lax.Precision.HIGHEST


def dot_nt(a, b):
    return lax.dot_general(a, b, (((1,), (1,)), ((), ())), preferred_element_type=F32)


def dot_tn(a, b):
    return lax.dot_general(a, b, (((0,), (0,)), ((), ())), preferred_element_type=F32)


def call(body, outs, *args, grid=None, in_specs=None, out_specs=None, scratch=()):
    specs = {}
    if in_specs is not None:
        specs["in_specs"] = in_specs
    if out_specs is not None:
        specs["out_specs"] = out_specs
    if grid is not None:
        specs["grid"] = grid
    return pl.pallas_call(body, out_shape=outs, scratch_shapes=scratch, **specs)(*args)


def whole(count):
    return [pl.BlockSpec(memory_space=pltpu.VMEM)] * count


def first_body(gv, gg, q, g, wr, wc, f, v, operand, copies):
    operand[...] = jnp.concatenate([w[...] for w in (gv, gg, q, g, wr, wc)], axis=1)
    joined = jnp.concatenate([f[...], v[...]], axis=1)
    for k in range(copies.shape[0]):
        copies[k] = joined


def again_body(value, copies):
    for k in range(copies.shape[0]):
        copies[k] = value[...]


def norm_body(places, gain, *refs):
    *pieces, out, tail = refs
    share = tail.shape[0]
    for n, piece in enumerate(pieces):
        values_in = piece[...].astype(F32)
        row_scale = lax.rsqrt(jnp.mean(values_in * values_in, axis=1, keepdims=True) + 1e-06)
        scaled = (values_in * row_scale * gain[...]).astype(BF16)
        out[pl.ds(pl.multiple_of(places[n] * share, share), share)] = scaled
    tail[...] = out[out.shape[0] - share :]


def pack_state(out, state, total):
    high = total.astype(BF16).astype(F32)
    row = lax.broadcasted_iota(jnp.int32, (8, total.shape[1]), 0)
    tail = jnp.where(row == 0, high, jnp.where(row == 1, total - high, 0.0)).astype(BF16)
    state = state.astype(BF16)
    width = state.shape[0]
    for k in range(out.shape[0]):
        out[k, :width] = state
        out[k, width:] = tail


def causal_mask():
    at_row = lax.broadcasted_iota(jnp.int32, (BLOCK, BLOCK), 0)
    at_col = lax.broadcasted_iota(jnp.int32, (BLOCK, BLOCK), 1)
    return at_row >= at_col


def state_body(normed, weights, leak, shift, sent, value_out, key, totals, starts, befores):
    rows = normed.shape[0]
    projected = jnp.dot(normed[...], weights[...], preferred_element_type=F32).astype(BF16)
    value = projected[:, HEAD_K:]
    value_out[...] = value
    in_gate = leak[...] * jax.nn.sigmoid(-projected[:, :HEAD_K].astype(F32))
    log_decay = jnp.log1p(-in_gate) + shift[...]
    triangle = jnp.where(causal_mask(), 1.0, 0.0).astype(F32)
    state = jnp.zeros((HEAD_K, HEAD_K), F32)
    before = jnp.zeros((1, HEAD_K), F32)
    kept = []
    for n in range(rows // BLOCK):
        at = slice(n * BLOCK, (n + 1) * BLOCK)
        total = jnp.dot(triangle, log_decay[at], precision=EXACT, preferred_element_type=F32)
        last = total[BLOCK - 1 :]
        totals[at] = total
        key[at] = (in_gate[at] * jnp.exp(-total)).astype(BF16)
        starts[n] = state.astype(BF16)
        kept.append(before)
        late_key = (in_gate[at] * jnp.exp(last - total)).astype(BF16)
        state = jnp.exp(last) * state + dot_tn(value[at], late_key)
        before = before + last
    befores[...] = jnp.concatenate(kept, axis=0)
    pack_state(sent, state, before)


def unpack(got, k):
    tail = got[k, HEAD_K:].astype(F32)
    return got[k, :HEAD_K].astype(F32), tail[0:1] + tail[1:2]


def gathered_before(got, position):
    state = inside_state = jnp.zeros((HEAD_K, HEAD_K), F32)
    total = inside_total = jnp.zeros((1, HEAD_K), F32)
    for k in range(got.shape[0]):
        passed = k < position
        new_state, new_total = unpack(got, k)
        state = jnp.exp(new_total) * state + new_state
        total = total + new_total
        inside_state = jnp.where(passed, state, inside_state)
        inside_total = jnp.where(passed, total, inside_total)
    return inside_state, inside_total, state, total


def inner_body(position, got, sent, inner_state, inner_total):
    inside_state, inside_total, state, total = gathered_before(got, position[0])
    inner_state[...] = inside_state
    inner_total[...] = jnp.broadcast_to(inside_total, inner_total.shape)
    pack_state(sent, state, total)


def outer_body(
    position,
    got,
    inner_state,
    inner_total,
    normed,
    weights,
    value,
    key,
    totals,
    starts,
    befores,
    gain,
    out,
):
    outside_state = gathered_before(got, position[0])[0]
    incoming = jnp.exp(inner_total[0:1]) * outside_state + inner_state[...]
    projected = jnp.dot(normed[...], weights[...], preferred_element_type=F32)
    projected = projected.astype(BF16).astype(F32)
    queries = jax.nn.silu(projected[:, :HEAD_K])
    gate_act = jax.nn.silu(projected[:, HEAD_K:])
    causal = causal_mask()
    for n in range(starts.shape[0]):
        at = slice(n * BLOCK, (n + 1) * BLOCK)
        query = (queries[at] * jnp.exp(totals[at])).astype(BF16)
        scores = jnp.where(causal, dot_nt(query, key[at]), 0.0).astype(BF16)
        state = jnp.exp(befores[n : n + 1]) * incoming + starts[n].astype(F32)
        recur = jnp.dot(scores, value[at], preferred_element_type=F32)
        recur = recur + dot_nt(query, state.astype(BF16))
        scaling = lax.rsqrt(jnp.mean(recur * recur, axis=1, keepdims=True) + 1e-06)
        out[at] = (recur * scaling * gain[...] * gate_act[at]).astype(BF16)


def conv_body(halo, normed, weights, taps, conv, stats, shifted):
    channels = conv.shape[1]
    rows = conv.shape[0]
    filled = HALO + rows
    extended = jnp.concatenate([halo[...], normed[...]], axis=0)
    projected = jnp.dot(extended, weights[...], preferred_element_type=F32)
    projected = projected.astype(BF16).astype(F32)
    glu = projected[:, :channels] * jax.nn.sigmoid(projected[:, channels:])
    shifted[0, :filled] = glu.astype(BF16).astype(F32)
    for r in range(1, 8):
        shifted[r, : filled - 8] = shifted[0, r : filled - 8 + r]
    first = HALO - (KERNEL - 1)
    step = 32
    for row in range(0, rows, step):
        accum = jnp.zeros((step, channels), F32)
        for tap in range(KERNEL):
            off = row + first + tap
            base = off // 8 * 8
            accum = accum + taps[tap : tap + 1] * shifted[off - base, base : base + step]
        conv[row : row + step] = accum
    summed = conv[...]
    ones = jnp.ones((8, channels), F32)

    def over_channels(value):
        return lax.dot_general(
            ones, value, (((1,), (1,)), ((), ())), precision=EXACT, preferred_element_type=F32
        )

    row = lax.broadcasted_iota(jnp.int32, (8, rows), 0)
    both = jnp.where(row == 0, over_channels(summed), over_channels(summed * summed))[0:2]
    for k in range(stats.shape[0]):
        stats[k] = both


def out_body(core, stats, conv, head_out, ln_gain, ln_bias, w_rec, w_low, w_high, out, own, rows_out):
    channels = conv.shape[1]
    share = conv.shape[0] // stats.shape[0]
    both = stats[0]
    for k in range(1, stats.shape[0]):
        both = both + stats[k]
    both = both / (channels * stats.shape[0])
    mean = both[0:1]
    inverse = lax.rsqrt(both[1:2] - mean * mean + 1e-05)
    row = lax.broadcasted_iota(jnp.int32, (8, both.shape[1]), 0)
    paired = jnp.where(row == 0, mean, jnp.where(row == 1, inverse, 0.0))

    def column(k):
        chosen = jnp.where(lax.broadcasted_iota(jnp.int32, (8, channels), 0) == k, 1.0, 0.0)
        return lax.dot_general(
            paired,
            chosen.astype(F32),
            (((0,), (0,)), ((), ())),
            precision=EXACT,
            preferred_element_type=F32,
        )

    normal = (conv[...] - column(0)) * column(1) * ln_gain[...] + ln_bias[...]
    conv_out = jax.nn.silu(normal).astype(BF16)
    for k in range(stats.shape[0]):
        piece = slice(k * share, (k + 1) * share)
        at = slice(k // 2 * share, (k // 2 + 1) * share)
        rows_out[k % 2, at, :HEAD_K] = head_out[piece]
        rows_out[k % 2, at, HEAD_K:] = conv_out[piece]
    out[...] = product(rows_out[1 - core[0]], w_rec, w_low, w_high)
    own[...] = product(rows_out[core[0]], w_rec, w_low, w_high)


def product(rows, w_rec, w_low, w_high):
    mixed = dot_nt(rows[:, :HEAD_K], w_rec[...])
    mixed = mixed + dot_nt(rows[:, HEAD_K : 2 * HEAD_K], w_low[...])
    mixed = mixed + dot_nt(rows[:, 2 * HEAD_K :], w_high[...])
    return mixed.astype(BF16)


def swap(value, axis):
    return lax.all_to_all(value, axis, split_axis=0, concat_axis=0, tiled=True)


def shifted_around(value, axis):
    count = lax.axis_size(axis)
    pieces = [value]
    for k in range(1, count):
        pieces.append(lax.ppermute(value, axis, [(n, (n + k) % count) for n in range(count)]))
    return pieces, (lax.axis_index(axis) + count - jnp.arange(count, dtype=jnp.int32)) % count


def on_device(
    tokens,
    norm_gain,
    w_query,
    w_forget,
    w_value,
    w_outgate,
    leak,
    decay_shift,
    head_gain,
    w_glu_value,
    w_glu_gate,
    conv_kernel,
    ln_gain,
    ln_bias,
    w_out_rec,
    w_out_conv,
):
    shape = jax.ShapeDtypeStruct
    smem = pl.BlockSpec(memory_space=pltpu.SMEM)
    inner_count = lax.axis_size(SP[1])
    group = lax.axis_size(TP)
    share, features = tokens.shape
    depth = w_query.shape[0]
    channels = conv_kernel.shape[1]
    columns = (w_glu_value, w_glu_gate, w_query, w_outgate, w_out_rec.T, w_out_conv.T)
    glu_width = 2 * channels
    all_width = sum(w.shape[1] for w in columns)
    outer_count = lax.axis_size(SP[0])
    operand, copies = call(
        first_body,
        (
            shape((depth, all_width), BF16),
            shape((inner_count, depth, 2 * HEAD_K), BF16),
        ),
        *columns,
        w_forget,
        w_value,
    )
    gathered = lax.all_gather(operand, SP, axis=0, tiled=True)
    column = swap(copies, SP[1])
    copies = call(again_body, shape((outer_count, *column.shape), BF16), column)
    state_weights = swap(copies, SP[0]).reshape(-1, 2 * HEAD_K)
    pieces, places = shifted_around(tokens, TP)
    rows = group * share
    normed, tail = call(
        norm_body,
        (shape((rows, features), BF16), shape((share, features), BF16)),
        places,
        norm_gain.reshape(1, -1),
        *pieces,
        in_specs=[smem] + whole(1 + len(pieces)),
    )
    count = lax.axis_size(SP)
    halo = lax.ppermute(tail, SP, [(k, k + 1) for k in range(count - 1)])
    message = shape((inner_count, HEAD_K + 8, HEAD_K), BF16)
    blocks = rows // BLOCK
    sent, *kept = call(
        state_body,
        (
            message,
            shape((rows, HEAD_K), BF16),
            shape((rows, HEAD_K), BF16),
            shape((rows, HEAD_K), F32),
            shape((blocks, HEAD_K, HEAD_K), BF16),
            shape((blocks, HEAD_K), F32),
        ),
        normed,
        state_weights,
        leak.reshape(1, -1),
        decay_shift,
    )
    sent, inner_state, inner_total = call(
        inner_body,
        (message, shape((HEAD_K, HEAD_K), F32), shape((8, HEAD_K), F32)),
        lax.axis_index(SP[1]).reshape(1),
        swap(sent, SP[1]),
        in_specs=[smem] + whole(1),
    )

    def part(size, at):
        return pl.BlockSpec((gathered.shape[0], size), lambda k: (0, at))

    def full(*lengths):
        return pl.BlockSpec(lengths, lambda k: (0,) * len(lengths))

    conv, stats = call(
        conv_body,
        (shape((rows, channels), F32), shape((group, 2, rows), F32)),
        halo,
        normed,
        gathered,
        conv_kernel,
        grid=(1,),
        in_specs=[
            full(*halo.shape),
            full(*normed.shape),
            part(glu_width, 0),
            full(*conv_kernel.shape),
        ],
        out_specs=(full(rows, channels), full(group, 2, rows)),
        scratch=(pltpu.VMEM((8, HALO + rows, channels), F32),),
    )
    stats = swap(stats, TP)
    outer_sent = swap(sent, SP[0])
    head_gain = head_gain.reshape(1, -1)
    head_out = call(
        outer_body,
        shape((rows, HEAD_K), BF16),
        lax.axis_index(SP[0]).reshape(1),
        outer_sent,
        inner_state,
        inner_total,
        normed,
        gathered,
        *kept,
        head_gain,
        grid=(1,),
        in_specs=[
            smem,
            *[full(*a.shape) for a in (outer_sent, inner_state, inner_total, normed)],
            part(2 * HEAD_K, glu_width // (2 * HEAD_K)),
            *[full(*a.shape) for a in kept],
            full(*head_gain.shape),
        ],
        out_specs=full(rows, HEAD_K),
    )
    first = glu_width // HEAD_K + 2
    half = rows // 2
    width = HEAD_K + channels
    core = lax.axis_index(TP[1]).reshape(1)
    weights = [gathered] * 3
    weight_specs = [part(HEAD_K, first + k) for k in range(3)]
    sent, own = call(
        out_body,
        (shape((half, features), BF16),) * 2,
        core,
        stats,
        conv,
        head_out,
        ln_gain.reshape(1, -1),
        ln_bias.reshape(1, -1),
        *weights,
        grid=(1,),
        in_specs=[
            smem,
            full(*stats.shape),
            full(rows, channels),
            full(rows, HEAD_K),
            full(1, channels),
            full(1, channels),
            *weight_specs,
        ],
        out_specs=(full(half, features),) * 2,
        scratch=(pltpu.VMEM((2, half, width), BF16),),
    )
    received = lax.ppermute(sent, TP[1], [(0, 1), (1, 0)])
    pair = (own.astype(F32) + received.astype(F32)).astype(BF16)
    arrived = swap(pair.reshape(group // 2, share, features), TP[0])
    return arrived.astype(F32).sum(axis=0).astype(BF16)


def solution(mesh):
    torus = Mesh(mesh.devices.reshape(8, 8, mesh.shape["tp"] // 2, 2), SP_TP)
    placed = (
        P(SP_TP, None),
        P(),
        P(SP, TP),
        P(SP, TP),
        P(SP, TP),
        P(SP, TP),
        P(TP),
        P(SP, TP),
        P(),
        P(SP, TP),
        P(SP, TP),
        P(None, TP),
        P(TP),
        P(TP),
        P(TP, SP),
        P(TP, SP),
    )

    return jax.shard_map(
        on_device, mesh=torus, in_specs=placed, out_specs=P(SP_TP, None), check_vma=False
    )
```

```python
import jax
import jax.numpy as jnp
from jax import lax
from jax.experimental import pallas as pl
from jax.experimental.pallas import tpu as pltpu
from jax.sharding import Mesh
from jax.sharding import PartitionSpec as P

HEAD_K = 128
KERNEL = 31
BLOCK = 64
HALO = 32
SP = ("sp_0", "sp_1")
TP = ("x", "core")
SP_TP = SP + TP
F32 = jnp.float32
BF16 = jnp.bfloat16
EXACT = lax.Precision.HIGHEST
ANY = pl.BlockSpec(memory_space=pl.ANY)


def dot_nt(a, b):
    return lax.dot_general(a, b, (((1,), (1,)), ((), ())), preferred_element_type=F32)


def dot_tn(a, b):
    return lax.dot_general(a, b, (((0,), (0,)), ((), ())), preferred_element_type=F32)


def call(body, outs, *args, grid=None, in_specs=None, out_specs=None, scratch=()):
    specs = {}
    if in_specs is not None:
        specs["in_specs"] = in_specs
    if out_specs is not None:
        specs["out_specs"] = out_specs
    if grid is not None:
        specs["grid"] = grid
    return pl.pallas_call(body, out_shape=outs, scratch_shapes=scratch, **specs)(*args)


def whole(count):
    return [pl.BlockSpec(memory_space=pltpu.VMEM)] * count


def first_body(gv, gg, q, g, wr, wc, f, v, operand, copies):
    operand[...] = jnp.concatenate([w[...] for w in (gv, gg, q, g, wr, wc)], axis=1)
    joined = jnp.concatenate([f[...], v[...]], axis=1)
    for k in range(copies.shape[0]):
        copies[k] = joined


def again_body(value, copies):
    for k in range(copies.shape[0]):
        copies[k] = value[...]


def norm_body(places, gain, *refs):
    *pieces, out, tail = refs
    share = tail.shape[0]
    for n, piece in enumerate(pieces):
        values_in = piece[...].astype(F32)
        row_scale = lax.rsqrt(jnp.mean(values_in * values_in, axis=1, keepdims=True) + 1e-06)
        scaled = (values_in * row_scale * gain[...]).astype(BF16)
        out[pl.ds(pl.multiple_of(places[n] * share, share), share)] = scaled
    tail[...] = out[out.shape[0] - share :]


def pack_state(out, state, total):
    high = total.astype(BF16).astype(F32)
    row = lax.broadcasted_iota(jnp.int32, (8, total.shape[1]), 0)
    tail = jnp.where(row == 0, high, jnp.where(row == 1, total - high, 0.0)).astype(BF16)
    state = state.astype(BF16)
    width = state.shape[0]
    for k in range(out.shape[0]):
        out[k, :width] = state
        out[k, width:] = tail


def causal_mask():
    at_row = lax.broadcasted_iota(jnp.int32, (BLOCK, BLOCK), 0)
    at_col = lax.broadcasted_iota(jnp.int32, (BLOCK, BLOCK), 1)
    return at_row >= at_col


def state_body(normed, weights, leak, shift, sent, value_out, key, totals, starts, befores):
    rows = normed.shape[0]
    projected = jnp.dot(normed[...], weights[...], preferred_element_type=F32).astype(BF16)
    value = projected[:, HEAD_K:]
    value_out[...] = value
    in_gate = leak[...] * jax.nn.sigmoid(-projected[:, :HEAD_K].astype(F32))
    log_decay = jnp.log1p(-in_gate) + shift[...]
    triangle = jnp.where(causal_mask(), 1.0, 0.0).astype(F32)
    state = jnp.zeros((HEAD_K, HEAD_K), F32)
    before = jnp.zeros((1, HEAD_K), F32)
    kept = []
    for n in range(rows // BLOCK):
        at = slice(n * BLOCK, (n + 1) * BLOCK)
        total = jnp.dot(triangle, log_decay[at], precision=EXACT, preferred_element_type=F32)
        last = total[BLOCK - 1 :]
        totals[at] = total
        key[at] = (in_gate[at] * jnp.exp(-total)).astype(BF16)
        starts[n] = state.astype(BF16)
        kept.append(before)
        late_key = (in_gate[at] * jnp.exp(last - total)).astype(BF16)
        state = jnp.exp(last) * state + dot_tn(value[at], late_key)
        before = before + last
    befores[...] = jnp.concatenate(kept, axis=0)
    pack_state(sent, state, before)


def unpack(got, k):
    tail = got[k, HEAD_K:].astype(F32)
    return got[k, :HEAD_K].astype(F32), tail[0:1] + tail[1:2]


def gathered_before(got, position):
    state = inside_state = jnp.zeros((HEAD_K, HEAD_K), F32)
    total = inside_total = jnp.zeros((1, HEAD_K), F32)
    for k in range(got.shape[0]):
        passed = k < position
        new_state, new_total = unpack(got, k)
        state = jnp.exp(new_total) * state + new_state
        total = total + new_total
        inside_state = jnp.where(passed, state, inside_state)
        inside_total = jnp.where(passed, total, inside_total)
    return inside_state, inside_total, state, total


def inner_body(position, got, sent, inner_state, inner_total):
    inside_state, inside_total, state, total = gathered_before(got, position[0])
    inner_state[...] = inside_state
    inner_total[...] = jnp.broadcast_to(inside_total, inner_total.shape)
    pack_state(sent, state, total)


def outer_body(
    position,
    got,
    inner_state,
    inner_total,
    normed,
    weights,
    value,
    key,
    totals,
    starts,
    befores,
    gain,
    out,
):
    outside_state = gathered_before(got, position[0])[0]
    incoming = jnp.exp(inner_total[0:1]) * outside_state + inner_state[...]
    projected = jnp.dot(normed[...], weights[...], preferred_element_type=F32)
    projected = projected.astype(BF16).astype(F32)
    queries = jax.nn.silu(projected[:, :HEAD_K])
    gate_act = jax.nn.silu(projected[:, HEAD_K:])
    causal = causal_mask()
    for n in range(starts.shape[0]):
        at = slice(n * BLOCK, (n + 1) * BLOCK)
        query = (queries[at] * jnp.exp(totals[at])).astype(BF16)
        scores = jnp.where(causal, dot_nt(query, key[at]), 0.0).astype(BF16)
        state = jnp.exp(befores[n : n + 1]) * incoming + starts[n].astype(F32)
        recur = jnp.dot(scores, value[at], preferred_element_type=F32)
        recur = recur + dot_nt(query, state.astype(BF16))
        scaling = lax.rsqrt(jnp.mean(recur * recur, axis=1, keepdims=True) + 1e-06)
        out[at] = (recur * scaling * gain[...] * gate_act[at]).astype(BF16)


def conv_body(halo, normed, gathered, taps, conv, stats, shifted, extended, weights, sems):
    channels = conv.shape[1]
    rows = conv.shape[0]
    filled = HALO + rows
    depth, width = weights.shape
    chunk = depth // 2
    chunks = [slice(k * chunk, (k + 1) * chunk) for k in range(2)]
    copies = [
        pltpu.make_async_copy(halo, extended.at[0:HALO], sems.at[0]),
        pltpu.make_async_copy(normed, extended.at[HALO:filled], sems.at[1]),
        *[
            pltpu.make_async_copy(gathered.at[at, 0:width], weights.at[at], sems.at[2 + k])
            for k, at in enumerate(chunks)
        ],
    ]
    for copy in copies:
        copy.start()
    for copy in copies[:3]:
        copy.wait()
    first_at, second_at = chunks
    projected = jnp.dot(extended[:, first_at], weights[first_at], preferred_element_type=F32)
    copies[3].wait()
    projected = projected + jnp.dot(
        extended[:, second_at], weights[second_at], preferred_element_type=F32
    )
    projected = projected.astype(BF16).astype(F32)
    glu = projected[:, :channels] * jax.nn.sigmoid(projected[:, channels:])
    shifted[0, :filled] = glu.astype(BF16).astype(F32)
    for r in range(1, 8):
        shifted[r, : filled - 8] = shifted[0, r : filled - 8 + r]
    first = HALO - (KERNEL - 1)
    step = 32
    for row in range(0, rows, step):
        accum = jnp.zeros((step, channels), F32)
        for tap in range(KERNEL):
            off = row + first + tap
            base = off // 8 * 8
            accum = accum + taps[tap : tap + 1] * shifted[off - base, base : base + step]
        conv[row : row + step] = accum
    summed = conv[...]
    ones = jnp.ones((8, channels), F32)

    def over_channels(value):
        return lax.dot_general(
            ones, value, (((1,), (1,)), ((), ())), precision=EXACT, preferred_element_type=F32
        )

    row = lax.broadcasted_iota(jnp.int32, (8, rows), 0)
    both = jnp.where(row == 0, over_channels(summed), over_channels(summed * summed))[0:2]
    for k in range(stats.shape[0]):
        stats[k] = both


def out_body(
    core, stats, conv, head_out, ln_gain, ln_bias, gathered, out, own, rows_out, weights, sem
):
    channels = conv.shape[1]
    share = conv.shape[0] // stats.shape[0]
    used = weights.shape[1]
    all_width = gathered.shape[1]
    copy = pltpu.make_async_copy(gathered.at[:, all_width - used : all_width], weights, sem)
    copy.start()
    both = stats[0]
    for k in range(1, stats.shape[0]):
        both = both + stats[k]
    both = both / (channels * stats.shape[0])
    mean = both[0:1]
    inverse = lax.rsqrt(both[1:2] - mean * mean + 1e-05)
    row = lax.broadcasted_iota(jnp.int32, (8, both.shape[1]), 0)
    paired = jnp.where(row == 0, mean, jnp.where(row == 1, inverse, 0.0))

    def column(k):
        chosen = jnp.where(lax.broadcasted_iota(jnp.int32, (8, channels), 0) == k, 1.0, 0.0)
        return lax.dot_general(
            paired,
            chosen.astype(F32),
            (((0,), (0,)), ((), ())),
            precision=EXACT,
            preferred_element_type=F32,
        )

    normal = (conv[...] - column(0)) * column(1) * ln_gain[...] + ln_bias[...]
    conv_out = jax.nn.silu(normal).astype(BF16)
    for k in range(stats.shape[0]):
        piece = slice(k * share, (k + 1) * share)
        at = slice(k // 2 * share, (k // 2 + 1) * share)
        rows_out[k % 2, at, :HEAD_K] = head_out[piece]
        rows_out[k % 2, at, HEAD_K:] = conv_out[piece]
    copy.wait()
    out[...] = dot_nt(rows_out[1 - core[0]], weights[...]).astype(BF16)
    own[...] = dot_nt(rows_out[core[0]], weights[...]).astype(BF16)


def swap(value, axis):
    return lax.all_to_all(value, axis, split_axis=0, concat_axis=0, tiled=True)


def shifted_around(value, axis):
    count = lax.axis_size(axis)
    pieces = [value]
    for k in range(1, count):
        pieces.append(lax.ppermute(value, axis, [(n, (n + k) % count) for n in range(count)]))
    return pieces, (lax.axis_index(axis) + count - jnp.arange(count, dtype=jnp.int32)) % count


def on_device(
    tokens,
    norm_gain,
    w_query,
    w_forget,
    w_value,
    w_outgate,
    leak,
    decay_shift,
    head_gain,
    w_glu_value,
    w_glu_gate,
    conv_kernel,
    ln_gain,
    ln_bias,
    w_out_rec,
    w_out_conv,
):
    shape = jax.ShapeDtypeStruct
    smem = pl.BlockSpec(memory_space=pltpu.SMEM)
    inner_count = lax.axis_size(SP[1])
    group = lax.axis_size(TP)
    share, features = tokens.shape
    depth = w_query.shape[0]
    channels = conv_kernel.shape[1]
    columns = (w_glu_value, w_glu_gate, w_query, w_outgate, w_out_rec.T, w_out_conv.T)
    glu_width = 2 * channels
    all_width = sum(w.shape[1] for w in columns)
    outer_count = lax.axis_size(SP[0])
    operand, copies = call(
        first_body,
        (
            shape((depth, all_width), BF16),
            shape((inner_count, depth, 2 * HEAD_K), BF16),
        ),
        *columns,
        w_forget,
        w_value,
    )
    gathered = lax.all_gather(operand, SP, axis=0, tiled=True)
    column = swap(copies, SP[1])
    copies = call(again_body, shape((outer_count, *column.shape), BF16), column)
    state_weights = swap(copies, SP[0]).reshape(-1, 2 * HEAD_K)
    pieces, places = shifted_around(tokens, TP)
    rows = group * share
    normed, tail = call(
        norm_body,
        (shape((rows, features), BF16), shape((share, features), BF16)),
        places,
        norm_gain.reshape(1, -1),
        *pieces,
        in_specs=[smem] + whole(1 + len(pieces)),
    )
    count = lax.axis_size(SP)
    halo = lax.ppermute(tail, SP, [(k, k + 1) for k in range(count - 1)])
    message = shape((inner_count, HEAD_K + 8, HEAD_K), BF16)
    blocks = rows // BLOCK
    sent, *kept = call(
        state_body,
        (
            message,
            shape((rows, HEAD_K), BF16),
            shape((rows, HEAD_K), BF16),
            shape((rows, HEAD_K), F32),
            shape((blocks, HEAD_K, HEAD_K), BF16),
            shape((blocks, HEAD_K), F32),
        ),
        normed,
        state_weights,
        leak.reshape(1, -1),
        decay_shift,
    )
    sent, inner_state, inner_total = call(
        inner_body,
        (message, shape((HEAD_K, HEAD_K), F32), shape((8, HEAD_K), F32)),
        lax.axis_index(SP[1]).reshape(1),
        swap(sent, SP[1]),
        in_specs=[smem] + whole(1),
    )

    def part(size, at):
        return pl.BlockSpec((gathered.shape[0], size), lambda k: (0, at))

    def full(*lengths):
        return pl.BlockSpec(lengths, lambda k: (0,) * len(lengths))

    conv, stats = call(
        conv_body,
        (shape((rows, channels), F32), shape((group, 2, rows), F32)),
        halo,
        normed,
        gathered,
        conv_kernel,
        grid=(1,),
        in_specs=[ANY, ANY, ANY, full(*conv_kernel.shape)],
        out_specs=(full(rows, channels), full(group, 2, rows)),
        scratch=(
            pltpu.VMEM((8, HALO + rows, channels), F32),
            pltpu.VMEM((HALO + rows, features), BF16),
            pltpu.VMEM((features, glu_width), BF16),
            pltpu.SemaphoreType.DMA((4,)),
        ),
    )
    stats = swap(stats, TP)
    outer_sent = swap(sent, SP[0])
    head_gain = head_gain.reshape(1, -1)
    head_out = call(
        outer_body,
        shape((rows, HEAD_K), BF16),
        lax.axis_index(SP[0]).reshape(1),
        outer_sent,
        inner_state,
        inner_total,
        normed,
        gathered,
        *kept,
        head_gain,
        grid=(1,),
        in_specs=[
            smem,
            *[full(*a.shape) for a in (outer_sent, inner_state, inner_total, normed)],
            part(2 * HEAD_K, glu_width // (2 * HEAD_K)),
            *[full(*a.shape) for a in kept],
            full(*head_gain.shape),
        ],
        out_specs=full(rows, HEAD_K),
    )
    half = rows // 2
    width = HEAD_K + channels
    core = lax.axis_index(TP[1]).reshape(1)
    sent, own = call(
        out_body,
        (shape((half, features), BF16),) * 2,
        core,
        stats,
        conv,
        head_out,
        ln_gain.reshape(1, -1),
        ln_bias.reshape(1, -1),
        gathered,
        grid=(1,),
        in_specs=[
            smem,
            full(*stats.shape),
            full(rows, channels),
            full(rows, HEAD_K),
            full(1, channels),
            full(1, channels),
            ANY,
        ],
        out_specs=(full(half, features),) * 2,
        scratch=(
            pltpu.VMEM((2, half, width), BF16),
            pltpu.VMEM((features, width), BF16),
            pltpu.SemaphoreType.DMA,
        ),
    )
    received = lax.ppermute(sent, TP[1], [(0, 1), (1, 0)])
    pair = (own.astype(F32) + received.astype(F32)).astype(BF16)
    arrived = swap(pair.reshape(group // 2, share, features), TP[0])
    return arrived.astype(F32).sum(axis=0).astype(BF16)


def solution(mesh):
    torus = Mesh(mesh.devices.reshape(8, 8, mesh.shape["tp"] // 2, 2), SP_TP)
    placed = (
        P(SP_TP, None),
        P(),
        P(SP, TP),
        P(SP, TP),
        P(SP, TP),
        P(SP, TP),
        P(TP),
        P(SP, TP),
        P(),
        P(SP, TP),
        P(SP, TP),
        P(None, TP),
        P(TP),
        P(TP),
        P(TP, SP),
        P(TP, SP),
    )

    return jax.shard_map(
        on_device, mesh=torus, in_specs=placed, out_specs=P(SP_TP, None), check_vma=False
    )
```

```python
import jax
import jax.numpy as jnp
from jax import lax
from jax.experimental import pallas as pl
from jax.experimental.pallas import tpu as pltpu
from jax.sharding import Mesh
from jax.sharding import PartitionSpec as P

HEAD_K = 128
KERNEL = 31
BLOCK = 64
HALO = 32
SP = ("sp_0", "sp_1")
TP = ("x", "core")
SP_TP = SP + TP
F32 = jnp.float32
BF16 = jnp.bfloat16
EXACT = lax.Precision.HIGHEST


def dot_nt(a, b):
    return lax.dot_general(a, b, (((1,), (1,)), ((), ())), preferred_element_type=F32)


def dot_tn(a, b):
    return lax.dot_general(a, b, (((0,), (0,)), ((), ())), preferred_element_type=F32)


def call(body, outs, *args, grid=None, in_specs=None, out_specs=None, scratch=()):
    specs = {}
    if in_specs is not None:
        specs["in_specs"] = in_specs
    if out_specs is not None:
        specs["out_specs"] = out_specs
    if grid is not None:
        specs["grid"] = grid
    return pl.pallas_call(body, out_shape=outs, scratch_shapes=scratch, **specs)(*args)


def whole(count):
    return [pl.BlockSpec(memory_space=pltpu.VMEM)] * count


def first_body(gv, gg, q, g, wr, wc, f, v, operand, copies):
    operand[...] = jnp.concatenate([w[...] for w in (gv, gg, q, g, wr, wc)], axis=1)
    joined = jnp.concatenate([f[...], v[...]], axis=1)
    for k in range(copies.shape[0]):
        copies[k] = joined


def again_body(value, copies):
    for k in range(copies.shape[0]):
        copies[k] = value[...]


def norm_body(places, gain, *refs):
    *pieces, out, tail = refs
    share = tail.shape[0]
    for n, piece in enumerate(pieces):
        values_in = piece[...].astype(F32)
        row_scale = lax.rsqrt(jnp.mean(values_in * values_in, axis=1, keepdims=True) + 1e-06)
        scaled = (values_in * row_scale * gain[...]).astype(BF16)
        out[pl.ds(pl.multiple_of(places[n] * share, share), share)] = scaled
    tail[...] = out[out.shape[0] - share :]


def pack_state(out, state, total):
    high = total.astype(BF16).astype(F32)
    row = lax.broadcasted_iota(jnp.int32, (8, total.shape[1]), 0)
    tail = jnp.where(row == 0, high, jnp.where(row == 1, total - high, 0.0)).astype(BF16)
    state = state.astype(BF16)
    width = state.shape[0]
    for k in range(out.shape[0]):
        out[k, :width] = state
        out[k, width:] = tail


def causal_mask():
    at_row = lax.broadcasted_iota(jnp.int32, (BLOCK, BLOCK), 0)
    at_col = lax.broadcasted_iota(jnp.int32, (BLOCK, BLOCK), 1)
    return at_row >= at_col


def state_body(normed, weights, leak, shift, sent, value_out, key, totals, starts, befores):
    rows = normed.shape[0]
    projected = jnp.dot(normed[...], weights[...], preferred_element_type=F32).astype(BF16)
    value = projected[:, HEAD_K:]
    value_out[...] = value
    in_gate = leak[...] * jax.nn.sigmoid(-projected[:, :HEAD_K].astype(F32))
    log_decay = jnp.log1p(-in_gate) + shift[...]
    triangle = jnp.where(causal_mask(), 1.0, 0.0).astype(F32)
    state = jnp.zeros((HEAD_K, HEAD_K), F32)
    before = jnp.zeros((1, HEAD_K), F32)
    kept = []
    for n in range(rows // BLOCK):
        at = slice(n * BLOCK, (n + 1) * BLOCK)
        total = jnp.dot(triangle, log_decay[at], precision=EXACT, preferred_element_type=F32)
        last = total[BLOCK - 1 :]
        totals[at] = total
        key[at] = (in_gate[at] * jnp.exp(-total)).astype(BF16)
        starts[n] = state.astype(BF16)
        kept.append(before)
        late_key = (in_gate[at] * jnp.exp(last - total)).astype(BF16)
        state = jnp.exp(last) * state + dot_tn(value[at], late_key)
        before = before + last
    befores[...] = jnp.concatenate(kept, axis=0)
    pack_state(sent, state, before)


def unpack(got, k):
    tail = got[k, HEAD_K:].astype(F32)
    return got[k, :HEAD_K].astype(F32), tail[0:1] + tail[1:2]


def gathered_before(got, position):
    state = inside_state = jnp.zeros((HEAD_K, HEAD_K), F32)
    total = inside_total = jnp.zeros((1, HEAD_K), F32)
    for k in range(got.shape[0]):
        passed = k < position
        new_state, new_total = unpack(got, k)
        state = jnp.exp(new_total) * state + new_state
        total = total + new_total
        inside_state = jnp.where(passed, state, inside_state)
        inside_total = jnp.where(passed, total, inside_total)
    return inside_state, inside_total, state, total


def inner_body(position, got, sent, inner_state, inner_total):
    inside_state, inside_total, state, total = gathered_before(got, position[0])
    inner_state[...] = inside_state
    inner_total[...] = jnp.broadcast_to(inside_total, inner_total.shape)
    pack_state(sent, state, total)


def outer_body(position, got, inner_state, inner_total, starts, befores, states):
    outside_state = gathered_before(got, position[0])[0]
    incoming = jnp.exp(inner_total[0:1]) * outside_state + inner_state[...]
    for n in range(starts.shape[0]):
        state = jnp.exp(befores[n : n + 1]) * incoming + starts[n].astype(F32)
        states[n] = state.astype(BF16)


def head_body(normed, weights, value, key, totals, states, gain, out):
    projected = jnp.dot(normed[...], weights[...], preferred_element_type=F32)
    projected = projected.astype(BF16).astype(F32)
    queries = jax.nn.silu(projected[:, :HEAD_K])
    gate_act = jax.nn.silu(projected[:, HEAD_K:])
    causal = causal_mask()
    for n in range(states.shape[0]):
        at = slice(n * BLOCK, (n + 1) * BLOCK)
        query = (queries[at] * jnp.exp(totals[at])).astype(BF16)
        scores = jnp.where(causal, dot_nt(query, key[at]), 0.0).astype(BF16)
        recur = jnp.dot(scores, value[at], preferred_element_type=F32)
        recur = recur + dot_nt(query, states[n])
        scaling = lax.rsqrt(jnp.mean(recur * recur, axis=1, keepdims=True) + 1e-06)
        out[at] = (recur * scaling * gain[...] * gate_act[at]).astype(BF16)


def conv_body(halo, normed, weights, taps, _, conv, stats, shifted):
    channels = conv.shape[1]
    rows = conv.shape[0]
    filled = HALO + rows
    extended = jnp.concatenate([halo[...], normed[...]], axis=0)
    projected = jnp.dot(extended, weights[...], preferred_element_type=F32)
    projected = projected.astype(BF16).astype(F32)
    glu = projected[:, :channels] * jax.nn.sigmoid(projected[:, channels:])
    shifted[0, :filled] = glu.astype(BF16).astype(F32)
    for r in range(1, 8):
        shifted[r, : filled - 8] = shifted[0, r : filled - 8 + r]
    first = HALO - (KERNEL - 1)
    step = 64
    for row in range(0, rows, step):
        accum = jnp.zeros((step, channels), F32)
        for tap in range(KERNEL):
            off = row + first + tap
            base = off // 8 * 8
            accum = accum + taps[tap : tap + 1] * shifted[off - base, base : base + step]
        conv[row : row + step] = accum
    summed = conv[...]
    lane = lax.broadcasted_iota(jnp.int32, (rows, 128), 1)
    sums = jnp.sum(summed, axis=1, keepdims=True)
    squares = jnp.sum(summed * summed, axis=1, keepdims=True)
    both = jnp.where(lane == 0, sums, squares).T[0:2]
    for k in range(stats.shape[0]):
        stats[k] = both


def out_body(core, stats, conv, head_out, ln_gain, ln_bias, w_rec, w_low, w_high, out, own, rows_out):
    channels = conv.shape[1]
    share = conv.shape[0] // stats.shape[0]
    both = stats[0]
    for k in range(1, stats.shape[0]):
        both = both + stats[k]
    both = both / (channels * stats.shape[0])
    mean = both[0:1]
    inverse = lax.rsqrt(both[1:2] - mean * mean + 1e-05)
    row = lax.broadcasted_iota(jnp.int32, (128, both.shape[1]), 0)
    turned = jnp.where(row == 0, mean, inverse).T
    normal = (conv[...] - turned[:, 0:1]) * turned[:, 1:2] * ln_gain[...] + ln_bias[...]
    conv_out = jax.nn.silu(normal).astype(BF16)
    for k in range(stats.shape[0]):
        piece = slice(k * share, (k + 1) * share)
        at = slice(k // 2 * share, (k // 2 + 1) * share)
        rows_out[k % 2, at, :HEAD_K] = head_out[piece]
        rows_out[k % 2, at, HEAD_K:] = conv_out[piece]
    out[...] = product(rows_out[1 - core[0]], w_rec, w_low, w_high)
    own[...] = product(rows_out[core[0]], w_rec, w_low, w_high)


def product(rows, w_rec, w_low, w_high):
    mixed = dot_nt(rows[:, :HEAD_K], w_rec[...])
    mixed = mixed + dot_nt(rows[:, HEAD_K : 2 * HEAD_K], w_low[...])
    mixed = mixed + dot_nt(rows[:, 2 * HEAD_K :], w_high[...])
    return mixed.astype(BF16)


def swap(value, axis):
    return lax.all_to_all(value, axis, split_axis=0, concat_axis=0, tiled=True)


def shifted_around(value, axis):
    count = lax.axis_size(axis)
    pieces = [value]
    for k in range(1, count):
        pieces.append(lax.ppermute(value, axis, [(n, (n + k) % count) for n in range(count)]))
    return pieces, (lax.axis_index(axis) + count - jnp.arange(count, dtype=jnp.int32)) % count


def on_device(
    tokens,
    norm_gain,
    w_query,
    w_forget,
    w_value,
    w_outgate,
    leak,
    decay_shift,
    head_gain,
    w_glu_value,
    w_glu_gate,
    conv_kernel,
    ln_gain,
    ln_bias,
    w_out_rec,
    w_out_conv,
):
    shape = jax.ShapeDtypeStruct
    smem = pl.BlockSpec(memory_space=pltpu.SMEM)
    inner_count = lax.axis_size(SP[1])
    group = lax.axis_size(TP)
    share, features = tokens.shape
    depth = w_query.shape[0]
    channels = conv_kernel.shape[1]
    columns = (w_glu_value, w_glu_gate, w_query, w_outgate, w_out_rec.T, w_out_conv.T)
    glu_width = 2 * channels
    all_width = sum(w.shape[1] for w in columns)
    outer_count = lax.axis_size(SP[0])
    operand, copies = call(
        first_body,
        (
            shape((depth, all_width), BF16),
            shape((inner_count, depth, 2 * HEAD_K), BF16),
        ),
        *columns,
        w_forget,
        w_value,
    )
    gathered = lax.all_gather(operand, SP, axis=0, tiled=True)
    column = swap(copies, SP[1])
    copies = call(again_body, shape((outer_count, *column.shape), BF16), column)
    state_weights = swap(copies, SP[0]).reshape(-1, 2 * HEAD_K)
    pieces, places = shifted_around(tokens, TP)
    rows = group * share
    normed, tail = call(
        norm_body,
        (shape((rows, features), BF16), shape((share, features), BF16)),
        places,
        norm_gain.reshape(1, -1),
        *pieces,
        in_specs=[smem] + whole(1 + len(pieces)),
    )
    count = lax.axis_size(SP)
    halo = lax.ppermute(tail, SP, [(k, k + 1) for k in range(count - 1)])
    message = shape((inner_count, HEAD_K + 8, HEAD_K), BF16)
    blocks = rows // BLOCK
    sent, *kept = call(
        state_body,
        (
            message,
            shape((rows, HEAD_K), BF16),
            shape((rows, HEAD_K), BF16),
            shape((rows, HEAD_K), F32),
            shape((blocks, HEAD_K, HEAD_K), BF16),
            shape((blocks, HEAD_K), F32),
        ),
        normed,
        state_weights,
        leak.reshape(1, -1),
        decay_shift,
    )
    sent, inner_state, inner_total = call(
        inner_body,
        (message, shape((HEAD_K, HEAD_K), F32), shape((8, HEAD_K), F32)),
        lax.axis_index(SP[1]).reshape(1),
        swap(sent, SP[1]),
        in_specs=[smem] + whole(1),
    )

    def part(size, at):
        return pl.BlockSpec((gathered.shape[0], size), lambda k: (0, at))

    def full(*lengths):
        return pl.BlockSpec(lengths, lambda k: (0,) * len(lengths))

    *kept, starts, befores = kept
    states = call(
        outer_body,
        shape(starts.shape, BF16),
        lax.axis_index(SP[0]).reshape(1),
        swap(sent, SP[0]),
        inner_state,
        inner_total,
        starts,
        befores,
        in_specs=[smem] + whole(5),
    )
    conv, stats = call(
        conv_body,
        (shape((rows, channels), F32), shape((group, 2, rows), F32)),
        halo,
        normed,
        gathered,
        conv_kernel,
        states,
        grid=(1,),
        in_specs=[
            full(*halo.shape),
            full(*normed.shape),
            part(glu_width, 0),
            full(*conv_kernel.shape),
            pl.BlockSpec(memory_space=pl.ANY),
        ],
        out_specs=(full(rows, channels), full(group, 2, rows)),
        scratch=(pltpu.VMEM((8, HALO + rows, channels), F32),),
    )
    stats = swap(stats, TP)
    head_gain = head_gain.reshape(1, -1)
    kept = (*kept, states, head_gain)
    head_out = call(
        head_body,
        shape((rows, HEAD_K), BF16),
        normed,
        gathered,
        *kept,
        grid=(1,),
        in_specs=[
            full(*normed.shape),
            part(2 * HEAD_K, glu_width // (2 * HEAD_K)),
            *[full(*a.shape) for a in kept],
        ],
        out_specs=full(rows, HEAD_K),
    )
    first = glu_width // HEAD_K + 2
    half = rows // 2
    width = HEAD_K + channels
    core = lax.axis_index(TP[1]).reshape(1)
    weights = [gathered] * 3
    weight_specs = [part(HEAD_K, first + k) for k in range(3)]
    sent, own = call(
        out_body,
        (shape((half, features), BF16),) * 2,
        core,
        stats,
        conv,
        head_out,
        ln_gain.reshape(1, -1),
        ln_bias.reshape(1, -1),
        *weights,
        grid=(1,),
        in_specs=[
            smem,
            full(*stats.shape),
            full(rows, channels),
            full(rows, HEAD_K),
            full(1, channels),
            full(1, channels),
            *weight_specs,
        ],
        out_specs=(full(half, features),) * 2,
        scratch=(pltpu.VMEM((2, half, width), BF16),),
    )
    received = lax.ppermute(sent, TP[1], [(0, 1), (1, 0)])
    pair = (own.astype(F32) + received.astype(F32)).astype(BF16)
    arrived = swap(pair.reshape(group // 2, share, features), TP[0])
    return arrived.astype(F32).sum(axis=0).astype(BF16)


def solution(mesh):
    torus = Mesh(mesh.devices.reshape(8, 8, mesh.shape["tp"] // 2, 2), SP_TP)
    placed = (
        P(SP_TP, None),
        P(),
        P(SP, TP),
        P(SP, TP),
        P(SP, TP),
        P(SP, TP),
        P(TP),
        P(SP, TP),
        P(),
        P(SP, TP),
        P(SP, TP),
        P(None, TP),
        P(TP),
        P(TP),
        P(TP, SP),
        P(TP, SP),
    )

    return jax.shard_map(
        on_device, mesh=torus, in_specs=placed, out_specs=P(SP_TP, None), check_vma=False
    )
```

```python
import jax
import jax.numpy as jnp
from jax import lax
from jax.experimental import pallas as pl
from jax.experimental.pallas import tpu as pltpu
from jax.sharding import Mesh
from jax.sharding import PartitionSpec as P

HEAD_K = 128
KERNEL = 31
BLOCK = 64
HALO = 32
SP = ("sp_0", "sp_1")
TP = ("x", "core")
SP_TP = SP + TP
F32 = jnp.float32
BF16 = jnp.bfloat16
EXACT = lax.Precision.HIGHEST


def dot_nt(a, b):
    return lax.dot_general(a, b, (((1,), (1,)), ((), ())), preferred_element_type=F32)


def dot_tn(a, b):
    return lax.dot_general(a, b, (((0,), (0,)), ((), ())), preferred_element_type=F32)


def call(body, outs, *args, grid=None, in_specs=None, out_specs=None, scratch=()):
    specs = {}
    if in_specs is not None:
        specs["in_specs"] = in_specs
    if out_specs is not None:
        specs["out_specs"] = out_specs
    if grid is not None:
        specs["grid"] = grid
    return pl.pallas_call(body, out_shape=outs, scratch_shapes=scratch, **specs)(*args)


def whole(count):
    return [pl.BlockSpec(memory_space=pltpu.VMEM)] * count


def first_body(gv, gg, q, g, wr, wc, f, v, operand, copies):
    operand[...] = jnp.concatenate([w[...] for w in (gv, gg, q, g, wr, wc)], axis=1)
    joined = jnp.concatenate([f[...], v[...]], axis=1)
    for k in range(copies.shape[0]):
        copies[k] = joined


def again_body(value, copies):
    for k in range(copies.shape[0]):
        copies[k] = value[...]


def norm_body(places, gain, *refs):
    *pieces, out, tail = refs
    share = tail.shape[0]
    for n, piece in enumerate(pieces):
        values_in = piece[...].astype(F32)
        row_scale = lax.rsqrt(jnp.mean(values_in * values_in, axis=1, keepdims=True) + 1e-06)
        scaled = (values_in * row_scale * gain[...]).astype(BF16)
        out[pl.ds(pl.multiple_of(places[n] * share, share), share)] = scaled
    tail[...] = out[out.shape[0] - share :]


def pack_state(out, state, total):
    high = total.astype(BF16).astype(F32)
    row = lax.broadcasted_iota(jnp.int32, (8, total.shape[1]), 0)
    tail = jnp.where(row == 0, high, jnp.where(row == 1, total - high, 0.0)).astype(BF16)
    state = state.astype(BF16)
    width = state.shape[0]
    for k in range(out.shape[0]):
        out[k, :width] = state
        out[k, width:] = tail


def causal_mask():
    at_row = lax.broadcasted_iota(jnp.int32, (BLOCK, BLOCK), 0)
    at_col = lax.broadcasted_iota(jnp.int32, (BLOCK, BLOCK), 1)
    return at_row >= at_col


def state_body(normed, weights, leak, shift, sent, value_out, key, totals, starts, befores):
    rows = normed.shape[0]
    projected = jnp.dot(normed[...], weights[...], preferred_element_type=F32).astype(BF16)
    value = projected[:, HEAD_K:]
    value_out[...] = value
    in_gate = leak[...] * jax.nn.sigmoid(-projected[:, :HEAD_K].astype(F32))
    log_decay = jnp.log1p(-in_gate) + shift[...]
    triangle = jnp.where(causal_mask(), 1.0, 0.0).astype(F32)
    state = jnp.zeros((HEAD_K, HEAD_K), F32)
    before = jnp.zeros((1, HEAD_K), F32)
    kept = []
    for n in range(rows // BLOCK):
        at = slice(n * BLOCK, (n + 1) * BLOCK)
        total = jnp.dot(triangle, log_decay[at], precision=EXACT, preferred_element_type=F32)
        last = total[BLOCK - 1 :]
        totals[at] = total
        key[at] = (in_gate[at] * jnp.exp(-total)).astype(BF16)
        starts[n] = state.astype(BF16)
        kept.append(before)
        late_key = (in_gate[at] * jnp.exp(last - total)).astype(BF16)
        state = jnp.exp(last) * state + dot_tn(value[at], late_key)
        before = before + last
    befores[...] = jnp.concatenate(kept, axis=0)
    pack_state(sent, state, before)


def unpack(got, k):
    tail = got[k, HEAD_K:].astype(F32)
    return got[k, :HEAD_K].astype(F32), tail[0:1] + tail[1:2]


def gathered_before(got, position):
    state = inside_state = jnp.zeros((HEAD_K, HEAD_K), F32)
    total = inside_total = jnp.zeros((1, HEAD_K), F32)
    for k in range(got.shape[0]):
        passed = k < position
        new_state, new_total = unpack(got, k)
        state = jnp.exp(new_total) * state + new_state
        total = total + new_total
        inside_state = jnp.where(passed, state, inside_state)
        inside_total = jnp.where(passed, total, inside_total)
    return inside_state, inside_total, state, total


def inner_body(position, got, sent, inner_state, inner_total):
    inside_state, inside_total, state, total = gathered_before(got, position[0])
    inner_state[...] = inside_state
    inner_total[...] = jnp.broadcast_to(inside_total, inner_total.shape)
    pack_state(sent, state, total)


def outer_body(
    position,
    got,
    inner_state,
    inner_total,
    normed,
    weights,
    value,
    key,
    totals,
    starts,
    befores,
    gain,
    out,
):
    outside_state = gathered_before(got, position[0])[0]
    incoming = jnp.exp(inner_total[0:1]) * outside_state + inner_state[...]
    projected = jnp.dot(normed[...], weights[...], preferred_element_type=F32)
    projected = projected.astype(BF16).astype(F32)
    queries = jax.nn.silu(projected[:, :HEAD_K])
    gate_act = jax.nn.silu(projected[:, HEAD_K:])
    causal = causal_mask()
    for n in range(starts.shape[0]):
        at = slice(n * BLOCK, (n + 1) * BLOCK)
        query = (queries[at] * jnp.exp(totals[at])).astype(BF16)
        scores = jnp.where(causal, dot_nt(query, key[at]), 0.0).astype(BF16)
        state = jnp.exp(befores[n : n + 1]) * incoming + starts[n].astype(F32)
        recur = jnp.dot(scores, value[at], preferred_element_type=F32)
        recur = recur + dot_nt(query, state.astype(BF16))
        scaling = lax.rsqrt(jnp.mean(recur * recur, axis=1, keepdims=True) + 1e-06)
        out[at] = (recur * scaling * gain[...] * gate_act[at]).astype(BF16)


def conv_body(halo, normed, weights, taps, conv, stats, shifted):
    channels = conv.shape[1]
    rows = conv.shape[0]
    filled = HALO + rows
    extended = jnp.concatenate([halo[...], normed[...]], axis=0)
    projected = jnp.dot(extended, weights[...], preferred_element_type=F32)
    projected = projected.astype(BF16).astype(F32)
    glu = projected[:, :channels] * jax.nn.sigmoid(projected[:, channels:])
    shifted[0, :filled] = glu.astype(BF16).astype(F32)
    for r in range(1, 8):
        shifted[r, : filled - 8] = shifted[0, r : filled - 8 + r]
    first = HALO - (KERNEL - 1)
    step = 128
    for row in range(0, rows, step):
        accum = jnp.zeros((step, channels), F32)
        for tap in range(KERNEL):
            off = row + first + tap
            base = off // 8 * 8
            accum = accum + taps[tap : tap + 1] * shifted[off - base, base : base + step]
        conv[row : row + step] = accum
    summed = conv[...]
    lane = lax.broadcasted_iota(jnp.int32, (rows, 128), 1)
    sums = jnp.sum(summed, axis=1, keepdims=True)
    squares = jnp.sum(summed * summed, axis=1, keepdims=True)
    both = jnp.where(lane == 0, sums, squares).T[0:2]
    for k in range(stats.shape[0]):
        stats[k] = both


def out_body(core, stats, conv, head_out, ln_gain, ln_bias, w_rec, w_low, w_high, out, own, rows_out):
    channels = conv.shape[1]
    share = conv.shape[0] // stats.shape[0]
    both = stats[0]
    for k in range(1, stats.shape[0]):
        both = both + stats[k]
    both = both / (channels * stats.shape[0])
    mean = both[0:1]
    inverse = lax.rsqrt(both[1:2] - mean * mean + 1e-05)
    row = lax.broadcasted_iota(jnp.int32, (128, both.shape[1]), 0)
    turned = jnp.where(row == 0, mean, inverse).T
    normal = (conv[...] - turned[:, 0:1]) * turned[:, 1:2] * ln_gain[...] + ln_bias[...]
    conv_out = jax.nn.silu(normal).astype(BF16)
    for k in range(stats.shape[0]):
        piece = slice(k * share, (k + 1) * share)
        at = slice(k // 2 * share, (k // 2 + 1) * share)
        rows_out[k % 2, at, :HEAD_K] = head_out[piece]
        rows_out[k % 2, at, HEAD_K:] = conv_out[piece]
    out[...] = product(rows_out[1 - core[0]], w_rec, w_low, w_high)
    own[...] = product(rows_out[core[0]], w_rec, w_low, w_high)


def product(rows, w_rec, w_low, w_high):
    mixed = dot_nt(rows[:, :HEAD_K], w_rec[...])
    mixed = mixed + dot_nt(rows[:, HEAD_K : 2 * HEAD_K], w_low[...])
    mixed = mixed + dot_nt(rows[:, 2 * HEAD_K :], w_high[...])
    return mixed.astype(BF16)


def swap(value, axis):
    return lax.all_to_all(value, axis, split_axis=0, concat_axis=0, tiled=True)


def shifted_around(value, axis):
    count = lax.axis_size(axis)
    pieces = [value]
    for k in range(1, count):
        pieces.append(lax.ppermute(value, axis, [(n, (n + k) % count) for n in range(count)]))
    return pieces, (lax.axis_index(axis) + count - jnp.arange(count, dtype=jnp.int32)) % count


def on_device(
    tokens,
    norm_gain,
    w_query,
    w_forget,
    w_value,
    w_outgate,
    leak,
    decay_shift,
    head_gain,
    w_glu_value,
    w_glu_gate,
    conv_kernel,
    ln_gain,
    ln_bias,
    w_out_rec,
    w_out_conv,
):
    shape = jax.ShapeDtypeStruct
    smem = pl.BlockSpec(memory_space=pltpu.SMEM)
    inner_count = lax.axis_size(SP[1])
    group = lax.axis_size(TP)
    share, features = tokens.shape
    depth = w_query.shape[0]
    channels = conv_kernel.shape[1]
    columns = (w_glu_value, w_glu_gate, w_query, w_outgate, w_out_rec.T, w_out_conv.T)
    glu_width = 2 * channels
    all_width = sum(w.shape[1] for w in columns)
    outer_count = lax.axis_size(SP[0])
    operand, copies = call(
        first_body,
        (
            shape((depth, all_width), BF16),
            shape((inner_count, depth, 2 * HEAD_K), BF16),
        ),
        *columns,
        w_forget,
        w_value,
    )
    gathered = lax.all_gather(operand, SP, axis=0, tiled=True)
    column = swap(copies, SP[1])
    copies = call(again_body, shape((outer_count, *column.shape), BF16), column)
    state_weights = swap(copies, SP[0]).reshape(-1, 2 * HEAD_K)
    pieces, places = shifted_around(tokens, TP)
    rows = group * share
    normed, tail = call(
        norm_body,
        (shape((rows, features), BF16), shape((share, features), BF16)),
        places,
        norm_gain.reshape(1, -1),
        *pieces,
        in_specs=[smem] + whole(1 + len(pieces)),
    )
    count = lax.axis_size(SP)
    halo = lax.ppermute(tail, SP, [(k, k + 1) for k in range(count - 1)])
    message = shape((inner_count, HEAD_K + 8, HEAD_K), BF16)
    blocks = rows // BLOCK
    sent, *kept = call(
        state_body,
        (
            message,
            shape((rows, HEAD_K), BF16),
            shape((rows, HEAD_K), BF16),
            shape((rows, HEAD_K), F32),
            shape((blocks, HEAD_K, HEAD_K), BF16),
            shape((blocks, HEAD_K), F32),
        ),
        normed,
        state_weights,
        leak.reshape(1, -1),
        decay_shift,
    )
    sent, inner_state, inner_total = call(
        inner_body,
        (message, shape((HEAD_K, HEAD_K), F32), shape((8, HEAD_K), F32)),
        lax.axis_index(SP[1]).reshape(1),
        swap(sent, SP[1]),
        in_specs=[smem] + whole(1),
    )

    def part(size, at):
        return pl.BlockSpec((gathered.shape[0], size), lambda k: (0, at))

    def full(*lengths):
        return pl.BlockSpec(lengths, lambda k: (0,) * len(lengths))

    conv, stats = call(
        conv_body,
        (shape((rows, channels), F32), shape((group, 2, rows), F32)),
        halo,
        normed,
        gathered,
        conv_kernel,
        grid=(1,),
        in_specs=[
            full(*halo.shape),
            full(*normed.shape),
            part(glu_width, 0),
            full(*conv_kernel.shape),
        ],
        out_specs=(full(rows, channels), full(group, 2, rows)),
        scratch=(pltpu.VMEM((8, HALO + rows, channels), F32),),
    )
    stats = swap(stats, TP)
    outer_sent = swap(sent, SP[0])
    head_gain = head_gain.reshape(1, -1)
    head_out = call(
        outer_body,
        shape((rows, HEAD_K), BF16),
        lax.axis_index(SP[0]).reshape(1),
        outer_sent,
        inner_state,
        inner_total,
        normed,
        gathered,
        *kept,
        head_gain,
        grid=(1,),
        in_specs=[
            smem,
            *[full(*a.shape) for a in (outer_sent, inner_state, inner_total, normed)],
            part(2 * HEAD_K, glu_width // (2 * HEAD_K)),
            *[full(*a.shape) for a in kept],
            full(*head_gain.shape),
        ],
        out_specs=full(rows, HEAD_K),
    )
    first = glu_width // HEAD_K + 2
    half = rows // 2
    width = HEAD_K + channels
    core = lax.axis_index(TP[1]).reshape(1)
    weights = [gathered] * 3
    weight_specs = [part(HEAD_K, first + k) for k in range(3)]
    sent, own = call(
        out_body,
        (shape((half, features), BF16),) * 2,
        core,
        stats,
        conv,
        head_out,
        ln_gain.reshape(1, -1),
        ln_bias.reshape(1, -1),
        *weights,
        grid=(1,),
        in_specs=[
            smem,
            full(*stats.shape),
            full(rows, channels),
            full(rows, HEAD_K),
            full(1, channels),
            full(1, channels),
            *weight_specs,
        ],
        out_specs=(full(half, features),) * 2,
        scratch=(pltpu.VMEM((2, half, width), BF16),),
    )
    received = lax.ppermute(sent, TP[1], [(0, 1), (1, 0)])
    pair = (own.astype(F32) + received.astype(F32)).astype(BF16)
    arrived = swap(pair.reshape(group // 2, share, features), TP[0])
    return arrived.astype(F32).sum(axis=0).astype(BF16)


def solution(mesh):
    torus = Mesh(mesh.devices.reshape(8, 8, mesh.shape["tp"] // 2, 2), SP_TP)
    placed = (
        P(SP_TP, None),
        P(),
        P(SP, TP),
        P(SP, TP),
        P(SP, TP),
        P(SP, TP),
        P(TP),
        P(SP, TP),
        P(),
        P(SP, TP),
        P(SP, TP),
        P(None, TP),
        P(TP),
        P(TP),
        P(TP, SP),
        P(TP, SP),
    )

    return jax.shard_map(
        on_device, mesh=torus, in_specs=placed, out_specs=P(SP_TP, None), check_vma=False
    )
```
